256 devices in a mesh: sp: 64 (over z, x, core), tp: 4 (over y).
Axes of the slice: x: 4, y: 4, z: 8, core: 2. Of those that a mesh axis runs over, the one named last changes fastest.
Arguments:
- query_rows: bfloat16 [32768, 1024], P('sp', 'tp'), may hold values from -6 to 6
- key_rows: bfloat16 [32768, 1024], P('sp', 'tp'), may hold values from -6 to 6
- value_rows: bfloat16 [32768, 2048], P('sp', 'tp'), may hold values from -6 to 6
- out_gate_pre: bfloat16 [32768, 2048], P('sp', 'tp'), may hold values from -8 to 8
- input_gate_pre: float32 [4, 32768], P('tp', 'sp'), may hold values from -8 to 8
- forget_gate_pre: float32 [4, 32768], P('tp', 'sp'), may hold values from -26 to 26
- residual: bfloat16 [32768, 2048], P(('sp', 'tp')), may hold values from -6 to 6
- out_proj: bfloat16 [2048, 2048], P('tp'), may hold values from -0.125 to 0.125
- mix_gain: float32 [2048], replicated, may hold values from 0.1 to 1.9
- pre_gain: float32 [2048], replicated, may hold values from 0.1 to 1.9
- gate_proj: bfloat16 [2048, 3072], P('sp', 'tp'), may hold values from -0.125 to 0.125
- value_proj: bfloat16 [2048, 3072], P('sp', 'tp'), may hold values from -0.125 to 0.125
- gate_kernel: float32 [3, 3072], P(None, 'tp'), may hold values from -3.5 to 3.5
- value_kernel: float32 [3, 3072], P(None, 'tp'), may hold values from -3.5 to 3.5
- down_proj: bfloat16 [2048, 3072], P('sp', 'tp'), may hold values from -0.109375 to 0.109375
- post_gain: float32 [2048], replicated, may hold values from 0.1 to 1.9
Outputs:
- result: bfloat16 [32768, 2048], P(('sp', 'tp'))
The draws below stay inside these ranges and needn't reach their ends.
All inputs are finite; a program needn't handle non-finite values.
Results may differ from the reference program's by a relative error of at most 0.017.
Values may be sent and summed in bfloat16 or wider, within the bound.
A program may use at most 128 MiB of HBM per device.

```python
import math
import jax
import jax.numpy as jnp
from jax import lax

D = 2048
HEADS = 4
QK = 256
HV = 512
FF = 3072
BLOCK = 64
CONV = 3
TOK_DEV = 512
SEQUENCE_TOKENS = 32768
N_TP = 4


def draw_forget_gate_pre(key, part):
    sequence_lanes = jax.random.split(jax.random.fold_in(key, 7301), 6)
    order = jax.random.permutation(sequence_lanes[0], HEADS)
    slow_count = HEADS // 2
    sluggish_decay = (order < slow_count)[:, None]
    spans = SEQUENCE_TOKENS // TOK_DEV
    factor = jnp.exp(jax.random.uniform(sequence_lanes[1], (HEADS, spans), jnp.float32, math.log(0.15), math.log(0.5)))
    factor = jnp.repeat(factor, TOK_DEV, axis=1)
    slow_rate = factor * (math.log(10.0) / SEQUENCE_TOKENS)
    fast_rate = jnp.exp(-jax.random.uniform(sequence_lanes[2], (HEADS, 1), jnp.float32, math.log(8.0), math.log(40.0)))
    rate = jnp.where(sluggish_decay, slow_rate, fast_rate)
    noise = 0.7 * jax.random.normal(sequence_lanes[3], (HEADS, SEQUENCE_TOKENS), jnp.float32)
    magnitude_value = -jnp.log(rate) + noise
    spike_locations = jax.random.randint(sequence_lanes[4], (4,), 0, SEQUENCE_TOKENS)
    spiked_entries = jnp.any(jnp.arange(SEQUENCE_TOKENS)[None, :] == spike_locations[:, None], axis=0)[None, :]
    retained_entries = jax.random.uniform(sequence_lanes[5], (HEADS, SEQUENCE_TOKENS), jnp.float32, 0.5, 0.8)
    spike_height = jnp.log(retained_entries / (1.0 - retained_entries))
    magnitude_value = jnp.where(spiked_entries & sluggish_decay, spike_height, magnitude_value)
    magnitude_value = jnp.clip(magnitude_value, -14.0, 14.0)
    ratio = magnitude_value / 15.0
    return 7.5 * jnp.log((1.0 + ratio) / (1.0 - ratio))


def steps_of(rng, extent, cuts, least, high):
    loudness = 1.0
    for dim, parts in cuts:
        draws = jax.random.uniform(jax.random.fold_in(jax.random.fold_in(rng, 6), dim), (parts,), jnp.float32, least / len(cuts), high / len(cuts))
        loudness = loudness * jnp.repeat(jnp.exp(draws), extent[dim] // parts).reshape((-1,) + (1,) * (len(extent) - 1 - dim))
    return loudness


def scatter_about(rng, extent, deviation, reach, pieces=(), kind=jnp.bfloat16):
    drawn = jax.random.normal(rng, extent, jnp.float32) * deviation
    if len(pieces) > 0:
        drawn = steps_of(rng, extent, pieces, -0.22, 0.18) * drawn
    return jnp.clip(drawn, min=-reach, max=reach).astype(kind)


def setup_inputs(seed: int = 0) -> dict:
    splits = jax.random.split(jax.random.key(seed), 17)
    query_rows = scatter_about(splits[0], (SEQUENCE_TOKENS, HEADS * QK), 1.0, 6.0, ((0, 64), (1, 4)))
    key_rows = scatter_about(splits[1], (SEQUENCE_TOKENS, HEADS * QK), 1.0, 6.0, ((0, 64), (1, 4)))
    value_rows = scatter_about(splits[2], (SEQUENCE_TOKENS, HEADS * HV), 1.0, 6.0, ((0, 64), (1, 4)))
    out_gate_pre = scatter_about(splits[3], (SEQUENCE_TOKENS, HEADS * HV), 1.5, 8.0, ((0, 64), (1, 4)))
    input_gate_pre = scatter_about(splits[4], (HEADS, SEQUENCE_TOKENS), 2.0, 8.0, ((0, 4), (1, 64)), jnp.float32)
    forget_gate_pre = draw_forget_gate_pre(jax.random.fold_in(splits[16], 71), 0)
    residual = scatter_about(splits[6], (SEQUENCE_TOKENS, D), 1.0, 6.0, ((0, 256),))
    out_proj = scatter_about(splits[7], (HEADS * HV, D), (HEADS * HV) ** -0.5, 0.125, ((0, 4),))
    mix_gain = jnp.clip(1.0 + 0.18 * jax.random.normal(splits[8], (D,), jnp.float32), 0.1, 1.9)
    pre_gain = jnp.clip(1.0 + 0.18 * jax.random.normal(splits[9], (D,), jnp.float32), 0.1, 1.9)
    gate_proj = scatter_about(splits[10], (D, FF), D ** -0.5, 0.125, ((0, 64), (1, 4)))
    value_proj = scatter_about(splits[11], (D, FF), D ** -0.5, 0.125, ((0, 64), (1, 4)))
    gate_kernel = scatter_about(splits[12], (CONV, FF), CONV ** -0.5, 3.5, ((1, 4),), jnp.float32)
    value_kernel = scatter_about(splits[13], (CONV, FF), CONV ** -0.5, 3.5, ((1, 4),), jnp.float32)
    down_proj = scatter_about(splits[14], (D, FF), FF ** -0.5, 0.109375, ((0, 64), (1, 4)))
    post_gain = jnp.clip(1.0 + 0.18 * jax.random.normal(splits[15], (D,), jnp.float32), 0.1, 1.9)
    return {"query_rows": query_rows, "key_rows": key_rows, "value_rows": value_rows, "out_gate_pre": out_gate_pre, "input_gate_pre": input_gate_pre, "forget_gate_pre": forget_gate_pre, "residual": residual, "out_proj": out_proj, "mix_gain": mix_gain, "pre_gain": pre_gain, "gate_proj": gate_proj, "value_proj": value_proj, "gate_kernel": gate_kernel, "value_kernel": value_kernel, "down_proj": down_proj, "post_gain": post_gain}


gate_cap = 15.0
epsilon = 1e-06
highest = lax.Precision.HIGHEST

def softcap(values):
    return gate_cap * jnp.tanh(values / gate_cap)

def normalize(values, gains):
    return values * lax.rsqrt(lax.optimization_barrier(jnp.mean(values * values, axis=-1, keepdims=True)) + epsilon) * gains

def barrier_round(values):
    rounded = lax.optimization_barrier(values.astype(jnp.bfloat16))
    return rounded.astype(jnp.float32)

def head_cells(inputs):
    queries, key_heads, value_heads, log_input, log_forget = inputs
    nblocks = SEQUENCE_TOKENS // BLOCK
    causal = jnp.tril(jnp.ones((BLOCK, BLOCK), dtype=bool))

    def advance(carried_state, block_inputs):
        memory, normer, stabilizer = carried_state
        query_blk, key_blk, value_blk, input_blk, forget_blk = block_inputs
        running = jnp.cumsum(forget_blk)
        block_total = running[-1]
        log_weights = jnp.where(causal, running[:, None] - running[None, :] + input_blk[None, :], -jnp.inf)
        carried = running + stabilizer
        row_max = jnp.maximum(carried, lax.optimization_barrier(jnp.max(log_weights, axis=1)))
        inner_weights = jnp.exp(log_weights - row_max[:, None])
        outer_weights = jnp.exp(carried - row_max)
        scores = jnp.dot(query_blk, key_blk.T, precision=highest) * inner_weights
        numerator = outer_weights[:, None] * jnp.dot(query_blk, memory, precision=highest) + jnp.dot(scores, value_blk, precision=highest)
        denominator = outer_weights * jnp.dot(query_blk, normer, precision=highest) + lax.optimization_barrier(jnp.sum(scores, axis=1))
        cell_rows = numerator / jnp.maximum(jnp.abs(denominator), jnp.exp(-row_max))[:, None]
        lead_logs = block_total - running + input_blk
        new_stabilizer = jnp.maximum(block_total + stabilizer, jnp.max(lead_logs))
        lead_weights = jnp.exp(lead_logs - new_stabilizer)
        decay_factor = jnp.exp(block_total + stabilizer - new_stabilizer)
        weighted = key_blk * lead_weights[:, None]
        memory = decay_factor * memory + jnp.dot(weighted.T, value_blk, precision=highest)
        normer = decay_factor * normer + lax.optimization_barrier(jnp.sum(weighted, axis=0))
        return ((memory, normer, new_stabilizer), cell_rows)
    initial = (jnp.zeros((QK, HV), jnp.float32), jnp.zeros((QK,), jnp.float32), jnp.zeros((), jnp.float32))
    stacked = (queries.reshape(nblocks, BLOCK, QK), key_heads.reshape(nblocks, BLOCK, QK), value_heads.reshape(nblocks, BLOCK, HV), log_input.reshape(nblocks, BLOCK), log_forget.reshape(nblocks, BLOCK))
    ignored, outputs = lax.scan(advance, initial, stacked)
    return outputs.reshape(SEQUENCE_TOKENS, HV)

def grouped_sum(left, right, right_axis):
    group_width = left.shape[1] // N_TP
    summed = jnp.zeros((left.shape[0], right.shape[1 - right_axis]), jnp.float32)
    for group_index in range(N_TP):
        left_part = left[:, group_index * group_width:(group_index + 1) * group_width]
        right_part = lax.slice_in_dim(right, group_index * group_width, (group_index + 1) * group_width, axis=right_axis)
        partial_sum = lax.dot_general(left_part, right_part, (((1,), (right_axis,)), ((), ())), preferred_element_type=jnp.float32)
        summed = summed + barrier_round(partial_sum)
    return summed.astype(jnp.bfloat16)

def depthwise(up_rows, kernel):
    length = up_rows.shape[0]
    padded = jnp.pad(up_rows.astype(jnp.float32), ((CONV - 1, 0), (0, 0)))
    summed = kernel[0] * padded[0:length]
    for offset in range(1, CONV):
        summed = summed + kernel[offset] * padded[offset:offset + length]
    return summed

def reference(query_rows, key_rows, value_rows, out_gate_pre, input_gate_pre, forget_gate_pre, residual, out_proj, mix_gain, pre_gain, gate_proj, value_proj, gate_kernel, value_kernel, down_proj, post_gain):
    query_scale = QK ** (-0.5)
    queries = query_rows.astype(jnp.float32).reshape(SEQUENCE_TOKENS, HEADS, QK).transpose(1, 0, 2) * query_scale
    key_heads = key_rows.astype(jnp.float32).reshape(SEQUENCE_TOKENS, HEADS, QK).transpose(1, 0, 2)
    value_heads = value_rows.astype(jnp.float32).reshape(SEQUENCE_TOKENS, HEADS, HV).transpose(1, 0, 2)
    log_input = softcap(input_gate_pre)
    log_forget = jax.nn.log_sigmoid(softcap(forget_gate_pre))
    cell_rows = lax.map(head_cells, (queries, key_heads, value_heads, log_input, log_forget))
    cell_rows = cell_rows.transpose(1, 0, 2).reshape(SEQUENCE_TOKENS, HEADS * HV)
    gated = (cell_rows * jax.nn.sigmoid(out_gate_pre.astype(jnp.float32))).astype(jnp.bfloat16)
    mixed = grouped_sum(gated, out_proj, 0)
    stream = (residual.astype(jnp.float32) + normalize(mixed.astype(jnp.float32), mix_gain)).astype(jnp.bfloat16)
    normed = normalize(stream.astype(jnp.float32), pre_gain).astype(jnp.bfloat16)
    up_gate = jnp.dot(normed, gate_proj, preferred_element_type=jnp.float32).astype(jnp.bfloat16)
    up_value = jnp.dot(normed, value_proj, preferred_element_type=jnp.float32).astype(jnp.bfloat16)
    hidden = (jax.nn.silu(depthwise(up_gate, gate_kernel)) * depthwise(up_value, value_kernel)).astype(jnp.bfloat16)
    ffn = grouped_sum(hidden, down_proj, 1)
    return (stream.astype(jnp.float32) + normalize(ffn.astype(jnp.float32), post_gain)).astype(jnp.bfloat16)
```

```python
import functools

import jax
import jax.numpy as jnp
from jax import lax
from jax.experimental import pallas as pl
from jax.experimental.pallas import tpu as pltpu
from jax.sharding import PartitionSpec as P

f32 = jnp.float32
bf16 = jnp.bfloat16
MESH = pl.DeviceIdType.MESH

gate_cap = 15.0
epsilon = 1e-06
far_below = -1e30
CONV = 3
LANES = 128
ROW_STEP = 64
NORM_STEP = 16
CONV_STEP = 32
TILE = 256

SHAPES = {64: (8, 4, 2)}


def softcap(values):
    return gate_cap * jnp.tanh(values * (1.0 / gate_cap))


def log_one_plus(values):
    series = values * (
        1.0 + values * (-1 / 2 + values * (1 / 3 + values * (-1 / 4 + values * (1 / 5))))
    )
    return jnp.where(values < 0.015625, series, jnp.log(1.0 + values))


def log_sigmoid(values):
    return jnp.minimum(values, 0.0) - log_one_plus(jnp.exp(-jnp.abs(values)))


def normalize(values, gains):
    return values * lax.rsqrt(jnp.mean(values * values, axis=-1, keepdims=True) + epsilon) * gains


def matmul(left, right, left_dim=1, right_dim=0):
    return lax.dot_general(
        left, right, (((left_dim,), (right_dim,)), ((), ())), preferred_element_type=f32
    )


def mod(value, size):
    return lax.rem(value + size, jnp.int32(size))


def kernel(
    Z, X, C, T,
    q_ref, k_ref, v_ref, og_ref, ig_ref, fg_ref, res_ref, mixg_ref, preg_ref, postg_ref,
    gk_ref, vk_ref, outp_ref, gatep_ref, valuep_ref, downp_ref,
    out_ref,
    msend, mrecv, st_src, st_recv, ssend, srecv, nin, m_in, kwb, runc, a1, m1, d1,
    gsend, grecv, wo, wu, wd, rows_all, mixed, stream, upb, hidden, pbuf, from_left, from_right,
    relay_top, relay_bot,
    loc, p1, p2, xs, xd, zs, zd, wos, wod, ags, rss, a2, halo,
):
    NSP = Z * X * C
    rows, qk = q_ref.shape
    hv = v_ref.shape[1]
    own, D = out_ref.shape
    ffd = gatep_ref.shape[1]
    scale = float(qk) ** -0.5
    me = lax.axis_index("sp")
    tp = lax.axis_index("tp")
    core = lax.rem(me, jnp.int32(C))
    xx = lax.rem(lax.div(me, jnp.int32(C)), jnp.int32(X))
    zz = lax.div(me, jnp.int32(C * X))
    pending = []

    def at_sp(index):
        return {"sp": index, "tp": tp}

    def at_tp(index):
        return {"sp": me, "tp": index}

    def send(src, dst, ssem, rsem, device):
        copy = pltpu.make_async_remote_copy(
            src_ref=src, dst_ref=dst, send_sem=ssem, recv_sem=rsem,
            device_id=device, device_id_type=MESH,
        )
        copy.start()
        pending.append(copy)

    def arrived(dst, ssem, rsem, device):
        pltpu.make_async_remote_copy(
            src_ref=dst, dst_ref=dst, send_sem=ssem, recv_sem=rsem,
            device_id=device, device_id_type=MESH,
        ).wait_recv()

    def ds(start, size, step=None):
        return pl.ds(pl.multiple_of(start, step or size), size)

    sibling = at_sp(me + 1 - 2 * core) if C == 2 else None

    barrier = pltpu.get_barrier_semaphore()

    def greet(p, carry):
        pl.semaphore_signal(
            barrier, 1, device_id=at_sp(mod(me + p, NSP)), device_id_type=MESH
        )
        return carry

    lax.fori_loop(1, NSP, greet, 0)
    for k in range(1, T):
        pl.semaphore_signal(barrier, 1, device_id=at_tp(mod(tp + k, T)), device_id_type=MESH)

    shard = gatep_ref.shape[0]
    wrows = outp_ref.shape[0]
    mine = ds(me * shard, shard)
    local = [
        pltpu.make_async_copy(gatep_ref, wu.at[mine, pl.ds(0, ffd)], loc.at[0]),
        pltpu.make_async_copy(valuep_ref, wu.at[mine, pl.ds(ffd, ffd)], loc.at[1]),
        pltpu.make_async_copy(downp_ref, wd.at[mine], loc.at[2]),
        pltpu.make_async_copy(outp_ref, wo.at[ds(tp * wrows, wrows)], loc.at[3]),
    ]
    for copy in local:
        copy.start()

    steps = rows // ROW_STEP
    lane = lax.broadcasted_iota(jnp.int32, (ROW_STEP, rows), 1)
    line = lax.broadcasted_iota(jnp.int32, (ROW_STEP, rows), 0)
    li_row = softcap(ig_ref[...])
    lf_row = log_sigmoid(softcap(fg_ref[...]))

    def sums(b, run_row):
        here = line + b * ROW_STEP
        run_col = jnp.sum(jnp.where(lane <= here, lf_row, 0.0), axis=1, keepdims=True)
        runc[ds(b * ROW_STEP, ROW_STEP), :] = run_col
        return run_row + jnp.sum(jnp.where(lane == here, run_col, 0.0), axis=0, keepdims=True)

    run_row = lax.fori_loop(0, steps, sums, jnp.zeros((1, rows), f32))
    total = run_row[:, rows - 1 : rows]
    lead = total - run_row + li_row
    lead_max = jnp.max(lead, axis=1, keepdims=True)
    lead_weights = jnp.exp(lead - lead_max)

    def weigh(b, normer):
        here = line + b * ROW_STEP
        at = ds(b * ROW_STEP, ROW_STEP)
        column = jnp.sum(jnp.where(lane == here, lead_weights, 0.0), axis=1, keepdims=True)
        weighted = k_ref[at, :].astype(f32) * column
        kwb[at, :] = weighted.astype(bf16)
        return normer + jnp.sum(weighted, axis=0, keepdims=True)

    normer = lax.fori_loop(0, steps, weigh, jnp.zeros((1, qk), f32))
    nq = qk // LANES
    for r in range(nq):
        st_src[r : r + 1, :] = normer[:, r * LANES : (r + 1) * LANES]
    for r in range(nq, 4):
        st_src[r : r + 1, :] = jnp.broadcast_to(total if r == nq else lead_max, (1, LANES))
    R = msend.shape[1]
    nc = hv // LANES
    for r in range(nq):
        part = matmul(kwb[:, r * LANES : (r + 1) * LANES], v_ref[...], 0, 0)
        for rr in range(LANES // R):
            for c in range(nc):
                msend[(r * (LANES // R) + rr) * nc + c] = part[
                    rr * R : (rr + 1) * R, c * LANES : (c + 1) * LANES
                ].astype(bf16)

    pl.semaphore_wait(barrier, NSP - 1 + T - 1)

    mrecv[me] = msend[me]
    st_recv[me] = st_src[...]

    def scatter(p, carry):
        dst = mod(me + p, NSP)
        for src, to, s in ((msend.at[dst], mrecv.at[me], 0), (st_src, st_recv.at[me], 2)):
            pltpu.make_async_remote_copy(
                src_ref=src, dst_ref=to, send_sem=p1.at[s], recv_sem=p1.at[s + 1],
                device_id=at_sp(dst), device_id_type=MESH,
            ).start()
        return carry

    lax.fori_loop(1, NSP, scatter, 0)

    for copy in local:
        copy.wait()

    left, right, across = mod(tp - 1, T), mod(tp + 1, T), mod(tp + 2, T)

    def ring_start(buf, base, half, sems):
        top, bottom = buf.at[ds(base(tp), half)], buf.at[ds(base(tp) + half, half)]
        for k, piece, device in ((0, top, right), (1, bottom, left), (2, bottom, right), (3, top, left)):
            send(piece, piece, sems.at[0, k], sems.at[1, k], at_tp(device))

    def ring_piece(buf, base, half, k):
        block, low = ((left, 0), (right, 1), (left, 1), (right, 0), (across, 0), (across, 1))[k]
        return buf.at[ds(base(block) + low * half, half)]

    def ring_wait(buf, base, half, sems, k):
        piece = ring_piece(buf, base, half, k)
        arrived(piece, sems.at[0, k], sems.at[1, k], at_tp(left))
        if k < 2:
            send(piece, piece, sems.at[0, k + 4], sems.at[1, k + 4], at_tp((right, left)[k]))
        return piece

    wcore = wrows // C
    whalf = wcore // 2

    def wo_base(block):
        return block * wrows + core * wcore

    def wo_twin_base(block):
        return block * wrows + (C - 1 - core) * wcore

    def wo_step(k):
        piece = ring_wait(wo, wo_base, whalf, wos, k)
        if C == 2:
            send(piece, piece, wod.at[0, k], wod.at[1, k], sibling)

    def at_zx(z, x, c):
        return z * (X * C) + x * C + c

    def shard_of(index):
        at = ds(index * shard, shard)
        return (wu.at[at], wd.at[at])

    for w, piece in enumerate(shard_of(me)):
        if C == 2:
            send(piece, piece, xd.at[0, 0, w], xd.at[1, 0, w], sibling)
        for k in range(1, X):
            to = at_sp(at_zx(zz, mod(xx + k, X), core))
            send(piece, piece, xs.at[0, k, w], xs.at[1, k, w], to)
    ring_start(wo, wo_base, whalf, wos)

    def inside(b, carry):
        at = ds(b * ROW_STEP, ROW_STEP)
        here = line + b * ROW_STEP
        logs = jnp.where(lane <= here, runc[at, :] - run_row + li_row, far_below)
        top = jnp.max(logs, axis=1, keepdims=True)
        scores = matmul(q_ref[at, :], k_ref[...], 1, 1) * (jnp.exp(logs - top) * scale)
        m1[at, :] = top
        d1[at, :] = jnp.sum(scores, axis=1, keepdims=True)
        a1[at, :] = matmul(scores.astype(bf16), v_ref[...])
        return carry

    lax.fori_loop(0, steps, inside, 0)

    for k in range(1, X):
        src = at_zx(zz, mod(xx - k, X), core)
        for w, piece in enumerate(shard_of(src)):
            arrived(piece, xs.at[0, k, w], xs.at[1, k, w], at_sp(src))
            if C == 2:
                send(piece, piece, xd.at[0, k, w], xd.at[1, k, w], sibling)

    def all_but_one(buf):
        return buf.at[pl.ds(0, NSP - 1)]

    def bulk(buf, sems, s):
        pltpu.make_async_remote_copy(
            src_ref=all_but_one(buf), dst_ref=all_but_one(buf),
            send_sem=sems.at[s], recv_sem=sems.at[s + 1],
            device_id=at_sp(me), device_id_type=MESH,
        ).wait()

    bulk(mrecv, p1, 0)
    bulk(st_recv, p1, 2)

    def advance(i, state):
        highest, memory, norm = state
        for u in range(8):
            d = i * 8 + u
            ssend[d] = memory.astype(bf16)
            nin[d, 0:nq, :] = norm
            nin[d, nq : nq + 1, :] = highest
            following = st_recv[d]
            decayed = highest + following[nq : nq + 1, :]
            lead_d = following[nq + 1 : nq + 2, :]
            highest = jnp.maximum(decayed, lead_d)
            before = jnp.exp(decayed - highest)
            after = jnp.exp(lead_d - highest)
            memory = before * memory + after * mrecv[d].astype(f32)
            norm = before * norm + after * following[0:nq, :]
        return highest, memory, norm

    lax.fori_loop(
        0, NSP // 8, advance,
        (jnp.full((1, LANES), far_below, f32), jnp.zeros((R, LANES), f32), jnp.zeros((nq, LANES), f32)),
    )
    srecv[me] = ssend[me]

    def give_back(p, carry):
        dst = mod(me + p, NSP)
        pltpu.make_async_remote_copy(
            src_ref=ssend.at[dst], dst_ref=srecv.at[me], send_sem=p2.at[0], recv_sem=p2.at[1],
            device_id=at_sp(dst), device_id_type=MESH,
        ).start()
        return carry

    lax.fori_loop(1, NSP, give_back, 0)

    wo_step(0)
    wo_step(1)

    slab = shard * X * C
    part_rows = slab // C
    half_rows = part_rows // 2
    if C == 2:
        for k in range(X):
            src = at_zx(zz, mod(xx - k, X), 1 - core)
            for w, piece in enumerate(shard_of(src)):
                arrived(piece, xd.at[0, k, w], xd.at[1, k, w], sibling)
    ups = (at_zx(mod(zz + 1, Z), xx, core), at_zx(mod(zz - 1, Z), xx, core))

    def z_piece(w, direction, s, h, c):
        z = mod(zz - s if direction == 0 else zz + s, Z)
        at = ds(z * slab + c * part_rows + h * half_rows, half_rows)
        return (wu, wd)[w].at[at]

    def z_has(direction, s, h):
        return s < Z // 2 or (s == Z // 2 and h == direction)

    def z_send(w, direction, s, h):
        if z_has(direction, s, h):
            piece = z_piece(w, direction, s - 1, h, core)
            i = (s - 1) * 2 + h
            send(
                piece, piece, zs.at[0, direction, w, i], zs.at[1, direction, w, i],
                at_sp(ups[direction]),
            )

    def z_start(w):
        for h in range(2):
            for direction in range(2):
                z_send(w, direction, 1, h)

    def z_step(w, s, h):
        for direction in range(2):
            if z_has(direction, s, h):
                piece = z_piece(w, direction, s, h, core)
                i = (s - 1) * 2 + h
                arrived(
                    piece, zs.at[0, direction, w, i], zs.at[1, direction, w, i],
                    at_sp(ups[direction]),
                )
                z_send(w, direction, s + 1, h)
                if C == 2:
                    send(piece, piece, zd.at[0, direction, w, i], zd.at[1, direction, w, i], sibling)

    def z_twin(w):
        for s in range(1, Z // 2 + 1):
            for h in range(2):
                for direction in range(2):
                    if C == 2 and z_has(direction, s, h):
                        piece = z_piece(w, direction, s, h, 1 - core)
                        i = (s - 1) * 2 + h
                        arrived(piece, zd.at[0, direction, w, i], zd.at[1, direction, w, i], sibling)

    z_events = [(0, s, h) for s in range(1, Z // 2 + 1) for h in range(2)]
    d_events = [(1, s, h) for s in range(1, Z // 2 + 1) for h in range(2)]
    z_start(0)
    for event in z_events[:2]:
        z_step(*event)

    bulk(srecv, p2, 0)
    for j in range(NSP):
        r, c = divmod(j, nc)
        m_in[r * R : (r + 1) * R, c * LANES : (c + 1) * LANES] = srecv[j]
    stats = nin[me]
    normer_in = jnp.concatenate([stats[r : r + 1, :] for r in range(nq)], axis=1)
    stab = stats[nq : nq + 1, 0:1]

    def finish(b, carry):
        at = ds(b * ROW_STEP, ROW_STEP)
        queries = q_ref[at, :]
        carried = runc[at, :] + stab
        top = m1[at, :]
        row_max = jnp.maximum(carried, top)
        inner = jnp.exp(top - row_max)
        outer = jnp.exp(carried - row_max) * scale
        reach = jnp.sum(queries.astype(f32) * normer_in, axis=1, keepdims=True)
        denominator = inner * d1[at, :] + outer * reach
        floor = jnp.maximum(jnp.abs(denominator), jnp.exp(-row_max))
        numerator = inner * a1[at, :] + outer * matmul(queries, m_in[...])
        gate = 1.0 / (1.0 + jnp.exp(-og_ref[at, :].astype(f32)))
        gsend[at, :] = (numerator / floor * gate).astype(bf16)
        return carry

    lax.fori_loop(0, steps, finish, 0)

    grecv[tp] = gsend[ds(tp * own, own), :]
    for k in range(1, T):
        dst = mod(tp + k, T)
        send(gsend.at[ds(dst * own, own)], grecv.at[tp], a2.at[0, k], a2.at[1, k], at_tp(dst))

    wo_step(2)
    wo_step(3)
    for event in z_events[2:4]:
        z_step(*event)
    wo_step(4)
    wo_step(5)
    if C == 2:
        for k in range(6):
            piece = ring_piece(wo, wo_twin_base, whalf, k)
            arrived(piece, wod.at[0, k], wod.at[1, k], sibling)
    for k in range(1, T):
        src = mod(tp - k, T)
        arrived(grecv.at[src], a2.at[0, k], a2.at[1, k], at_tp(src))

    def project(n, carry):
        at = ds(n * TILE, TILE)
        acc = matmul(grecv[0], wo[0:hv, at])
        for h in range(1, T):
            acc = acc + matmul(grecv[h], wo[h * hv : (h + 1) * hv, at])
        mixed[:, at] = acc
        return carry

    lax.fori_loop(0, D // TILE, project, 0)

    def join(b, carry):
        at = ds(b * NORM_STEP, NORM_STEP)
        values = mixed[at, :].astype(bf16).astype(f32)
        joined = (res_ref[at, :].astype(f32) + normalize(values, mixg_ref[...])).astype(bf16)
        stream[at, :] = joined
        rows_all[ds(tp * own + b * NORM_STEP, NORM_STEP), :] = normalize(
            joined.astype(f32), preg_ref[...]
        ).astype(bf16)
        return carry

    lax.fori_loop(0, own // NORM_STEP, join, 0)

    half = own // 2

    def block_base(block):
        return block * own

    ring_start(rows_all, block_base, half, ags)
    for event in z_events[4:6]:
        z_step(*event)
    ring_wait(rows_all, block_base, half, ags, 0)
    ring_wait(rows_all, block_base, half, ags, 1)
    z_start(1)
    for event in z_events[6:]:
        z_step(*event)
    for event in d_events[:2]:
        z_step(*event)
    z_twin(0)
    for k in range(2, 6):
        ring_wait(rows_all, block_base, half, ags, k)

    def raise_tile(n, carry):
        at = ds(n * TILE, TILE)
        upb[8 : 8 + rows, at] = matmul(rows_all[...], wu[:, at]).astype(bf16).astype(f32)
        return carry

    lax.fori_loop(0, 2 * ffd // TILE, raise_tile, 0)

    last = pltpu.make_async_remote_copy(
        src_ref=upb.at[pl.ds(rows, 8)], dst_ref=upb.at[pl.ds(0, 8)],
        send_sem=halo.at[0], recv_sem=halo.at[1],
        device_id=at_sp(mod(me + 1, NSP)), device_id_type=MESH,
    )

    @pl.when(me < NSP - 1)
    def _():
        last.start()

    for event in d_events[2:]:
        z_step(*event)

    @pl.when(me == 0)
    def _():
        upb[0:8, :] = jnp.zeros((8, 2 * ffd), f32)

    @pl.when(me > 0)
    def _():
        last.wait_recv()

    def convolve(b, carry):
        window = ds(b * CONV_STEP, CONV_STEP + 8, CONV_STEP)
        at = ds(b * CONV_STEP, CONV_STEP)
        for c in range(0, ffd, TILE):
            both = []
            for taps, first in ((gk_ref, 0), (vk_ref, ffd)):
                block = upb[window, first + c : first + c + TILE]
                total_taps = 0.0
                for j in range(CONV):
                    low = 8 - CONV + 1 + j
                    total_taps = total_taps + taps[j : j + 1, c : c + TILE] * block[low : low + CONV_STEP]
                both.append(total_taps)
            hidden[at, c : c + TILE] = (both[0] / (1.0 + jnp.exp(-both[0])) * both[1]).astype(bf16)
        return carry

    lax.fori_loop(0, rows // CONV_STEP, convolve, 0)
    z_twin(1)

    def lower(n, carry):
        at = ds(n * TILE, TILE)
        pbuf[:, at] = matmul(hidden[...], wd[at, :], 1, 1).astype(bf16)
        return carry

    lax.fori_loop(0, D // TILE, lower, 0)

    def piece_of(block, low):
        return pbuf.at[ds(block * own + low * half, half)]

    def rs(src, dst, k, device):
        send(src, dst, rss.at[0, k], rss.at[1, k], at_tp(device))

    top, bottom = pl.ds(0, half), pl.ds(half, half)
    rs(piece_of(across, 0), relay_top, 2, right)
    rs(piece_of(across, 1), relay_bot, 3, left)
    rs(piece_of(right, 1), from_left.at[bottom], 0, right)
    rs(piece_of(left, 0), from_right.at[top], 1, left)
    for k, relay, block, low, dst in (
        (2, relay_top, right, 0, from_left.at[top]),
        (3, relay_bot, left, 1, from_right.at[bottom]),
    ):
        arrived(relay, rss.at[0, k], rss.at[1, k], at_tp(left))

        def merge(b, carry, relay=relay, block=block, low=low):
            at = ds(b * NORM_STEP, NORM_STEP)
            there = ds(block * own + low * half + b * NORM_STEP, NORM_STEP)
            relay[at, :] = (relay[at, :].astype(f32) + pbuf[there, :].astype(f32)).astype(bf16)
            return carry

        lax.fori_loop(0, half // NORM_STEP, merge, 0)
        rs(relay, dst, k + 2, (right, left)[k - 2])
    arrived(from_left.at[bottom], rss.at[0, 0], rss.at[1, 0], at_tp(left))
    arrived(from_right.at[top], rss.at[0, 1], rss.at[1, 1], at_tp(right))
    arrived(from_left.at[top], rss.at[0, 4], rss.at[1, 4], at_tp(left))
    arrived(from_right.at[bottom], rss.at[0, 5], rss.at[1, 5], at_tp(right))

    def close(b, carry):
        at = ds(b * NORM_STEP, NORM_STEP)
        summed = (
            pbuf[ds(tp * own + b * NORM_STEP, NORM_STEP), :].astype(f32)
            + from_left[at, :].astype(f32)
            + from_right[at, :].astype(f32)
        )
        values = summed.astype(bf16).astype(f32)
        out_ref[at, :] = (
            stream[at, :].astype(f32) + normalize(values, postg_ref[...])
        ).astype(bf16)
        return carry

    lax.fori_loop(0, own // NORM_STEP, close, 0)

    for copy in pending:
        copy.wait_send()

    @pl.when(me < NSP - 1)
    def _():
        last.wait_send()


def body(
    shape,
    query_rows, key_rows, value_rows, out_gate_pre, input_gate_pre, forget_gate_pre, residual,
    out_proj, mix_gain, pre_gain, gate_proj, value_proj, gate_kernel, value_kernel, down_proj,
    post_gain,
):
    Z, X, C, T = shape
    NSP = Z * X * C
    rows, qk = query_rows.shape
    hv = value_rows.shape[1]
    own, D = residual.shape
    ffd = gate_proj.shape[1]
    R = qk * hv // LANES // NSP
    dma = pltpu.SemaphoreType.DMA
    vm = pltpu.VMEM
    inner = pl.BlockSpec(memory_space=pltpu.VMEM)
    outer = pl.BlockSpec(memory_space=pl.ANY)
    return pl.pallas_call(
        functools.partial(kernel, Z, X, C, T),
        out_shape=jax.ShapeDtypeStruct((own, D), bf16),
        in_specs=[inner] * 12 + [outer] * 4,
        out_specs=inner,
        scratch_shapes=[
            vm((NSP, R, LANES), bf16),
            vm((NSP, R, LANES), bf16),
            vm((4, LANES), f32),
            vm((NSP, 4, LANES), f32),
            vm((NSP, R, LANES), bf16),
            vm((NSP, R, LANES), bf16),
            vm((NSP, 4, LANES), f32),
            vm((qk, hv), bf16),
            vm((rows, qk), bf16),
            vm((rows, 1), f32),
            vm((rows, hv), f32),
            vm((rows, 1), f32),
            vm((rows, 1), f32),
            vm((rows, hv), bf16),
            vm((T, own, hv), bf16),
            vm((T * hv, D), bf16),
            vm((D, 2 * ffd), bf16),
            vm((D, ffd), bf16),
            vm((rows, D), bf16),
            vm((own, D), f32),
            vm((own, D), bf16),
            vm((rows + 8, 2 * ffd), f32),
            vm((rows, ffd), bf16),
            vm((rows, D), bf16),
            vm((own, D), bf16),
            vm((own, D), bf16),
            vm((own // 2, D), bf16),
            vm((own // 2, D), bf16),
            dma((4,)),
            dma((4,)),
            dma((2,)),
            dma((2, X, 2)),
            dma((2, X, 2)),
            dma((2, 2, 2, max(Z, 1))),
            dma((2, 2, 2, max(Z, 1))),
            dma((2, 6)),
            dma((2, 6)),
            dma((2, 6)),
            dma((2, 6)),
            dma((2, T)),
            dma((2,)),
        ],
        compiler_params=pltpu.CompilerParams(
            collective_id=0, has_side_effects=True, vmem_limit_bytes=60 * 1024 * 1024
        ),
        name="cell_and_mixer",
    )(
        query_rows, key_rows, value_rows, out_gate_pre, input_gate_pre, forget_gate_pre, residual,
        mix_gain.reshape(1, D), pre_gain.reshape(1, D), post_gain.reshape(1, D),
        gate_kernel, value_kernel, out_proj, gate_proj, value_proj, down_proj,
    )


def solution(mesh):
    shape = (*SHAPES[mesh.shape["sp"]], mesh.shape["tp"])
    placed = (
        P("sp", "tp"),
        P("sp", "tp"),
        P("sp", "tp"),
        P("sp", "tp"),
        P("tp", "sp"),
        P("tp", "sp"),
        P(("sp", "tp"), None),
        P("tp", None),
        P(),
        P(),
        P("sp", "tp"),
        P("sp", "tp"),
        P(None, "tp"),
        P(None, "tp"),
        P("sp", "tp"),
        P(),
    )
    return jax.shard_map(
        functools.partial(body, shape), mesh=mesh, in_specs=placed,
        out_specs=P(("sp", "tp"), None), check_vma=False,
    )
```

```python
import functools

import jax
import jax.numpy as jnp
from jax import lax
from jax.experimental import pallas as pl
from jax.experimental.pallas import tpu as pltpu
from jax.sharding import PartitionSpec as P

f32 = jnp.float32
bf16 = jnp.bfloat16
MESH = pl.DeviceIdType.MESH

gate_cap = 15.0
epsilon = 1e-06
far_below = -1e30
CONV = 3
LANES = 128
ROW_STEP = 64
NORM_STEP = 16
CONV_STEP = 32
TILE = 256
HALO = 16

SHAPES = {64: (8, 4, 2)}


def softcap(values):
    return gate_cap * jnp.tanh(values * (1.0 / gate_cap))


def log_one_plus(values):
    series = values * (
        1.0 + values * (-1 / 2 + values * (1 / 3 + values * (-1 / 4 + values * (1 / 5))))
    )
    return jnp.where(values < 0.015625, series, jnp.log(1.0 + values))


def log_sigmoid(values):
    return jnp.minimum(values, 0.0) - log_one_plus(jnp.exp(-jnp.abs(values)))


def normalize(values, gains):
    return values * lax.rsqrt(jnp.mean(values * values, axis=-1, keepdims=True) + epsilon) * gains


def matmul(left, right, left_dim=1, right_dim=0):
    return lax.dot_general(
        left, right, (((left_dim,), (right_dim,)), ((), ())), preferred_element_type=f32
    )


def mod(value, size):
    return lax.rem(value + size, jnp.int32(size))


def kernel(
    Z, X, C, T,
    q_in, k_in, v_in, og_in, ig_in, fg_in, res_in, mixg_in, preg_in, postg_in, gk_in, vk_in,
    outp_ref, gatep_ref, valuep_ref, downp_ref,
    out_ref,
    q_ref, k_ref, v_ref, og_ref, ig_ref, fg_ref, res_ref, mixg_ref, preg_ref, postg_ref, gk_own, vk_own,
    msend, mrecv, st_src, st_recv, ssend, srecv, nin, m_in, kwb, runc, a1, m1, d1,
    gated, wo, ushard, wu, dshard, wd, gk_ref, vk_ref, rows_all, stream, upb, hidden,
    mix_part, mix_left, mix_right, mix_top, mix_bot,
    ffn_part, ffn_left, ffn_right, ffn_top, ffn_bot,
    loc, loaded, p1, p2, xs, xd, zs, zd, taps, ags, mss, rss, halo,
):
    NSP = Z * X * C
    rows, qk = q_ref.shape
    hv = v_ref.shape[1]
    own, D = out_ref.shape
    ffd = gatep_ref.shape[1]
    scale = float(qk) ** -0.5
    me = lax.axis_index("sp")
    tp = lax.axis_index("tp")
    core = lax.rem(me, jnp.int32(C))
    xx = lax.rem(lax.div(me, jnp.int32(C)), jnp.int32(X))
    zz = lax.div(me, jnp.int32(C * X))
    pending = []

    def at_sp(index):
        return {"sp": index, "tp": tp}

    def at_tp(index):
        return {"sp": me, "tp": index}

    def at_zx(z, x, c):
        return z * (X * C) + x * C + c

    def remote(src, dst, ssem, rsem, device):
        return pltpu.make_async_remote_copy(
            src_ref=src, dst_ref=dst, send_sem=ssem, recv_sem=rsem,
            device_id=device, device_id_type=MESH,
        )

    def send(src, dst, ssem, rsem, device):
        copy = remote(src, dst, ssem, rsem, device)
        copy.start()
        pending.append(copy)

    def send_if(condition, src, dst, ssem, rsem, device):
        copy = remote(src, dst, ssem, rsem, device)
        pl.when(condition)(copy.start)
        pending.append((condition, copy))

    def arrived(dst, ssem, rsem, device):
        remote(dst, dst, ssem, rsem, device).wait_recv()

    def ds(start, size, step=None):
        return pl.ds(pl.multiple_of(start, step or size), size)

    sibling = at_sp(me + 1 - 2 * core)

    units = lax.rem(xx + tp, jnp.int32(T))

    def holder(x):
        return {"sp": at_zx(zz, x, core), "tp": mod(tp - x, T)}

    def source(x):
        return {"sp": at_zx(zz, x, core), "tp": units}

    barrier = pltpu.get_barrier_semaphore()

    def greet(p, carry):
        pl.semaphore_signal(
            barrier, 1, device_id=at_sp(mod(me + p, NSP)), device_id_type=MESH
        )
        return carry

    lax.fori_loop(1, NSP, greet, 0)
    for k in range(1, T):
        pl.semaphore_signal(barrier, 1, device_id=at_tp(mod(tp + k, T)), device_id_type=MESH)
    for k in range(X):

        @pl.when(xx + k > 0)
        def _(k=k):
            pl.semaphore_signal(barrier, 1, device_id=source(k), device_id_type=MESH)

    loads = [
        pltpu.make_async_copy(src, dst, loaded.at[i])
        for i, (src, dst) in enumerate((
            (ig_in, ig_ref), (fg_in, fg_ref), (k_in, k_ref), (v_in, v_ref), (q_in, q_ref),
            (og_in, og_ref), (res_in, res_ref), (mixg_in, mixg_ref), (preg_in, preg_ref),
            (postg_in, postg_ref), (gk_in, gk_own), (vk_in, vk_own),
        ))
    ]
    shard = gatep_ref.shape[0]
    local = [
        pltpu.make_async_copy(gatep_ref, ushard.at[:, pl.ds(0, ffd)], loc.at[0]),
        pltpu.make_async_copy(valuep_ref, ushard.at[:, pl.ds(ffd, ffd)], loc.at[1]),
        pltpu.make_async_copy(downp_ref, dshard, loc.at[2]),
        pltpu.make_async_copy(outp_ref, wo, loc.at[3]),
    ]
    for copy in loads + local:
        copy.start()

    steps = rows // ROW_STEP
    lane = lax.broadcasted_iota(jnp.int32, (ROW_STEP, rows), 1)
    line = lax.broadcasted_iota(jnp.int32, (ROW_STEP, rows), 0)
    loads[0].wait()
    loads[1].wait()
    li_row = softcap(ig_ref[...])
    lf_row = log_sigmoid(softcap(fg_ref[...]))

    def sums(b, run_row):
        here = line + b * ROW_STEP
        run_col = jnp.sum(jnp.where(lane <= here, lf_row, 0.0), axis=1, keepdims=True)
        runc[ds(b * ROW_STEP, ROW_STEP), :] = run_col
        return run_row + jnp.sum(jnp.where(lane == here, run_col, 0.0), axis=0, keepdims=True)

    run_row = lax.fori_loop(0, steps, sums, jnp.zeros((1, rows), f32))
    total = run_row[:, rows - 1 : rows]
    lead = total - run_row + li_row
    lead_max = jnp.max(lead, axis=1, keepdims=True)
    lead_weights = jnp.exp(lead - lead_max)
    loads[2].wait()
    loads[3].wait()

    def weigh(b, normer):
        here = line + b * ROW_STEP
        at = ds(b * ROW_STEP, ROW_STEP)
        column = jnp.sum(jnp.where(lane == here, lead_weights, 0.0), axis=1, keepdims=True)
        weighted = k_ref[at, :].astype(f32) * column
        kwb[at, :] = weighted.astype(bf16)
        return normer + jnp.sum(weighted, axis=0, keepdims=True)

    normer = lax.fori_loop(0, steps, weigh, jnp.zeros((1, qk), f32))
    nq = qk // LANES
    for r in range(nq):
        st_src[r : r + 1, :] = normer[:, r * LANES : (r + 1) * LANES]
    for r in range(nq, 4):
        st_src[r : r + 1, :] = jnp.broadcast_to(total if r == nq else lead_max, (1, LANES))
    R = msend.shape[1]
    nc = hv // LANES
    for r in range(nq):
        part = matmul(kwb[:, r * LANES : (r + 1) * LANES], v_ref[...], 0, 0)
        for rr in range(LANES // R):
            for c in range(nc):
                msend[(r * (LANES // R) + rr) * nc + c] = part[
                    rr * R : (rr + 1) * R, c * LANES : (c + 1) * LANES
                ].astype(bf16)

    with jax.named_scope("barrier"):
        pl.semaphore_wait(barrier, NSP - 1 + T - 1 + X - 1 + jnp.minimum(xx, 1))

    mrecv[me] = msend[me]
    st_recv[me] = st_src[...]

    def scatter(p, carry):
        dst = mod(me + p, NSP)
        remote(msend.at[dst], mrecv.at[me], p1.at[0], p1.at[1], at_sp(dst)).start()
        remote(st_src, st_recv.at[me], p1.at[2], p1.at[3], at_sp(dst)).start()
        return carry

    with jax.named_scope("scatter"):
        lax.fori_loop(1, NSP, scatter, 0)

    left, right, across = mod(tp - 1, T), mod(tp + 1, T), mod(tp + 2, T)
    along_y = (tp, left, right, across, at_tp)

    def ring_start(buf, base, half, sems, ring):
        me_r, left_r, right_r, across_r, at = ring
        top, bottom = buf.at[ds(base(me_r), half, 16)], buf.at[ds(base(me_r) + half, half, 16)]
        for k, piece, device in ((0, top, right_r), (1, bottom, left_r), (2, bottom, right_r), (3, top, left_r)):
            send(piece, piece, sems.at[0, k], sems.at[1, k], at(device))

    def ring_piece(buf, base, half, ring, k):
        me_r, left_r, right_r, across_r, at = ring
        block, low = (
            (left_r, 0), (right_r, 1), (left_r, 1), (right_r, 0), (across_r, 0), (across_r, 1)
        )[k]
        return buf.at[ds(base(block) + low * half, half, 16)]

    def ring_wait(buf, base, half, sems, ring, k):
        piece = ring_piece(buf, base, half, ring, k)
        arrived(piece, sems.at[0, k], sems.at[1, k], ring[4](ring[1]))
        if k < 2:
            to = ring[4]((ring[2], ring[1])[k])
            send(piece, piece, sems.at[0, k + 4], sems.at[1, k + 4], to)
        return piece

    for copy in local:
        copy.wait()
    for copy in loads[4:]:
        copy.wait()

    def rows_of(index):
        return ds(index * shard, shard)

    weights = ((ushard, wu), (dshard, wd))
    for w, (src, dst) in enumerate(weights):
        for k in range(X):
            send_if(
                xx + k > 0, src, dst.at[rows_of(me)], xs.at[0, k, w], xs.at[1, xx, w], holder(k)
            )

    @pl.when(xx == 0)
    def _():
        for src, dst in weights:
            dst[rows_of(me), :] = src[...]

    for i, (src, dst) in enumerate(((gk_own, gk_ref), (vk_own, vk_ref))):
        send_if(xx > 0, src, dst, taps.at[0, i], taps.at[1, i], at_tp(mod(tp - xx, T)))

    @pl.when(xx == 0)
    def _():
        gk_ref[...] = gk_own[...]
        vk_ref[...] = vk_own[...]

    def inside(b, carry):
        at = ds(b * ROW_STEP, ROW_STEP)
        here = line + b * ROW_STEP
        logs = jnp.where(lane <= here, runc[at, :] - run_row + li_row, far_below)
        top = jnp.max(logs, axis=1, keepdims=True)
        scores = matmul(q_ref[at, :], k_ref[...], 1, 1) * (jnp.exp(logs - top) * scale)
        m1[at, :] = top
        d1[at, :] = jnp.sum(scores, axis=1, keepdims=True)
        a1[at, :] = matmul(scores.astype(bf16), v_ref[...])
        return carry

    with jax.named_scope("inside"):
        lax.fori_loop(0, steps, inside, 0)

    def shards(w):
        for k in range(X):
            piece = weights[w][1].at[rows_of(at_zx(zz, k, core))]

            @pl.when(xx + k > 0)
            def _():
                arrived(piece, xs.at[0, k, w], xs.at[1, k, w], source(k))

            send(piece, piece, xd.at[0, k, w], xd.at[1, k, w], sibling)

    def shard_twins(w):
        for k in range(X):
            piece = weights[w][1].at[rows_of(at_zx(zz, k, 1 - core))]
            arrived(piece, xd.at[0, k, w], xd.at[1, k, w], sibling)

    with jax.named_scope("ushards"):
        shards(0)

    def all_but_one(buf):
        return buf.at[pl.ds(0, NSP - 1)]

    def bulk(buf, sems, s):
        remote(all_but_one(buf), all_but_one(buf), sems.at[s], sems.at[s + 1], at_sp(me)).wait()

    with jax.named_scope("p1wait"):
        bulk(mrecv, p1, 0)
        bulk(st_recv, p1, 2)

    def advance(i, state):
        highest, memory, norm = state
        for u in range(8):
            d = i * 8 + u
            ssend[d] = memory.astype(bf16)
            nin[d, 0:nq, :] = norm
            nin[d, nq : nq + 1, :] = highest
            following = st_recv[d]
            decayed = highest + following[nq : nq + 1, :]
            lead_d = following[nq + 1 : nq + 2, :]
            highest = jnp.maximum(decayed, lead_d)
            before = jnp.exp(decayed - highest)
            after = jnp.exp(lead_d - highest)
            memory = before * memory + after * mrecv[d].astype(f32)
            norm = before * norm + after * following[0:nq, :]
        return highest, memory, norm

    lax.fori_loop(
        0, NSP // 8, advance,
        (jnp.full((1, LANES), far_below, f32), jnp.zeros((R, LANES), f32), jnp.zeros((nq, LANES), f32)),
    )
    srecv[me] = ssend[me]

    def give_back(p, carry):
        dst = mod(me + p, NSP)
        remote(ssend.at[dst], srecv.at[me], p2.at[0], p2.at[1], at_sp(dst)).start()
        return carry

    with jax.named_scope("giveback"):
        lax.fori_loop(1, NSP, give_back, 0)

    slab = shard * X * C
    part_rows = slab // C
    half_rows = part_rows // 2
    ups = (at_zx(mod(zz + 1, Z), xx, core), at_zx(mod(zz - 1, Z), xx, core))

    def z_piece(w, direction, s, h, c):
        z = mod(zz - s if direction == 0 else zz + s, Z)
        return weights[w][1].at[ds(z * slab + c * part_rows + h * half_rows, half_rows)]

    def z_has(direction, s, h):
        return s < Z // 2 or (s == Z // 2 and h == direction)

    def z_send(w, direction, s, h):
        if z_has(direction, s, h):
            piece = z_piece(w, direction, s - 1, h, core)
            i = (s - 1) * 2 + h
            send(
                piece, piece, zs.at[0, w, direction, i], zs.at[1, w, direction, i],
                at_sp(ups[direction]),
            )

    def z_start(w):
        for h in range(2):
            for direction in range(2):
                z_send(w, direction, 1, h)

    def z_step(w, s, h):
        with jax.named_scope(("uring", "dring")[w] + str(s) + str(h)):
            for direction in range(2):
                if z_has(direction, s, h):
                    piece = z_piece(w, direction, s, h, core)
                    i = (s - 1) * 2 + h
                    arrived(
                        piece, zs.at[0, w, direction, i], zs.at[1, w, direction, i],
                        at_sp(ups[direction]),
                    )
                    z_send(w, direction, s + 1, h)
                    send(piece, piece, zd.at[0, w, direction, i], zd.at[1, w, direction, i], sibling)

    def z_twin(w):
        with jax.named_scope(("utwin", "dtwin")[w]):
            for s in range(1, Z // 2 + 1):
                for h in range(2):
                    for direction in range(2):
                        if z_has(direction, s, h):
                            piece = z_piece(w, direction, s, h, 1 - core)
                            i = (s - 1) * 2 + h
                            arrived(
                                piece, zd.at[0, w, direction, i], zd.at[1, w, direction, i], sibling
                            )

    u_events = [(0, s, h) for s in range(1, Z // 2 + 1) for h in range(2)]
    d_events = [(1, s, h) for s in range(1, Z // 2 + 1) for h in range(2)]

    def z_next(events):
        if events:
            z_step(*events.pop(0))

    with jax.named_scope("ushtwins"):
        shard_twins(0)
    z_start(0)
    z_next(u_events)

    with jax.named_scope("p2wait"):
        bulk(srecv, p2, 0)
    for j in range(NSP):
        r, c = divmod(j, nc)
        m_in[r * R : (r + 1) * R, c * LANES : (c + 1) * LANES] = srecv[j]
    stats = nin[me]
    normer_in = jnp.concatenate([stats[r : r + 1, :] for r in range(nq)], axis=1)
    stab = stats[nq : nq + 1, 0:1]

    def finish(b, carry):
        at = ds(b * ROW_STEP, ROW_STEP)
        queries = q_ref[at, :]
        carried = runc[at, :] + stab
        top = m1[at, :]
        row_max = jnp.maximum(carried, top)
        inner = jnp.exp(top - row_max)
        outer = jnp.exp(carried - row_max) * scale
        reach = jnp.sum(queries.astype(f32) * normer_in, axis=1, keepdims=True)
        denominator = inner * d1[at, :] + outer * reach
        floor = jnp.maximum(jnp.abs(denominator), jnp.exp(-row_max))
        numerator = inner * a1[at, :] + outer * matmul(queries, m_in[...])
        gate = 1.0 / (1.0 + jnp.exp(-og_ref[at, :].astype(f32)))
        gated[at, :] = (numerator / floor * gate).astype(bf16)
        return carry

    with jax.named_scope("finish"):
        lax.fori_loop(0, steps, finish, 0)

    half = own // 2
    top, bottom = pl.ds(0, half), pl.ds(half, half)

    class Sums:
        def __init__(self, piece, ring, sems, from_left, from_right, relay_top, relay_bot):
            self.piece, self.ring, self.sems = piece, ring, sems
            self.from_left, self.from_right = from_left, from_right
            self.relays = (relay_top, relay_bot)

        def send(self, src, dst, k, side):
            to = self.ring[4](self.ring[side])
            send(src, dst, self.sems.at[0, k], self.sems.at[1, k], to)

        def wait(self, dst, k):
            arrived(dst, self.sems.at[0, k], self.sems.at[1, k], self.ring[4](self.ring[1]))

        def far(self):
            self.send(self.piece(3, 0, half)[0], self.relays[0], 2, 2)
            self.send(self.piece(3, 1, half)[0], self.relays[1], 3, 1)

        def near(self):
            self.send(self.piece(2, 1, half)[0], self.from_left.at[bottom], 0, 2)
            self.send(self.piece(1, 0, half)[0], self.from_right.at[top], 1, 1)

        def relay(self):
            for k, relay, side, low, dst in (
                (2, self.relays[0], 2, 0, self.from_left.at[top]),
                (3, self.relays[1], 1, 1, self.from_right.at[bottom]),
            ):
                with jax.named_scope("relay"):
                    self.wait(relay, k)
                own_piece = self.piece(side, low, half)[0]

                def merge(b, carry, relay=relay, own_piece=own_piece):
                    at = ds(b * NORM_STEP, NORM_STEP)
                    relay[at, :] = (relay[at, :].astype(f32) + own_piece[at, :].astype(f32)).astype(bf16)
                    return carry

                lax.fori_loop(0, half // NORM_STEP, merge, 0)
                self.send(relay, dst, k + 2, side)

        def finish(self):
            with jax.named_scope("sumwait"):
                self.wait(self.from_left.at[bottom], 0)
                self.wait(self.from_right.at[top], 1)
                self.wait(self.from_left.at[top], 4)
                self.wait(self.from_right.at[bottom], 5)

        def total(self, b):
            at = ds(b * NORM_STEP, NORM_STEP)
            mine = self.piece(0, 0, own)[0]
            summed = (
                mine[at, :].astype(f32)
                + self.from_left[at, :].astype(f32)
                + self.from_right[at, :].astype(f32)
            )
            return summed.astype(bf16).astype(f32)

    def mix_piece(side, low, size):
        return (mix_part.at[ds(along_y[side] * own + low * half, size, half)],)

    mixes = Sums(mix_piece, along_y, mss, mix_left, mix_right, mix_top, mix_bot)

    def project(n, carry):
        at = ds(n * TILE, TILE)
        mix_part[:, at] = matmul(gated[...], wo[:, at]).astype(bf16)
        return carry

    with jax.named_scope("project"):
        lax.fori_loop(0, D // TILE, project, 0)
    mixes.far()
    mixes.near()
    z_next(u_events)
    z_next(u_events)
    mixes.relay()
    z_next(u_events)
    with jax.named_scope("dshards"):
        shards(1)
    z_next(u_events)
    with jax.named_scope("dshtwins"):
        shard_twins(1)
    z_start(1)
    mixes.finish()
    z_next(u_events)

    def at_ring(index):
        return {
            "sp": me + core * (at_zx(zz, index, core) - me),
            "tp": index + core * (tp - index),
        }

    spot = tp + core * (xx - tp)
    fl, fr, fo = mod(spot - 1, T), mod(spot + 1, T), mod(spot + 2, T)
    ring = (spot, fl, fr, fo, at_ring)
    block_rows = own + HALO

    def block_base(block):
        return block * block_rows + HALO

    def join(b, carry):
        at = ds(b * NORM_STEP, NORM_STEP)
        values = mixes.total(b)
        joined = (res_ref[at, :].astype(f32) + normalize(values, mixg_ref[...])).astype(bf16)
        stream[at, :] = joined
        rows_all[ds(block_base(spot) + b * NORM_STEP, NORM_STEP), :] = normalize(
            joined.astype(f32), preg_ref[...]
        ).astype(bf16)
        return carry

    with jax.named_scope("join"):
        lax.fori_loop(0, own // NORM_STEP, join, 0)

    ring_start(rows_all, block_base, half, ags, ring)

    place = me * T + tp
    after = place + 1
    is_last = after == NSP * T
    nsp = lax.rem(lax.div(after, jnp.int32(T)), jnp.int32(NSP))
    ntp = lax.rem(after, jnp.int32(T))
    ncore = lax.rem(nsp, jnp.int32(C))
    nx = lax.rem(lax.div(nsp, jnp.int32(C)), jnp.int32(X))
    nz = lax.div(nsp, jnp.int32(C * X))
    slot = ntp + ncore * (nx - ntp)
    tail = rows_all.at[ds(block_base(spot) + own - HALO, HALO, 16)]
    tail_to = rows_all.at[ds(slot * block_rows, HALO, 16)]
    for k in range(T):
        to_sp = nsp + ncore * (at_zx(nz, k, ncore) - nsp)
        to_tp = k + ncore * (ntp - k)
        to_self = to_sp * T + to_tp == place
        go = jnp.logical_not(jnp.logical_or(is_last, to_self))
        send_if(go, tail, tail_to, halo.at[0, k], halo.at[1, slot], {"sp": to_sp, "tp": to_tp})

        @pl.when(jnp.logical_and(to_self, jnp.logical_not(is_last)))
        def _():
            rows_all[ds(slot * block_rows, HALO, 16), :] = rows_all[
                ds(block_base(spot) + own - HALO, HALO, 16), :
            ]

    def halo_wait(block):
        device = at_ring(block)
        ahead = device["sp"] * T + device["tp"] - 1
        here = rows_all.at[ds(block * block_rows, HALO, 16)]

        @pl.when(ahead < 0)
        def _():
            rows_all[ds(block * block_rows, HALO, 16), :] = jnp.zeros((HALO, D), bf16)

        @pl.when(jnp.logical_and(ahead >= 0, ahead != place))
        def _():
            arrived(here, halo.at[0, 0], halo.at[1, block], device)

    def ag_wait(k):
        with jax.named_scope("ag" + str(k)):
            ring_wait(rows_all, block_base, half, ags, ring, k)

    while u_events:
        z_next(u_events)
    z_next(d_events)
    ag_wait(0)
    ag_wait(1)

    @pl.when(xx > 0)
    def _():
        for i, dst in enumerate((gk_ref, vk_ref)):
            arrived(dst, taps.at[0, i], taps.at[1, i], at_tp(mod(tp + xx, T)))

    z_twin(0)

    def mix(block, place_in):
        halo_wait(block)
        lines = ds(block * block_rows, block_rows, 16)

        def raise_tile(n, carry):
            at = ds(n * TILE, TILE)
            upb[:, at] = matmul(rows_all[lines, :], wu[:, at]).astype(bf16).astype(f32)
            return carry

        with jax.named_scope("raise"):
            lax.fori_loop(0, 2 * ffd // TILE, raise_tile, 0)

        def convolve(b, carry):
            window = ds(b * CONV_STEP + HALO - 8, CONV_STEP + 8, 8)
            at = ds(b * CONV_STEP + place_in * own, CONV_STEP)
            for c in range(0, ffd, TILE):
                both = []
                for taps_ref, first in ((gk_ref, 0), (vk_ref, ffd)):
                    block_values = upb[window, first + c : first + c + TILE]
                    summed = 0.0
                    for j in range(CONV):
                        low = 8 - CONV + 1 + j
                        summed = summed + taps_ref[j : j + 1, c : c + TILE] * block_values[low : low + CONV_STEP]
                    both.append(summed)
                hidden[at, c : c + TILE] = (both[0] / (1.0 + jnp.exp(-both[0])) * both[1]).astype(bf16)
            return carry

        with jax.named_scope("conv"):
            lax.fori_loop(0, own // CONV_STEP, convolve, 0)

    order = (3, 2, 1, 0)

    def lower(first, last):
        lines = pl.ds(first * own, (last - first) * own)

        def lower_tile(n, carry):
            at = ds(n * TILE, TILE)
            ffn_part[lines, at] = matmul(hidden[lines, :], wd[at, :], 1, 1).astype(bf16)
            return carry

        with jax.named_scope("lower"):
            lax.fori_loop(0, D // TILE, lower_tile, 0)

    def ffn_piece(side, low, size):
        return (ffn_part.at[pl.ds(order.index(side) * own + low * half, size)],)

    ffns = Sums(ffn_piece, ring, rss, ffn_left, ffn_right, ffn_top, ffn_bot)
    mix(spot, 3)
    z_next(d_events)
    ag_wait(2)
    mix(fl, 2)
    z_next(d_events)
    ag_wait(3)
    mix(fr, 1)
    z_next(d_events)
    ag_wait(4)
    ag_wait(5)
    mix(fo, 0)
    while d_events:
        z_next(d_events)
    z_twin(1)
    lower(0, 1)
    ffns.far()
    lower(1, T)
    ffns.near()
    ffns.relay()
    ffns.finish()

    def close(b, carry):
        at = ds(b * NORM_STEP, NORM_STEP)
        values = ffns.total(b)
        out_ref[at, :] = (
            stream[at, :].astype(f32) + normalize(values, postg_ref[...])
        ).astype(bf16)
        return carry

    with jax.named_scope("close"):
        lax.fori_loop(0, own // NORM_STEP, close, 0)

    for copy in pending:
        if isinstance(copy, tuple):
            pl.when(copy[0])(copy[1].wait_send)
        else:
            copy.wait_send()


def body(
    shape,
    query_rows, key_rows, value_rows, out_gate_pre, input_gate_pre, forget_gate_pre, residual,
    out_proj, mix_gain, pre_gain, gate_proj, value_proj, gate_kernel, value_kernel, down_proj,
    post_gain,
):
    Z, X, C, T = shape
    NSP = Z * X * C
    rows, qk = query_rows.shape
    hv = value_rows.shape[1]
    own, D = residual.shape
    ffd = gate_proj.shape[1]
    R = qk * hv // LANES // NSP
    dma = pltpu.SemaphoreType.DMA
    vm = pltpu.VMEM
    inner = pl.BlockSpec(memory_space=pltpu.VMEM)
    outer = pl.BlockSpec(memory_space=pl.ANY)
    return pl.pallas_call(
        functools.partial(kernel, Z, X, C, T),
        out_shape=jax.ShapeDtypeStruct((own, D), bf16),
        in_specs=[outer] * 16,
        out_specs=inner,
        scratch_shapes=[
            vm((rows, qk), bf16),
            vm((rows, qk), bf16),
            vm((rows, hv), bf16),
            vm((rows, hv), bf16),
            vm((1, rows), f32),
            vm((1, rows), f32),
            vm((own, D), bf16),
            vm((1, D), f32),
            vm((1, D), f32),
            vm((1, D), f32),
            vm((CONV, ffd), f32),
            vm((CONV, ffd), f32),
            vm((NSP, R, LANES), bf16),
            vm((NSP, R, LANES), bf16),
            vm((4, LANES), f32),
            vm((NSP, 4, LANES), f32),
            vm((NSP, R, LANES), bf16),
            vm((NSP, R, LANES), bf16),
            vm((NSP, 4, LANES), f32),
            vm((qk, hv), bf16),
            vm((rows, qk), bf16),
            vm((rows, 1), f32),
            vm((rows, hv), f32),
            vm((rows, 1), f32),
            vm((rows, 1), f32),
            vm((rows, hv), bf16),
            vm((hv, D), bf16),
            vm((D // NSP, 2 * ffd), bf16),
            vm((D, 2 * ffd), bf16),
            vm((D // NSP, ffd), bf16),
            vm((D, ffd), bf16),
            vm((CONV, ffd), f32),
            vm((CONV, ffd), f32),
            vm((T * (own + HALO), D), bf16),
            vm((own, D), bf16),
            vm((own + HALO, 2 * ffd), f32),
            vm((rows, ffd), bf16),
        ]
        + 2 * [
            vm((rows, D), bf16),
            vm((own, D), bf16),
            vm((own, D), bf16),
            vm((own // 2, D), bf16),
            vm((own // 2, D), bf16),
        ]
        + [
            dma((4,)),
            dma((12,)),
            dma((4,)),
            dma((2,)),
            dma((2, X, 2)),
            dma((2, X, 2)),
            dma((2, 2, 2, Z)),
            dma((2, 2, 2, Z)),
            dma((2, 2)),
            dma((2, 6)),
            dma((2, 6)),
            dma((2, 6)),
            dma((2, T)),
        ],
        compiler_params=pltpu.CompilerParams(
            collective_id=0, has_side_effects=True, vmem_limit_bytes=60 * 1024 * 1024
        ),
        name="cell_and_mixer",
    )(
        query_rows, key_rows, value_rows, out_gate_pre, input_gate_pre, forget_gate_pre, residual,
        mix_gain.reshape(1, D), pre_gain.reshape(1, D), post_gain.reshape(1, D),
        gate_kernel, value_kernel, out_proj, gate_proj, value_proj, down_proj,
    )


def solution(mesh):
    shape = (*SHAPES[mesh.shape["sp"]], mesh.shape["tp"])
    placed = (
        P("sp", "tp"),
        P("sp", "tp"),
        P("sp", "tp"),
        P("sp", "tp"),
        P("tp", "sp"),
        P("tp", "sp"),
        P(("sp", "tp"), None),
        P("tp", None),
        P(),
        P(),
        P("sp", "tp"),
        P("sp", "tp"),
        P(None, "tp"),
        P(None, "tp"),
        P("sp", "tp"),
        P(),
    )
    return jax.shard_map(
        functools.partial(body, shape), mesh=mesh, in_specs=placed,
        out_specs=P(("sp", "tp"), None), check_vma=False,
    )
```

```python
import functools

import jax
import jax.numpy as jnp
from jax import lax
from jax.experimental import pallas as pl
from jax.experimental.pallas import tpu as pltpu
from jax.sharding import PartitionSpec as P

f32 = jnp.float32
bf16 = jnp.bfloat16
MESH = pl.DeviceIdType.MESH

gate_cap = 15.0
epsilon = 1e-06
far_below = -1e30
CONV = 3
LANES = 128
ROW_STEP = 64
NORM_STEP = 16
CONV_STEP = 32
TILE = 256
HALO = 16
SLOT = (0, 3, 1, 2)

SHAPES = {64: (8, 4, 2)}


def softcap(values):
    return gate_cap * jnp.tanh(values * (1.0 / gate_cap))


def log_one_plus(values):
    series = values * (
        1.0 + values * (-1 / 2 + values * (1 / 3 + values * (-1 / 4 + values * (1 / 5))))
    )
    return jnp.where(values < 0.015625, series, jnp.log(1.0 + values))


def log_sigmoid(values):
    return jnp.minimum(values, 0.0) - log_one_plus(jnp.exp(-jnp.abs(values)))


def normalize(values, gains):
    return values * lax.rsqrt(jnp.mean(values * values, axis=-1, keepdims=True) + epsilon) * gains


def matmul(left, right, left_dim=1, right_dim=0):
    return lax.dot_general(
        left, right, (((left_dim,), (right_dim,)), ((), ())), preferred_element_type=f32
    )


def mod(value, size):
    return lax.rem(value + size, jnp.int32(size))


def kernel(
    Z, X, C, T,
    q_in, k_in, v_in, og_in, ig_in, fg_in, res_in, mixg_in, preg_in, postg_in, gk_in, vk_in,
    outp_ref, gatep_ref, valuep_ref, downp_ref,
    out_ref,
    q_ref, k_ref, v_ref, og_ref, ig_ref, fg_ref, res_ref, mixg_ref, preg_ref, postg_ref, gk_own, vk_own,
    msend, sib_m, csend, mrecv, st_src, sib_st, cst, st_recv, ssend, srecv, nin, m_in, kwb, runc, a1, m1, d1,
    gated, wo, ushard, wu, dshard, wd, gk_ref, vk_ref, rows_all, stream, upb, hidden,
    mix_part, mix_left, mix_right, mix_top, mix_bot,
    ffn_part, ffn_left, ffn_right, ffn_top, ffn_bot,
    loc, loaded, pre, p1, p2, post, xs, xd, zs, zd, taps, ags, mss, rss, halo,
):
    NSP = Z * X * C
    rows, qk = q_ref.shape
    hv = v_ref.shape[1]
    own, D = out_ref.shape
    ffd = gatep_ref.shape[1]
    scale = float(qk) ** -0.5
    me = lax.axis_index("sp")
    tp = lax.axis_index("tp")
    core = lax.rem(me, jnp.int32(C))
    xx = lax.rem(lax.div(me, jnp.int32(C)), jnp.int32(X))
    zz = lax.div(me, jnp.int32(C * X))
    pending = []

    def at_sp(index):
        return {"sp": index, "tp": tp}

    def at_tp(index):
        return {"sp": me, "tp": index}

    def at_zx(z, x, c):
        return z * (X * C) + x * C + c

    def remote(src, dst, ssem, rsem, device):
        return pltpu.make_async_remote_copy(
            src_ref=src, dst_ref=dst, send_sem=ssem, recv_sem=rsem,
            device_id=device, device_id_type=MESH,
        )

    def send(src, dst, ssem, rsem, device):
        copy = remote(src, dst, ssem, rsem, device)
        copy.start()
        pending.append(copy)

    def send_if(condition, src, dst, ssem, rsem, device):
        copy = remote(src, dst, ssem, rsem, device)
        pl.when(condition)(copy.start)
        pending.append((condition, copy))

    def arrived(dst, ssem, rsem, device):
        remote(dst, dst, ssem, rsem, device).wait_recv()

    def ds(start, size, step=None):
        return pl.ds(pl.multiple_of(start, step or size), size)

    sibling = at_sp(me + 1 - 2 * core)

    units = lax.rem(xx + tp, jnp.int32(T))

    def holder(x):
        return {"sp": at_zx(zz, x, core), "tp": mod(tp - x, T)}

    def source(x):
        return {"sp": at_zx(zz, x, core), "tp": units}

    barrier = pltpu.get_barrier_semaphore()

    chips = NSP // C
    chip = lax.div(me, jnp.int32(C))

    def at_chip(index):
        return at_sp(index * C + core)

    def greet(p, carry):
        pl.semaphore_signal(
            barrier, 1, device_id=at_chip(mod(chip + p, chips)), device_id_type=MESH
        )
        return carry

    lax.fori_loop(1, chips, greet, 0)
    pl.semaphore_signal(barrier, 1, device_id=sibling, device_id_type=MESH)
    for k in range(1, T):
        pl.semaphore_signal(barrier, 1, device_id=at_tp(mod(tp + k, T)), device_id_type=MESH)
    for k in range(X):

        @pl.when(xx + k > 0)
        def _(k=k):
            pl.semaphore_signal(barrier, 1, device_id=source(k), device_id_type=MESH)

    loads = [
        pltpu.make_async_copy(src, dst, loaded.at[i])
        for i, (src, dst) in enumerate((
            (ig_in, ig_ref), (fg_in, fg_ref), (k_in, k_ref), (v_in, v_ref), (q_in, q_ref),
            (og_in, og_ref), (res_in, res_ref), (mixg_in, mixg_ref), (preg_in, preg_ref),
            (postg_in, postg_ref), (gk_in, gk_own), (vk_in, vk_own),
        ))
    ]
    shard = gatep_ref.shape[0]
    local = [
        pltpu.make_async_copy(gatep_ref, ushard.at[:, pl.ds(0, ffd)], loc.at[0]),
        pltpu.make_async_copy(valuep_ref, ushard.at[:, pl.ds(ffd, ffd)], loc.at[1]),
        pltpu.make_async_copy(downp_ref, dshard, loc.at[2]),
        pltpu.make_async_copy(outp_ref, wo, loc.at[3]),
    ]
    for copy in loads + local:
        copy.start()

    steps = rows // ROW_STEP
    lane = lax.broadcasted_iota(jnp.int32, (ROW_STEP, rows), 1)
    line = lax.broadcasted_iota(jnp.int32, (ROW_STEP, rows), 0)
    loads[0].wait()
    loads[1].wait()
    li_row = softcap(ig_ref[...])
    lf_row = log_sigmoid(softcap(fg_ref[...]))

    def sums(b, run_row):
        here = line + b * ROW_STEP
        run_col = jnp.sum(jnp.where(lane <= here, lf_row, 0.0), axis=1, keepdims=True)
        runc[ds(b * ROW_STEP, ROW_STEP), :] = run_col
        return run_row + jnp.sum(jnp.where(lane == here, run_col, 0.0), axis=0, keepdims=True)

    run_row = lax.fori_loop(0, steps, sums, jnp.zeros((1, rows), f32))
    total = run_row[:, rows - 1 : rows]
    lead = total - run_row + li_row
    lead_max = jnp.max(lead, axis=1, keepdims=True)
    lead_weights = jnp.exp(lead - lead_max)
    loads[2].wait()
    loads[3].wait()

    def weigh(b, normer):
        here = line + b * ROW_STEP
        at = ds(b * ROW_STEP, ROW_STEP)
        column = jnp.sum(jnp.where(lane == here, lead_weights, 0.0), axis=1, keepdims=True)
        weighted = k_ref[at, :].astype(f32) * column
        kwb[at, :] = weighted.astype(bf16)
        return normer + jnp.sum(weighted, axis=0, keepdims=True)

    normer = lax.fori_loop(0, steps, weigh, jnp.zeros((1, qk), f32))
    nq = qk // LANES
    for r in range(nq):
        st_src[r : r + 1, :] = normer[:, r * LANES : (r + 1) * LANES]
    for r in range(nq, 4):
        st_src[r : r + 1, :] = jnp.broadcast_to(total if r == nq else lead_max, (1, LANES))
    R = msend.shape[1]
    nc = hv // LANES
    for r in range(nq):
        part = matmul(kwb[:, r * LANES : (r + 1) * LANES], v_ref[...], 0, 0)
        for rr in range(LANES // R):
            for c in range(nc):
                j = (r * (LANES // R) + rr) * nc + c
                msend[j % C * chips + j // C] = part[
                    rr * R : (rr + 1) * R, c * LANES : (c + 1) * LANES
                ].astype(bf16)

    with jax.named_scope("barrier"):
        pl.semaphore_wait(barrier, chips + T - 1 + X - 1 + jnp.minimum(xx, 1))

    send(msend, sib_m, pre.at[0, 0], pre.at[1, 0], sibling)
    send(st_src, sib_st, pre.at[0, 1], pre.at[1, 1], sibling)
    is_first = core == 0
    with jax.named_scope("pair"):
        arrived(sib_st, pre.at[0, 1], pre.at[1, 1], sibling)
        arrived(sib_m, pre.at[0, 0], pre.at[1, 0], sibling)
    one = jnp.where(is_first, st_src[...], sib_st[...])
    two = jnp.where(is_first, sib_st[...], st_src[...])

    def meet(highest, following):
        decayed = highest + following[nq : nq + 1, :]
        lead_d = following[nq + 1 : nq + 2, :]
        new = jnp.maximum(decayed, lead_d)
        return new, jnp.exp(decayed - new), jnp.exp(lead_d - new)

    pair_max, weight_one, weight_two = meet(one[nq + 1 : nq + 2, :], two)
    cst[0:nq, :] = weight_one * one[0:nq, :] + weight_two * two[0:nq, :]
    cst[nq : nq + 1, :] = one[nq : nq + 1, :] + two[nq : nq + 1, :]
    cst[nq + 1 : nq + 2, :] = pair_max
    weight_mine = jnp.where(is_first, weight_one, weight_two)
    weight_sib = jnp.where(is_first, weight_two, weight_one)

    def pair(i, carry):
        for u in range(4):
            j = i * 4 + u
            csend[j] = (
                weight_mine * msend[core * chips + j].astype(f32)
                + weight_sib * sib_m[core * chips + j].astype(f32)
            ).astype(bf16)
        return carry

    lax.fori_loop(0, chips // 4, pair, 0)

    mrecv[chip] = csend[chip]
    st_recv[chip] = cst[...]

    def scatter(p, carry):
        dst = mod(chip + p, chips)
        remote(csend.at[dst], mrecv.at[chip], p1.at[0], p1.at[1], at_chip(dst)).start()
        remote(cst, st_recv.at[chip], p1.at[2], p1.at[3], at_chip(dst)).start()
        return carry

    with jax.named_scope("scatter"):
        lax.fori_loop(1, chips, scatter, 0)

    left, right, across = mod(tp - 1, T), mod(tp + 1, T), mod(tp + 2, T)
    along_y = (tp, left, right, across, at_tp)

    def block_piece(side, low, r):
        return rows_all.at[pl.ds(block_base(side) + low * half + r * part, part)]

    def ring_start(r, ks):
        for k in ks:
            low, side = ((0, 2), (1, 1), (1, 2), (0, 1))[k]
            send(
                block_piece(0, low, r), block_piece(3 - side, low, r),
                ags.at[0, r, k], ags.at[1, r, k], at_ring(ring[side]),
            )

    def ag_wait(r, k):
        with jax.named_scope("ag" + str(k)):
            side, low = ((1, 0), (2, 1), (1, 1), (2, 0), (3, 0), (3, 1))[k]
            piece = block_piece(side, low, r)
            arrived(piece, ags.at[0, r, k], ags.at[1, r, k], at_ring(fl))
            if k < 2:
                to = at_ring((fr, fl)[k])
                send(piece, block_piece(3, low, r), ags.at[0, r, k + 4], ags.at[1, r, k + 4], to)

    for copy in local:
        copy.wait()
    for copy in loads[4:]:
        copy.wait()

    def rows_of(index):
        return ds(index * shard, shard)

    weights = ((ushard, wu), (dshard, wd))
    def spread(w):
        src, dst = weights[w]
        for k in range(X):
            send_if(
                xx + k > 0, src, dst.at[rows_of(me)], xs.at[0, k, w], xs.at[1, xx, w], holder(k)
            )

    spread(0)

    @pl.when(xx == 0)
    def _():
        for src, dst in weights:
            dst[rows_of(me), :] = src[...]

    for i, (src, dst) in enumerate(((gk_own, gk_ref), (vk_own, vk_ref))):
        send_if(xx > 0, src, dst, taps.at[0, i], taps.at[1, i], at_tp(mod(tp - xx, T)))

    @pl.when(xx == 0)
    def _():
        gk_ref[...] = gk_own[...]
        vk_ref[...] = vk_own[...]

    def inside(b, carry):
        at = ds(b * ROW_STEP, ROW_STEP)
        here = line + b * ROW_STEP
        logs = jnp.where(lane <= here, runc[at, :] - run_row + li_row, far_below)
        top = jnp.max(logs, axis=1, keepdims=True)
        scores = matmul(q_ref[at, :], k_ref[...], 1, 1) * (jnp.exp(logs - top) * scale)
        m1[at, :] = top
        d1[at, :] = jnp.sum(scores, axis=1, keepdims=True)
        a1[at, :] = matmul(scores.astype(bf16), v_ref[...])
        return carry

    with jax.named_scope("inside"):
        lax.fori_loop(0, steps, inside, 0)

    def shards(w, ks):
        for k in ks:
            piece = weights[w][1].at[rows_of(at_zx(zz, k, core))]

            @pl.when(xx + k > 0)
            def _():
                arrived(piece, xs.at[0, k, w], xs.at[1, k, w], source(k))

            send(piece, piece, xd.at[0, k, w], xd.at[1, k, w], sibling)

    def shard_twins(w):
        for k in range(X):
            piece = weights[w][1].at[rows_of(at_zx(zz, k, 1 - core))]
            arrived(piece, xd.at[0, k, w], xd.at[1, k, w], sibling)

    def all_but_one(buf):
        return buf.at[pl.ds(0, chips - 1)]

    def bulk(buf, sems, s):
        remote(all_but_one(buf), all_but_one(buf), sems.at[s], sems.at[s + 1], at_sp(me)).wait()

    with jax.named_scope("p1wait"):
        bulk(mrecv, p1, 0)
        bulk(st_recv, p1, 2)

    def advance(i, state):
        highest, memory, norm = state
        for u in range(4):
            d = i * 4 + u
            ssend[d] = memory.astype(bf16)
            nin[d, 0:nq, :] = norm
            nin[d, nq : nq + 1, :] = highest
            following = st_recv[d]
            highest, before, after = meet(highest, following)
            memory = before * memory + after * mrecv[d].astype(f32)
            norm = before * norm + after * following[0:nq, :]
        return highest, memory, norm

    lax.fori_loop(
        0, chips // 4, advance,
        (jnp.full((1, LANES), far_below, f32), jnp.zeros((R, LANES), f32), jnp.zeros((nq, LANES), f32)),
    )
    part_of_core = pl.ds(core * chips, chips)
    srecv[core * chips + chip] = ssend[chip]

    def give_back(p, carry):
        dst = mod(chip + p, chips)
        remote(
            ssend.at[dst], srecv.at[core * chips + chip], p2.at[0], p2.at[1], at_chip(dst)
        ).start()
        return carry

    with jax.named_scope("giveback"):
        lax.fori_loop(1, chips, give_back, 0)

    spread(1)
    slab = shard * X * C
    ups = (at_zx(mod(zz + 1, Z), xx, core), at_zx(mod(zz - 1, Z), xx, core))

    def z_piece(w, direction, s, h, c):
        z = mod(zz - s if direction == 0 else zz + s, Z)
        return [
            weights[w][1].at[rows_of(at_zx(z, h * (X // 2) + q, c))] for q in range(X // 2)
        ]

    def z_has(direction, s, h):
        return s < Z // 2 or (s == Z // 2 and h == direction)

    def z_send(w, direction, s, h):
        if z_has(direction, s, h):
            i = (s - 1) * 2 + h
            for q, piece in enumerate(z_piece(w, direction, s - 1, h, core)):
                send(
                    piece, piece, zs.at[0, w, direction, i, q], zs.at[1, w, direction, i, q],
                    at_sp(ups[direction]),
                )

    def z_start(w, h):
        for direction in range(2):
            z_send(w, direction, 1, h)

    def z_step(w, s, h):
        with jax.named_scope(("uring", "dring")[w] + str(s) + str(h)):
            for direction in range(2):
                if z_has(direction, s, h):
                    pieces = z_piece(w, direction, s, h, core)
                    i = (s - 1) * 2 + h
                    for q, piece in enumerate(pieces):
                        arrived(
                            piece, zs.at[0, w, direction, i, q], zs.at[1, w, direction, i, q],
                            at_sp(ups[direction]),
                        )
                    z_send(w, direction, s + 1, h)
                    for q, piece in enumerate(pieces):
                        send(
                            piece, piece, zd.at[0, w, direction, i, q], zd.at[1, w, direction, i, q],
                            sibling,
                        )

    def z_twin(w, distances):
        with jax.named_scope(("utwin", "dtwin")[w]):
            for s in distances:
                for h in range(2):
                    for direction in range(2):
                        if z_has(direction, s, h):
                            i = (s - 1) * 2 + h
                            for q, piece in enumerate(z_piece(w, direction, s, h, 1 - core)):
                                arrived(
                                    piece, zd.at[0, w, direction, i, q],
                                    zd.at[1, w, direction, i, q], sibling,
                                )

    u_events = [(0, s, h) for s in range(1, Z // 2 + 1) for h in range(2)]
    d_events = [(1, s, h) for s in range(1, Z // 2 + 1) for h in range(2)]

    def z_next(events):
        if events:
            z_step(*events.pop(0))

    with jax.named_scope("ushards"):
        shards(0, range(X // 2))
    z_start(0, 0)
    with jax.named_scope("ushards2"):
        shards(0, range(X // 2, X))

    with jax.named_scope("p2wait"):
        bulk(srecv, p2, 0)
    mine = srecv.at[part_of_core]
    send(mine, mine, post.at[0], post.at[1], sibling)
    z_start(0, 1)
    with jax.named_scope("postwait"):
        other = srecv.at[pl.ds((C - 1 - core) * chips, chips)]
        arrived(other, post.at[0], post.at[1], sibling)
    stats = nin[chip]
    ahead_max, ahead_scale, sib_scale = meet(stats[nq : nq + 1, :], sib_st[...])
    ahead_max = jnp.where(is_first, stats[nq : nq + 1, :], ahead_max)
    ahead_scale = jnp.where(is_first, 1.0, ahead_scale)
    sib_scale = jnp.where(is_first, 0.0, sib_scale)
    ahead_normer = ahead_scale * stats[0:nq, :] + sib_scale * sib_st[0:nq, :]
    for j in range(NSP):
        r, c = divmod(j, nc)
        i = j % C * chips + j // C
        m_in[r * R : (r + 1) * R, c * LANES : (c + 1) * LANES] = (
            ahead_scale * srecv[i].astype(f32) + sib_scale * sib_m[i].astype(f32)
        ).astype(bf16)
    normer_in = jnp.concatenate([ahead_normer[r : r + 1, :] for r in range(nq)], axis=1)
    stab = ahead_max[:, 0:1]

    def finish(b, carry):
        at = ds(b * ROW_STEP, ROW_STEP)
        queries = q_ref[at, :]
        carried = runc[at, :] + stab
        top = m1[at, :]
        row_max = jnp.maximum(carried, top)
        inner = jnp.exp(top - row_max)
        outer = jnp.exp(carried - row_max) * scale
        reach = jnp.sum(queries.astype(f32) * normer_in, axis=1, keepdims=True)
        denominator = inner * d1[at, :] + outer * reach
        floor = jnp.maximum(jnp.abs(denominator), jnp.exp(-row_max))
        numerator = inner * a1[at, :] + outer * matmul(queries, m_in[...])
        gate = 1.0 / (1.0 + jnp.exp(-og_ref[at, :].astype(f32)))
        gated[at, :] = (numerator / floor * gate).astype(bf16)
        return carry

    half = own // 2
    part = half // 2

    class Sums:
        def __init__(self, view, base, ring, sems, summed, from_left, from_right, relay_top, relay_bot):
            self.view, self.base, self.ring, self.sems, self.summed = view, base, ring, sems, summed
            self.from_left, self.from_right = from_left, from_right
            self.relays = (relay_top, relay_bot)

        def send(self, src, dst, r, k, side):
            to = self.ring[4](self.ring[side])
            send(src, dst, self.sems.at[0, r, k], self.sems.at[1, r, k], to)

        def wait(self, dst, r, k):
            arrived(dst, self.sems.at[0, r, k], self.sems.at[1, r, k], self.ring[4](self.ring[1]))

        def piece(self, side, low, r):
            return self.view(self.summed, self.base(side) + low * half, r)

        def at_owner(self, buf, low, r):
            return self.view(buf, low * half, r)

        def far(self, r):
            for low in range(2):
                self.send(
                    self.piece(3, low, r), self.view(self.relays[low], 0, r), r, 2 + low, 2 - low
                )

        def near(self, r):
            self.send(self.piece(2, 1, r), self.at_owner(self.from_left, 1, r), r, 0, 2)
            self.send(self.piece(1, 0, r), self.at_owner(self.from_right, 0, r), r, 1, 1)

        def relay(self, r):
            for low, buf in ((0, self.from_left), (1, self.from_right)):
                relay = self.view(self.relays[low], 0, r)
                own_piece = self.piece(2 - low, low, r)
                with jax.named_scope("relay"):
                    self.wait(relay, r, 2 + low)
                if len(relay.shape) == 3:
                    steps_here = relay.shape[0]
                else:
                    steps_here = relay.shape[0] // NORM_STEP

                def merge(b, carry, relay=relay, own_piece=own_piece):
                    at = b if len(relay.shape) == 3 else ds(b * NORM_STEP, NORM_STEP)
                    relay[at] = (relay[at].astype(f32) + own_piece[at].astype(f32)).astype(bf16)
                    return carry

                lax.fori_loop(0, steps_here, merge, 0)
                self.send(relay, self.at_owner(buf, low, r), r, 4 + low, 2 - low)

        def finish(self, r):
            with jax.named_scope("sumwait"):
                self.wait(self.at_owner(self.from_left, 1, r), r, 0)
                self.wait(self.at_owner(self.from_right, 0, r), r, 1)
                self.wait(self.at_owner(self.from_left, 0, r), r, 4)
                self.wait(self.at_owner(self.from_right, 1, r), r, 5)

    def mix_view(ref, row, r):
        return ref.at[ds(row + r * part, part, 16)]

    mixes = Sums(mix_view, lambda side: along_y[side] * own, along_y, mss, mix_part, mix_left, mix_right, mix_top, mix_bot)

    def project(block):
        lines = ds(block * own, own)

        def project_tile(n, carry):
            at = ds(n * TILE, TILE)
            mix_part[lines, at] = matmul(gated[lines, :], wo[:, at]).astype(bf16)
            return carry

        with jax.named_scope("finish"):
            each = own // ROW_STEP
            lax.fori_loop(block * each, (block + 1) * each, finish, 0)
        with jax.named_scope("project"):
            lax.fori_loop(0, D // TILE, project_tile, 0)

    project(across)
    mixes.far(0)
    mixes.far(1)
    z_next(u_events)
    project(right)
    project(left)
    mixes.near(0)
    project(tp)

    def at_ring(index):
        return {
            "sp": me + core * (at_zx(zz, index, core) - me),
            "tp": index + core * (tp - index),
        }

    spot = tp + core * (xx - tp)
    fl, fr, fo = mod(spot - 1, T), mod(spot + 1, T), mod(spot + 2, T)
    ring = (spot, fl, fr, fo, at_ring)
    block_rows = own + HALO

    def block_base(block):
        return SLOT[block] * block_rows + HALO

    def join(r):
        def join_rows(b, carry):
            row = lax.rem(b, jnp.int32(part // NORM_STEP)) * NORM_STEP + r * part
            row = row + lax.div(b, jnp.int32(part // NORM_STEP)) * half
            at = ds(row, NORM_STEP)
            summed = (
                mix_part[ds(tp * own + row, NORM_STEP), :].astype(f32)
                + mix_left[at, :].astype(f32)
                + mix_right[at, :].astype(f32)
            )
            values = summed.astype(bf16).astype(f32)
            joined = (res_ref[at, :].astype(f32) + normalize(values, mixg_ref[...])).astype(bf16)
            stream[at, :] = joined
            rows_all[ds(block_base(0) + row, NORM_STEP), :] = normalize(
                joined.astype(f32), preg_ref[...]
            ).astype(bf16)
            return carry

        with jax.named_scope("join"):
            lax.fori_loop(0, 2 * (part // NORM_STEP), join_rows, 0)

    z_next(u_events)
    mixes.relay(0)
    mixes.near(1)
    z_next(u_events)
    mixes.relay(1)
    z_next(u_events)
    with jax.named_scope("dshards"):
        shards(1, range(X))
    z_next(u_events)
    z_start(1, 0)
    mixes.finish(0)
    join(0)
    ring_start(0, (0, 1, 2, 3))
    z_next(u_events)
    z_start(1, 1)
    mixes.finish(1)
    join(1)
    ring_start(1, (0, 1))

    place = me * T + tp
    after = place + 1
    is_last = after == NSP * T
    nsp = lax.rem(lax.div(after, jnp.int32(T)), jnp.int32(NSP))
    ntp = lax.rem(after, jnp.int32(T))
    ncore = lax.rem(nsp, jnp.int32(C))
    nx = lax.rem(lax.div(nsp, jnp.int32(C)), jnp.int32(X))
    nz = lax.div(nsp, jnp.int32(C * X))
    npos = ntp + ncore * (nx - ntp)
    tail_lines = pl.ds(block_base(0) + own - HALO, HALO)
    for k in range(T):
        to_sp = nsp + ncore * (at_zx(nz, k, ncore) - nsp)
        to_tp = k + ncore * (ntp - k)
        slot = mod(npos - k, T)
        to_lines = ds(slot * block_rows, HALO, 16)
        to_self = to_sp * T + to_tp == place
        go = jnp.logical_not(jnp.logical_or(is_last, to_self))
        send_if(
            go, rows_all.at[tail_lines], rows_all.at[to_lines], halo.at[0, k], halo.at[1, slot],
            {"sp": to_sp, "tp": to_tp},
        )

        @pl.when(jnp.logical_and(to_self, jnp.logical_not(is_last)))
        def _(to_lines=to_lines):
            rows_all[to_lines, :] = rows_all[tail_lines, :]

    ring_start(1, (2, 3))

    def halo_wait(slot):
        device = at_ring(mod(spot + slot, T))
        ahead = device["sp"] * T + device["tp"] - 1
        lines = pl.ds(slot * block_rows, HALO)

        @pl.when(ahead < 0)
        def _():
            rows_all[lines, :] = jnp.zeros((HALO, D), bf16)

        @pl.when(jnp.logical_and(ahead >= 0, ahead != place))
        def _():
            arrived(rows_all.at[lines], halo.at[0, 0], halo.at[1, slot], device)

    ag_wait(0, 0)
    ag_wait(0, 1)
    while u_events:
        z_next(u_events)
    z_next(d_events)
    ag_wait(1, 0)
    ag_wait(1, 1)
    z_next(d_events)

    @pl.when(xx > 0)
    def _():
        for i, dst in enumerate((gk_ref, vk_ref)):
            arrived(dst, taps.at[0, i], taps.at[1, i], at_tp(mod(tp + xx, T)))

    with jax.named_scope("shtwins"):
        shard_twins(0)
        shard_twins(1)
    z_twin(0, range(1, Z // 2 + 1))

    def mix(first, last):
        for slot in range(first, last):
            halo_wait(slot)
        lines = pl.ds(first * block_rows, (last - first) * block_rows)
        within = pl.ds(0, (last - first) * block_rows)

        def raise_tile(n, carry):
            at = ds(n * TILE, TILE)
            upb[within, at] = matmul(rows_all[lines, :], wu[:, at]).astype(bf16).astype(f32)
            return carry

        with jax.named_scope("raise"):
            lax.fori_loop(0, 2 * ffd // TILE, raise_tile, 0)
        z_next(d_events)
        windows = own // CONV_STEP

        def convolve(b, carry):
            block = lax.div(b, jnp.int32(windows))
            row = lax.rem(b, jnp.int32(windows)) * CONV_STEP
            window = ds(block * block_rows + row + HALO - 8, CONV_STEP + 8, 8)
            at = ds((first + block) * own + row, CONV_STEP)
            for c in range(0, ffd, TILE):
                both = []
                for taps_ref, start in ((gk_ref, 0), (vk_ref, ffd)):
                    block_values = upb[window, start + c : start + c + TILE]
                    summed = 0.0
                    for j in range(CONV):
                        low = 8 - CONV + 1 + j
                        summed = summed + taps_ref[j : j + 1, c : c + TILE] * block_values[low : low + CONV_STEP]
                    both.append(summed)
                hidden[at, c : c + TILE] = (both[0] / (1.0 + jnp.exp(-both[0])) * both[1]).astype(bf16)
            return carry

        with jax.named_scope("conv"):
            lax.fori_loop(0, (last - first) * windows, convolve, 0)

    zs_order = [zz]
    for d in range(1, Z // 2):
        zs_order += [mod(zz - d, Z), mod(zz + d, Z)]
    zs_order.append(mod(zz + Z // 2, Z))
    early = max(1, Z - 3)

    def lower(tile):
        at = ds(zs_order[tile] * slab, slab)
        with jax.named_scope("lower"):
            ffn_part[tile] = matmul(hidden[...], wd[at, :], 1, 1).astype(bf16)

    def ffn_view(ref, row, r):
        tiles = pl.ds(0, early) if r == 0 else pl.ds(early, Z - early)
        return ref.at[tiles, ds(row, half), :]

    ffns = Sums(ffn_view, lambda side: SLOT[side] * own, ring, rss, ffn_part, ffn_left, ffn_right, ffn_top, ffn_bot)
    mix(0, 1)
    z_next(d_events)
    for k in (2, 3, 4, 5):
        ag_wait(0, k)
    for k in (2, 3, 4, 5):
        ag_wait(1, k)
    mix(1, T)
    while d_events and d_events[0][1] <= max(0, (early - 1) // 2):
        z_next(d_events)
    for tile in range(early):
        if tile % 2 == 1:
            z_twin(1, ((tile + 1) // 2,))
        lower(tile)
    ffns.far(0)
    ffns.near(0)
    for tile in range(early, Z):
        distance = (tile + 1) // 2
        while d_events and d_events[0][1] <= distance:
            z_next(d_events)
        if tile % 2 == 1:
            z_twin(1, (distance,))
        lower(tile)
    ffns.far(1)
    ffns.relay(0)
    ffns.near(1)
    ffns.relay(1)
    ffns.finish(0)
    ffns.finish(1)

    def close(b, carry):
        at = ds(b * NORM_STEP, NORM_STEP)
        mine = ds(b * NORM_STEP, NORM_STEP)
        values, squares = [], 0.0
        for tile in range(Z):
            summed = (
                ffn_part[tile, mine, :].astype(f32)
                + ffn_left[tile, at, :].astype(f32)
                + ffn_right[tile, at, :].astype(f32)
            )
            values.append(summed.astype(bf16).astype(f32))
            squares = squares + jnp.sum(values[-1] * values[-1], axis=-1, keepdims=True)
        factor = lax.rsqrt(squares * (1.0 / D) + epsilon)
        for tile in range(Z):
            to = ds(zs_order[tile] * slab, slab)
            out_ref[at, to] = (
                stream[at, to].astype(f32) + values[tile] * factor * postg_ref[:, to]
            ).astype(bf16)
        return carry

    with jax.named_scope("close"):
        lax.fori_loop(0, own // NORM_STEP, close, 0)

    for copy in pending:
        if isinstance(copy, tuple):
            pl.when(copy[0])(copy[1].wait_send)
        else:
            copy.wait_send()


def body(
    shape,
    query_rows, key_rows, value_rows, out_gate_pre, input_gate_pre, forget_gate_pre, residual,
    out_proj, mix_gain, pre_gain, gate_proj, value_proj, gate_kernel, value_kernel, down_proj,
    post_gain,
):
    Z, X, C, T = shape
    NSP = Z * X * C
    rows, qk = query_rows.shape
    hv = value_rows.shape[1]
    own, D = residual.shape
    ffd = gate_proj.shape[1]
    R = qk * hv // LANES // NSP
    dma = pltpu.SemaphoreType.DMA
    vm = pltpu.VMEM
    inner = pl.BlockSpec(memory_space=pltpu.VMEM)
    outer = pl.BlockSpec(memory_space=pl.ANY)
    return pl.pallas_call(
        functools.partial(kernel, Z, X, C, T),
        out_shape=jax.ShapeDtypeStruct((own, D), bf16),
        in_specs=[outer] * 16,
        out_specs=inner,
        scratch_shapes=[
            vm((rows, qk), bf16),
            vm((rows, qk), bf16),
            vm((rows, hv), bf16),
            vm((rows, hv), bf16),
            vm((1, rows), f32),
            vm((1, rows), f32),
            vm((own, D), bf16),
            vm((1, D), f32),
            vm((1, D), f32),
            vm((1, D), f32),
            vm((CONV, ffd), f32),
            vm((CONV, ffd), f32),
            vm((NSP, R, LANES), bf16),
            vm((NSP, R, LANES), bf16),
            vm((NSP // C, R, LANES), bf16),
            vm((NSP // C, R, LANES), bf16),
            vm((4, LANES), f32),
            vm((4, LANES), f32),
            vm((4, LANES), f32),
            vm((NSP // C, 4, LANES), f32),
            vm((NSP // C, R, LANES), bf16),
            vm((NSP, R, LANES), bf16),
            vm((NSP // C, 4, LANES), f32),
            vm((qk, hv), bf16),
            vm((rows, qk), bf16),
            vm((rows, 1), f32),
            vm((rows, hv), f32),
            vm((rows, 1), f32),
            vm((rows, 1), f32),
            vm((rows, hv), bf16),
            vm((hv, D), bf16),
            vm((D // NSP, 2 * ffd), bf16),
            vm((D, 2 * ffd), bf16),
            vm((D // NSP, ffd), bf16),
            vm((D, ffd), bf16),
            vm((CONV, ffd), f32),
            vm((CONV, ffd), f32),
            vm((T * (own + HALO), D), bf16),
            vm((own, D), bf16),
            vm(((T - 1) * (own + HALO), 2 * ffd), f32),
            vm((rows, ffd), bf16),
        ]
        + [
            vm((rows, D), bf16),
            vm((own, D), bf16),
            vm((own, D), bf16),
            vm((own // 2, D), bf16),
            vm((own // 2, D), bf16),
            vm((Z, rows, D // Z), bf16),
            vm((Z, own, D // Z), bf16),
            vm((Z, own, D // Z), bf16),
            vm((Z, own // 2, D // Z), bf16),
            vm((Z, own // 2, D // Z), bf16),
        ]
        + [
            dma((4,)),
            dma((12,)),
            dma((2, 2)),
            dma((4,)),
            dma((2,)),
            dma((2,)),
            dma((2, X, 2)),
            dma((2, X, 2)),
            dma((2, 2, 2, Z, X // 2)),
            dma((2, 2, 2, Z, X // 2)),
            dma((2, 2)),
            dma((2, 2, 6)),
            dma((2, 2, 6)),
            dma((2, 2, 6)),
            dma((2, T)),
        ],
        compiler_params=pltpu.CompilerParams(
            collective_id=0, has_side_effects=True, vmem_limit_bytes=60 * 1024 * 1024
        ),
        name="cell_and_mixer",
    )(
        query_rows, key_rows, value_rows, out_gate_pre, input_gate_pre, forget_gate_pre, residual,
        mix_gain.reshape(1, D), pre_gain.reshape(1, D), post_gain.reshape(1, D),
        gate_kernel, value_kernel, out_proj, gate_proj, value_proj, down_proj,
    )


def solution(mesh):
    shape = (*SHAPES[mesh.shape["sp"]], mesh.shape["tp"])
    placed = (
        P("sp", "tp"),
        P("sp", "tp"),
        P("sp", "tp"),
        P("sp", "tp"),
        P("tp", "sp"),
        P("tp", "sp"),
        P(("sp", "tp"), None),
        P("tp", None),
        P(),
        P(),
        P("sp", "tp"),
        P("sp", "tp"),
        P(None, "tp"),
        P(None, "tp"),
        P("sp", "tp"),
        P(),
    )
    return jax.shard_map(
        functools.partial(body, shape), mesh=mesh, in_specs=placed,
        out_specs=P(("sp", "tp"), None), check_vma=False,
    )
```

```python
import functools

import jax
import jax.numpy as jnp
from jax import lax
from jax.experimental import pallas as pl
from jax.experimental.pallas import tpu as pltpu
from jax.sharding import PartitionSpec as P

f32 = jnp.float32
bf16 = jnp.bfloat16
MESH = pl.DeviceIdType.MESH

gate_cap = 15.0
epsilon = 1e-06
far_below = -1e30
CONV = 3
LANES = 128
ROW_STEP = 64
NORM_STEP = 16
CONV_STEP = 32
TILE = 256
HALO = 16
SLOT = (0, 3, 1, 2)

SHAPES = {64: (8, 4, 2)}


def softcap(values):
    return gate_cap * jnp.tanh(values * (1.0 / gate_cap))


def log_one_plus(values):
    series = values * (
        1.0 + values * (-1 / 2 + values * (1 / 3 + values * (-1 / 4 + values * (1 / 5))))
    )
    return jnp.where(values < 0.015625, series, jnp.log(1.0 + values))


def log_sigmoid(values):
    return jnp.minimum(values, 0.0) - log_one_plus(jnp.exp(-jnp.abs(values)))


def normalize(values, gains):
    return values * lax.rsqrt(jnp.mean(values * values, axis=-1, keepdims=True) + epsilon) * gains


def matmul(left, right, left_dim=1, right_dim=0):
    return lax.dot_general(
        left, right, (((left_dim,), (right_dim,)), ((), ())), preferred_element_type=f32
    )


def mod(value, size):
    return lax.rem(value + size, jnp.int32(size))


def kernel(
    Z, X, C, T,
    q_in, k_in, v_in, og_in, ig_in, fg_in, res_in, mixg_in, preg_in, postg_in, gk_in, vk_in,
    outp_ref, gatep_ref, valuep_ref, downp_ref,
    out_ref,
    q_ref, k_ref, v_ref, og_ref, ig_ref, fg_ref, res_ref, mixg_ref, preg_ref, postg_ref, gk_own, vk_own,
    msend, sib_m, csend, mrecv, st_src, sib_st, cst, st_recv, ssend, srecv, nin, m_in, kwb, runc, a1, m1, d1,
    gated, wo, ushard, wu, dshard, wd, gk_ref, vk_ref, rows_all, stream, upb, hidden,
    mix_part, mix_left, mix_right, mix_top, mix_bot,
    ffn_part, ffn_left, ffn_right, ffn_top, ffn_bot,
    loc, loaded, pre, p1, p2, post, xs, xd, zs, zd, taps, ags, mss, rss, halo,
):
    NSP = Z * X * C
    rows, qk = q_ref.shape
    hv = v_ref.shape[1]
    own, D = out_ref.shape
    ffd = gatep_ref.shape[1]
    scale = float(qk) ** -0.5
    me = lax.axis_index("sp")
    tp = lax.axis_index("tp")
    core = lax.rem(me, jnp.int32(C))
    xx = lax.rem(lax.div(me, jnp.int32(C)), jnp.int32(X))
    zz = lax.div(me, jnp.int32(C * X))
    pending = []

    def at_sp(index):
        return {"sp": index, "tp": tp}

    def at_tp(index):
        return {"sp": me, "tp": index}

    def at_zx(z, x, c):
        return z * (X * C) + x * C + c

    def remote(src, dst, ssem, rsem, device):
        return pltpu.make_async_remote_copy(
            src_ref=src, dst_ref=dst, send_sem=ssem, recv_sem=rsem,
            device_id=device, device_id_type=MESH,
        )

    def send(src, dst, ssem, rsem, device):
        copy = remote(src, dst, ssem, rsem, device)
        copy.start()
        pending.append(copy)

    def send_if(condition, src, dst, ssem, rsem, device):
        copy = remote(src, dst, ssem, rsem, device)
        pl.when(condition)(copy.start)
        pending.append((condition, copy))

    def arrived(dst, ssem, rsem, device):
        remote(dst, dst, ssem, rsem, device).wait_recv()

    def ds(start, size, step=None):
        return pl.ds(pl.multiple_of(start, step or size), size)

    sibling = at_sp(me + 1 - 2 * core)

    units = lax.rem(xx + tp, jnp.int32(T))

    def holder(x):
        return {"sp": at_zx(zz, x, core), "tp": mod(tp - x, T)}

    def source(x):
        return {"sp": at_zx(zz, x, core), "tp": units}

    barrier = pltpu.get_barrier_semaphore()

    chips = NSP // C
    chip = lax.div(me, jnp.int32(C))

    def at_chip(index):
        return at_sp(index * C + core)

    def greet(p, carry):
        pl.semaphore_signal(
            barrier, 1, device_id=at_chip(mod(chip + p, chips)), device_id_type=MESH
        )
        return carry

    lax.fori_loop(1, chips, greet, 0)
    pl.semaphore_signal(barrier, 1, device_id=sibling, device_id_type=MESH)
    for k in range(1, T):
        pl.semaphore_signal(barrier, 1, device_id=at_tp(mod(tp + k, T)), device_id_type=MESH)
    for k in range(X):

        @pl.when(xx + k > 0)
        def _(k=k):
            pl.semaphore_signal(barrier, 1, device_id=source(k), device_id_type=MESH)

    loads = [
        pltpu.make_async_copy(src, dst, loaded.at[i])
        for i, (src, dst) in enumerate((
            (ig_in, ig_ref), (fg_in, fg_ref), (k_in, k_ref), (v_in, v_ref), (q_in, q_ref),
            (og_in, og_ref), (res_in, res_ref), (mixg_in, mixg_ref), (preg_in, preg_ref),
            (postg_in, postg_ref), (gk_in, gk_own), (vk_in, vk_own),
        ))
    ]
    shard = gatep_ref.shape[0]
    local = [
        pltpu.make_async_copy(gatep_ref, ushard.at[:, pl.ds(0, ffd)], loc.at[0]),
        pltpu.make_async_copy(valuep_ref, ushard.at[:, pl.ds(ffd, ffd)], loc.at[1]),
        pltpu.make_async_copy(downp_ref, dshard, loc.at[2]),
        pltpu.make_async_copy(outp_ref, wo, loc.at[3]),
    ]
    for copy in loads + local:
        copy.start()

    steps = rows // ROW_STEP
    lane = lax.broadcasted_iota(jnp.int32, (ROW_STEP, rows), 1)
    line = lax.broadcasted_iota(jnp.int32, (ROW_STEP, rows), 0)
    loads[0].wait()
    loads[1].wait()
    li_row = softcap(ig_ref[...])
    lf_row = log_sigmoid(softcap(fg_ref[...]))

    def sums(b, run_row):
        here = line + b * ROW_STEP
        run_col = jnp.sum(jnp.where(lane <= here, lf_row, 0.0), axis=1, keepdims=True)
        runc[ds(b * ROW_STEP, ROW_STEP), :] = run_col
        return run_row + jnp.sum(jnp.where(lane == here, run_col, 0.0), axis=0, keepdims=True)

    run_row = lax.fori_loop(0, steps, sums, jnp.zeros((1, rows), f32), unroll=True)
    total = run_row[:, rows - 1 : rows]
    lead = total - run_row + li_row
    lead_max = jnp.max(lead, axis=1, keepdims=True)
    lead_weights = jnp.exp(lead - lead_max)
    loads[2].wait()
    loads[3].wait()

    def weigh(b, normer):
        here = line + b * ROW_STEP
        at = ds(b * ROW_STEP, ROW_STEP)
        column = jnp.sum(jnp.where(lane == here, lead_weights, 0.0), axis=1, keepdims=True)
        weighted = k_ref[at, :].astype(f32) * column
        kwb[at, :] = weighted.astype(bf16)
        return normer + jnp.sum(weighted, axis=0, keepdims=True)

    normer = lax.fori_loop(0, steps, weigh, jnp.zeros((1, qk), f32), unroll=True)
    nq = qk // LANES
    for r in range(nq):
        st_src[r : r + 1, :] = normer[:, r * LANES : (r + 1) * LANES]
    for r in range(nq, 4):
        st_src[r : r + 1, :] = jnp.broadcast_to(total if r == nq else lead_max, (1, LANES))
    R = msend.shape[1]
    nc = hv // LANES
    for r in range(nq):
        part = matmul(kwb[:, r * LANES : (r + 1) * LANES], v_ref[...], 0, 0)
        for rr in range(LANES // R):
            for c in range(nc):
                j = (r * (LANES // R) + rr) * nc + c
                msend[j % C * chips + j // C] = part[
                    rr * R : (rr + 1) * R, c * LANES : (c + 1) * LANES
                ].astype(bf16)

    with jax.named_scope("barrier"):
        pl.semaphore_wait(barrier, chips + T - 1 + X - 1 + jnp.minimum(xx, 1))

    send(msend, sib_m, pre.at[0, 0], pre.at[1, 0], sibling)
    send(st_src, sib_st, pre.at[0, 1], pre.at[1, 1], sibling)
    is_first = core == 0
    with jax.named_scope("pair"):
        arrived(sib_st, pre.at[0, 1], pre.at[1, 1], sibling)
        arrived(sib_m, pre.at[0, 0], pre.at[1, 0], sibling)
    one = jnp.where(is_first, st_src[...], sib_st[...])
    two = jnp.where(is_first, sib_st[...], st_src[...])

    def meet(highest, following):
        decayed = highest + following[nq : nq + 1, :]
        lead_d = following[nq + 1 : nq + 2, :]
        new = jnp.maximum(decayed, lead_d)
        return new, jnp.exp(decayed - new), jnp.exp(lead_d - new)

    pair_max, weight_one, weight_two = meet(one[nq + 1 : nq + 2, :], two)
    cst[0:nq, :] = weight_one * one[0:nq, :] + weight_two * two[0:nq, :]
    cst[nq : nq + 1, :] = one[nq : nq + 1, :] + two[nq : nq + 1, :]
    cst[nq + 1 : nq + 2, :] = pair_max
    weight_mine = jnp.where(is_first, weight_one, weight_two)
    weight_sib = jnp.where(is_first, weight_two, weight_one)

    def pair(i, carry):
        for u in range(4):
            j = i * 4 + u
            csend[j] = (
                weight_mine * msend[core * chips + j].astype(f32)
                + weight_sib * sib_m[core * chips + j].astype(f32)
            ).astype(bf16)
        return carry

    lax.fori_loop(0, chips // 4, pair, 0)

    mrecv[chip] = csend[chip]
    st_recv[chip] = cst[...]

    def scatter(p, carry):
        dst = mod(chip + p, chips)
        remote(csend.at[dst], mrecv.at[chip], p1.at[0], p1.at[1], at_chip(dst)).start()
        remote(cst, st_recv.at[chip], p1.at[2], p1.at[3], at_chip(dst)).start()
        return carry

    with jax.named_scope("scatter"):
        lax.fori_loop(1, chips, scatter, 0)

    left, right, across = mod(tp - 1, T), mod(tp + 1, T), mod(tp + 2, T)
    along_y = (tp, left, right, across, at_tp)

    def block_piece(side, low, r):
        return rows_all.at[pl.ds(block_base(side) + low * half + r * part, part)]

    def ring_start(r, ks):
        for k in ks:
            low, side = ((0, 2), (1, 1), (1, 2), (0, 1))[k]
            send(
                block_piece(0, low, r), block_piece(3 - side, low, r),
                ags.at[0, r, k], ags.at[1, r, k], at_ring(ring[side]),
            )

    def ag_wait(r, k):
        with jax.named_scope("ag" + str(k)):
            side, low = ((1, 0), (2, 1), (1, 1), (2, 0), (3, 0), (3, 1))[k]
            piece = block_piece(side, low, r)
            arrived(piece, ags.at[0, r, k], ags.at[1, r, k], at_ring(fl))
            if k < 2:
                to = at_ring((fr, fl)[k])
                send(piece, block_piece(3, low, r), ags.at[0, r, k + 4], ags.at[1, r, k + 4], to)

    for copy in local:
        copy.wait()
    for copy in loads[4:]:
        copy.wait()

    def rows_of(index):
        return ds(index * shard, shard)

    weights = ((ushard, wu), (dshard, wd))
    def spread(w):
        src, dst = weights[w]
        for k in range(X):
            send_if(
                xx + k > 0, src, dst.at[rows_of(me)], xs.at[0, k, w], xs.at[1, xx, w], holder(k)
            )

    spread(0)

    @pl.when(xx == 0)
    def _():
        for src, dst in weights:
            dst[rows_of(me), :] = src[...]

    for i, (src, dst) in enumerate(((gk_own, gk_ref), (vk_own, vk_ref))):
        send_if(xx > 0, src, dst, taps.at[0, i], taps.at[1, i], at_tp(mod(tp - xx, T)))

    @pl.when(xx == 0)
    def _():
        gk_ref[...] = gk_own[...]
        vk_ref[...] = vk_own[...]

    def inside(b, carry):
        at = ds(b * ROW_STEP, ROW_STEP)
        here = line + b * ROW_STEP
        logs = jnp.where(lane <= here, runc[at, :] - run_row + li_row, far_below)
        top = jnp.max(logs, axis=1, keepdims=True)
        scores = matmul(q_ref[at, :], k_ref[...], 1, 1) * (jnp.exp(logs - top) * scale)
        m1[at, :] = top
        d1[at, :] = jnp.sum(scores, axis=1, keepdims=True)
        a1[at, :] = matmul(scores.astype(bf16), v_ref[...])
        return carry

    with jax.named_scope("inside"):
        lax.fori_loop(0, steps, inside, 0)

    def shards(w, ks):
        for k in ks:
            piece = weights[w][1].at[rows_of(at_zx(zz, k, core))]

            @pl.when(xx + k > 0)
            def _():
                arrived(piece, xs.at[0, k, w], xs.at[1, k, w], source(k))

            send(piece, piece, xd.at[0, k, w], xd.at[1, k, w], sibling)

    def shard_twins(w):
        for k in range(X):
            piece = weights[w][1].at[rows_of(at_zx(zz, k, 1 - core))]
            arrived(piece, xd.at[0, k, w], xd.at[1, k, w], sibling)

    def all_but_one(buf):
        return buf.at[pl.ds(0, chips - 1)]

    def bulk(buf, sems, s):
        remote(all_but_one(buf), all_but_one(buf), sems.at[s], sems.at[s + 1], at_sp(me)).wait()

    with jax.named_scope("p1wait"):
        bulk(mrecv, p1, 0)
        bulk(st_recv, p1, 2)

    def advance(i, state):
        highest, memory, norm = state
        for u in range(4):
            d = i * 4 + u
            ssend[d] = memory.astype(bf16)
            nin[d, 0:nq, :] = norm
            nin[d, nq : nq + 1, :] = highest
            following = st_recv[d]
            highest, before, after = meet(highest, following)
            memory = before * memory + after * mrecv[d].astype(f32)
            norm = before * norm + after * following[0:nq, :]
        return highest, memory, norm

    lax.fori_loop(
        0, chips // 4, advance,
        (jnp.full((1, LANES), far_below, f32), jnp.zeros((R, LANES), f32), jnp.zeros((nq, LANES), f32)),
    )
    part_of_core = pl.ds(core * chips, chips)
    srecv[core * chips + chip] = ssend[chip]

    def give_back(p, carry):
        dst = mod(chip + p, chips)
        remote(
            ssend.at[dst], srecv.at[core * chips + chip], p2.at[0], p2.at[1], at_chip(dst)
        ).start()
        return carry

    with jax.named_scope("giveback"):
        lax.fori_loop(1, chips, give_back, 0)

    spread(1)
    slab = shard * X * C
    ups = (at_zx(mod(zz + 1, Z), xx, core), at_zx(mod(zz - 1, Z), xx, core))

    def z_piece(w, direction, s, h, c):
        z = mod(zz - s if direction == 0 else zz + s, Z)
        return [
            weights[w][1].at[rows_of(at_zx(z, h * (X // 2) + q, c))] for q in range(X // 2)
        ]

    def z_has(direction, s, h):
        return s < Z // 2 or (s == Z // 2 and h == direction)

    def z_send(w, direction, s, h):
        if z_has(direction, s, h):
            i = (s - 1) * 2 + h
            for q, piece in enumerate(z_piece(w, direction, s - 1, h, core)):
                send(
                    piece, piece, zs.at[0, w, direction, i, q], zs.at[1, w, direction, i, q],
                    at_sp(ups[direction]),
                )

    def z_start(w, h):
        for direction in range(2):
            z_send(w, direction, 1, h)

    def z_step(w, s, h):
        with jax.named_scope(("uring", "dring")[w] + str(s) + str(h)):
            for direction in range(2):
                if z_has(direction, s, h):
                    pieces = z_piece(w, direction, s, h, core)
                    i = (s - 1) * 2 + h
                    for q, piece in enumerate(pieces):
                        arrived(
                            piece, zs.at[0, w, direction, i, q], zs.at[1, w, direction, i, q],
                            at_sp(ups[direction]),
                        )
                    z_send(w, direction, s + 1, h)
                    for q, piece in enumerate(pieces):
                        send(
                            piece, piece, zd.at[0, w, direction, i, q], zd.at[1, w, direction, i, q],
                            sibling,
                        )

    def z_twin(w, distances):
        with jax.named_scope(("utwin", "dtwin")[w]):
            for s in distances:
                for h in range(2):
                    for direction in range(2):
                        if z_has(direction, s, h):
                            i = (s - 1) * 2 + h
                            for q, piece in enumerate(z_piece(w, direction, s, h, 1 - core)):
                                arrived(
                                    piece, zd.at[0, w, direction, i, q],
                                    zd.at[1, w, direction, i, q], sibling,
                                )

    u_events = [(0, s, h) for s in range(1, Z // 2 + 1) for h in range(2)]
    d_events = [(1, s, h) for s in range(1, Z // 2 + 1) for h in range(2)]

    def z_next(events):
        if events:
            z_step(*events.pop(0))

    with jax.named_scope("ushards"):
        shards(0, range(X // 2))
    z_start(0, 0)
    with jax.named_scope("ushards2"):
        shards(0, range(X // 2, X))

    with jax.named_scope("p2wait"):
        bulk(srecv, p2, 0)
    mine = srecv.at[part_of_core]
    send(mine, mine, post.at[0], post.at[1], sibling)
    z_start(0, 1)
    with jax.named_scope("postwait"):
        other = srecv.at[pl.ds((C - 1 - core) * chips, chips)]
        arrived(other, post.at[0], post.at[1], sibling)
    stats = nin[chip]
    ahead_max, ahead_scale, sib_scale = meet(stats[nq : nq + 1, :], sib_st[...])
    ahead_max = jnp.where(is_first, stats[nq : nq + 1, :], ahead_max)
    ahead_scale = jnp.where(is_first, 1.0, ahead_scale)
    sib_scale = jnp.where(is_first, 0.0, sib_scale)
    ahead_normer = ahead_scale * stats[0:nq, :] + sib_scale * sib_st[0:nq, :]
    for j in range(NSP):
        r, c = divmod(j, nc)
        i = j % C * chips + j // C
        m_in[r * R : (r + 1) * R, c * LANES : (c + 1) * LANES] = (
            ahead_scale * srecv[i].astype(f32) + sib_scale * sib_m[i].astype(f32)
        ).astype(bf16)
    normer_in = jnp.concatenate([ahead_normer[r : r + 1, :] for r in range(nq)], axis=1)
    stab = ahead_max[:, 0:1]

    def finish(b, carry):
        at = ds(b * ROW_STEP, ROW_STEP)
        queries = q_ref[at, :]
        carried = runc[at, :] + stab
        top = m1[at, :]
        row_max = jnp.maximum(carried, top)
        inner = jnp.exp(top - row_max)
        outer = jnp.exp(carried - row_max) * scale
        reach = jnp.sum(queries.astype(f32) * normer_in, axis=1, keepdims=True)
        denominator = inner * d1[at, :] + outer * reach
        floor = jnp.maximum(jnp.abs(denominator), jnp.exp(-row_max))
        numerator = inner * a1[at, :] + outer * matmul(queries, m_in[...])
        gate = 1.0 / (1.0 + jnp.exp(-og_ref[at, :].astype(f32)))
        gated[at, :] = (numerator / floor * gate).astype(bf16)
        return carry

    half = own // 2
    part = half // 2

    class Sums:
        def __init__(self, view, base, ring, sems, summed, from_left, from_right, relay_top, relay_bot):
            self.view, self.base, self.ring, self.sems, self.summed = view, base, ring, sems, summed
            self.from_left, self.from_right = from_left, from_right
            self.relays = (relay_top, relay_bot)

        def send(self, src, dst, r, k, side):
            to = self.ring[4](self.ring[side])
            send(src, dst, self.sems.at[0, r, k], self.sems.at[1, r, k], to)

        def wait(self, dst, r, k):
            arrived(dst, self.sems.at[0, r, k], self.sems.at[1, r, k], self.ring[4](self.ring[1]))

        def piece(self, side, low, r):
            return self.view(self.summed, self.base(side) + low * half, r)

        def at_owner(self, buf, low, r):
            return self.view(buf, low * half, r)

        def far(self, r):
            for low in range(2):
                self.send(
                    self.piece(3, low, r), self.view(self.relays[low], 0, r), r, 2 + low, 2 - low
                )

        def near(self, r):
            self.send(self.piece(2, 1, r), self.at_owner(self.from_left, 1, r), r, 0, 2)
            self.send(self.piece(1, 0, r), self.at_owner(self.from_right, 0, r), r, 1, 1)

        def relay(self, r):
            for low, buf in ((0, self.from_left), (1, self.from_right)):
                relay = self.view(self.relays[low], 0, r)
                own_piece = self.piece(2 - low, low, r)
                with jax.named_scope("relay"):
                    self.wait(relay, r, 2 + low)
                if len(relay.shape) == 3:
                    steps_here = relay.shape[0]
                else:
                    steps_here = relay.shape[0] // NORM_STEP

                def merge(b, carry, relay=relay, own_piece=own_piece):
                    at = b if len(relay.shape) == 3 else ds(b * NORM_STEP, NORM_STEP)
                    relay[at] = (relay[at].astype(f32) + own_piece[at].astype(f32)).astype(bf16)
                    return carry

                lax.fori_loop(0, steps_here, merge, 0)
                self.send(relay, self.at_owner(buf, low, r), r, 4 + low, 2 - low)

        def finish(self, r):
            with jax.named_scope("sumwait"):
                self.wait(self.at_owner(self.from_left, 1, r), r, 0)
                self.wait(self.at_owner(self.from_right, 0, r), r, 1)
                self.wait(self.at_owner(self.from_left, 0, r), r, 4)
                self.wait(self.at_owner(self.from_right, 1, r), r, 5)

    def mix_view(ref, row, r):
        return ref.at[ds(row + r * part, part, 16)]

    mixes = Sums(mix_view, lambda side: along_y[side] * own, along_y, mss, mix_part, mix_left, mix_right, mix_top, mix_bot)

    def project(block):
        lines = ds(block * own, own)

        def project_tile(n, carry):
            at = ds(n * TILE, TILE)
            mix_part[lines, at] = matmul(gated[lines, :], wo[:, at]).astype(bf16)
            return carry

        with jax.named_scope("finish"):
            each = own // ROW_STEP
            lax.fori_loop(block * each, (block + 1) * each, finish, 0)
        with jax.named_scope("project"):
            lax.fori_loop(0, D // TILE, project_tile, 0)

    project(across)
    mixes.far(0)
    mixes.far(1)
    z_next(u_events)
    project(right)
    project(left)
    mixes.near(0)
    z_next(u_events)
    project(tp)

    def at_ring(index):
        return {
            "sp": me + core * (at_zx(zz, index, core) - me),
            "tp": index + core * (tp - index),
        }

    spot = tp + core * (xx - tp)
    fl, fr, fo = mod(spot - 1, T), mod(spot + 1, T), mod(spot + 2, T)
    ring = (spot, fl, fr, fo, at_ring)
    block_rows = own + HALO

    def block_base(block):
        return SLOT[block] * block_rows + HALO

    def join(r):
        def join_rows(b, carry):
            row = lax.rem(b, jnp.int32(part // NORM_STEP)) * NORM_STEP + r * part
            row = row + lax.div(b, jnp.int32(part // NORM_STEP)) * half
            at = ds(row, NORM_STEP)
            summed = (
                mix_part[ds(tp * own + row, NORM_STEP), :].astype(f32)
                + mix_left[at, :].astype(f32)
                + mix_right[at, :].astype(f32)
            )
            values = summed.astype(bf16).astype(f32)
            joined = (res_ref[at, :].astype(f32) + normalize(values, mixg_ref[...])).astype(bf16)
            stream[at, :] = joined
            rows_all[ds(block_base(0) + row, NORM_STEP), :] = normalize(
                joined.astype(f32), preg_ref[...]
            ).astype(bf16)
            return carry

        with jax.named_scope("join"):
            lax.fori_loop(0, 2 * (part // NORM_STEP), join_rows, 0)

    mixes.relay(0)
    mixes.near(1)
    z_next(u_events)
    mixes.relay(1)
    z_next(u_events)
    with jax.named_scope("dshards"):
        shards(1, range(X))
    z_next(u_events)
    z_start(1, 0)
    mixes.finish(0)
    join(0)
    ring_start(0, (0, 1, 2, 3))
    z_next(u_events)
    z_start(1, 1)
    mixes.finish(1)
    join(1)
    ring_start(1, (0, 1))

    place = me * T + tp
    after = place + 1
    is_last = after == NSP * T
    nsp = lax.rem(lax.div(after, jnp.int32(T)), jnp.int32(NSP))
    ntp = lax.rem(after, jnp.int32(T))
    ncore = lax.rem(nsp, jnp.int32(C))
    nx = lax.rem(lax.div(nsp, jnp.int32(C)), jnp.int32(X))
    nz = lax.div(nsp, jnp.int32(C * X))
    npos = ntp + ncore * (nx - ntp)
    tail_lines = pl.ds(block_base(0) + own - HALO, HALO)
    for k in range(T):
        to_sp = nsp + ncore * (at_zx(nz, k, ncore) - nsp)
        to_tp = k + ncore * (ntp - k)
        slot = mod(npos - k, T)
        to_lines = ds(slot * block_rows, HALO, 16)
        to_self = to_sp * T + to_tp == place
        go = jnp.logical_not(jnp.logical_or(is_last, to_self))
        send_if(
            go, rows_all.at[tail_lines], rows_all.at[to_lines], halo.at[0, k], halo.at[1, slot],
            {"sp": to_sp, "tp": to_tp},
        )

        @pl.when(jnp.logical_and(to_self, jnp.logical_not(is_last)))
        def _(to_lines=to_lines):
            rows_all[to_lines, :] = rows_all[tail_lines, :]

    ring_start(1, (2, 3))

    def halo_wait(slot):
        device = at_ring(mod(spot + slot, T))
        ahead = device["sp"] * T + device["tp"] - 1
        lines = pl.ds(slot * block_rows, HALO)

        @pl.when(ahead < 0)
        def _():
            rows_all[lines, :] = jnp.zeros((HALO, D), bf16)

        @pl.when(jnp.logical_and(ahead >= 0, ahead != place))
        def _():
            arrived(rows_all.at[lines], halo.at[0, 0], halo.at[1, slot], device)

    ag_wait(0, 0)
    ag_wait(0, 1)
    while u_events:
        z_next(u_events)
    z_next(d_events)
    ag_wait(1, 0)
    ag_wait(1, 1)
    z_next(d_events)

    @pl.when(xx > 0)
    def _():
        for i, dst in enumerate((gk_ref, vk_ref)):
            arrived(dst, taps.at[0, i], taps.at[1, i], at_tp(mod(tp + xx, T)))

    with jax.named_scope("shtwins"):
        shard_twins(0)
        shard_twins(1)
    z_twin(0, range(1, Z // 2 + 1))

    def mix(first, last):
        for slot in range(first, last):
            halo_wait(slot)
        lines = pl.ds(first * block_rows, (last - first) * block_rows)
        within = pl.ds(0, (last - first) * block_rows)

        def raise_tile(n, carry):
            at = ds(n * TILE, TILE)
            upb[within, at] = matmul(rows_all[lines, :], wu[:, at]).astype(bf16).astype(f32)
            return carry

        with jax.named_scope("raise"):
            lax.fori_loop(0, ffd // TILE, raise_tile, 0)
        if first > 0:
            z_next(d_events)
        with jax.named_scope("raise"):
            lax.fori_loop(ffd // TILE, 2 * ffd // TILE, raise_tile, 0)
        z_next(d_events)
        windows = own // CONV_STEP

        def convolve(b, carry):
            block = lax.div(b, jnp.int32(windows))
            row = lax.rem(b, jnp.int32(windows)) * CONV_STEP
            window = ds(block * block_rows + row + HALO - 8, CONV_STEP + 8, 8)
            at = ds((first + block) * own + row, CONV_STEP)
            for c in range(0, ffd, TILE):
                both = []
                for taps_ref, start in ((gk_ref, 0), (vk_ref, ffd)):
                    block_values = upb[window, start + c : start + c + TILE]
                    summed = 0.0
                    for j in range(CONV):
                        low = 8 - CONV + 1 + j
                        summed = summed + taps_ref[j : j + 1, c : c + TILE] * block_values[low : low + CONV_STEP]
                    both.append(summed)
                hidden[at, c : c + TILE] = (both[0] / (1.0 + jnp.exp(-both[0])) * both[1]).astype(bf16)
            return carry

        with jax.named_scope("conv"):
            lax.fori_loop(0, (last - first) * windows, convolve, 0)

    zs_order = [zz]
    for d in range(1, Z // 2):
        zs_order += [mod(zz - d, Z), mod(zz + d, Z)]
    zs_order.append(mod(zz + Z // 2, Z))
    early = max(1, Z - 3)

    def lower(first, last):
        def lower_tile(tile, carry):
            away = lax.div(tile + 1, jnp.int32(2)) * (1 - 2 * lax.rem(tile, jnp.int32(2)))
            z = lax.rem(zz + away + Z, jnp.int32(Z))
            ffn_part[tile] = matmul(hidden[...], wd[ds(z * slab, slab), :], 1, 1).astype(bf16)
            return carry

        with jax.named_scope("lower"):
            lax.fori_loop(first, last, lower_tile, 0)

    def ffn_view(ref, row, r):
        tiles = pl.ds(0, early) if r == 0 else pl.ds(early, Z - early)
        return ref.at[tiles, ds(row, half), :]

    ffns = Sums(ffn_view, lambda side: SLOT[side] * own, ring, rss, ffn_part, ffn_left, ffn_right, ffn_top, ffn_bot)
    mix(0, 1)
    z_next(d_events)
    for k in (2, 3, 4, 5):
        ag_wait(0, k)
    for k in (2, 3, 4, 5):
        ag_wait(1, k)
    mix(1, T)
    while d_events and d_events[0][1] <= max(0, (early - 1) // 2):
        z_next(d_events)
    z_twin(1, range(1, (early - 1) // 2 + 1))
    lower(0, early)
    ffns.far(0)
    ffns.near(0)
    while d_events:
        z_next(d_events)
    if early < Z - 1:
        z_twin(1, range((early - 1) // 2 + 1, Z // 2))
        lower(early, Z - 1)
    z_twin(1, (Z // 2,))
    lower(Z - 1, Z)
    ffns.far(1)
    ffns.relay(0)
    ffns.near(1)
    ffns.relay(1)
    ffns.finish(0)
    ffns.finish(1)

    def close(b, carry):
        at = ds(b * NORM_STEP, NORM_STEP)
        mine = ds(b * NORM_STEP, NORM_STEP)
        values, squares = [], 0.0
        for tile in range(Z):
            summed = (
                ffn_part[tile, mine, :].astype(f32)
                + ffn_left[tile, at, :].astype(f32)
                + ffn_right[tile, at, :].astype(f32)
            )
            values.append(summed.astype(bf16).astype(f32))
            squares = squares + jnp.sum(values[-1] * values[-1], axis=-1, keepdims=True)
        factor = lax.rsqrt(squares * (1.0 / D) + epsilon)
        for tile in range(Z):
            to = ds(zs_order[tile] * slab, slab)
            out_ref[at, to] = (
                stream[at, to].astype(f32) + values[tile] * factor * postg_ref[:, to]
            ).astype(bf16)
        return carry

    with jax.named_scope("close"):
        lax.fori_loop(0, own // NORM_STEP, close, 0)

    for copy in pending:
        if isinstance(copy, tuple):
            pl.when(copy[0])(copy[1].wait_send)
        else:
            copy.wait_send()


def body(
    shape,
    query_rows, key_rows, value_rows, out_gate_pre, input_gate_pre, forget_gate_pre, residual,
    out_proj, mix_gain, pre_gain, gate_proj, value_proj, gate_kernel, value_kernel, down_proj,
    post_gain,
):
    Z, X, C, T = shape
    NSP = Z * X * C
    rows, qk = query_rows.shape
    hv = value_rows.shape[1]
    own, D = residual.shape
    ffd = gate_proj.shape[1]
    R = qk * hv // LANES // NSP
    dma = pltpu.SemaphoreType.DMA
    vm = pltpu.VMEM
    inner = pl.BlockSpec(memory_space=pltpu.VMEM)
    outer = pl.BlockSpec(memory_space=pl.ANY)
    return pl.pallas_call(
        functools.partial(kernel, Z, X, C, T),
        out_shape=jax.ShapeDtypeStruct((own, D), bf16),
        in_specs=[outer] * 16,
        out_specs=inner,
        scratch_shapes=[
            vm((rows, qk), bf16),
            vm((rows, qk), bf16),
            vm((rows, hv), bf16),
            vm((rows, hv), bf16),
            vm((1, rows), f32),
            vm((1, rows), f32),
            vm((own, D), bf16),
            vm((1, D), f32),
            vm((1, D), f32),
            vm((1, D), f32),
            vm((CONV, ffd), f32),
            vm((CONV, ffd), f32),
            vm((NSP, R, LANES), bf16),
            vm((NSP, R, LANES), bf16),
            vm((NSP // C, R, LANES), bf16),
            vm((NSP // C, R, LANES), bf16),
            vm((4, LANES), f32),
            vm((4, LANES), f32),
            vm((4, LANES), f32),
            vm((NSP // C, 4, LANES), f32),
            vm((NSP // C, R, LANES), bf16),
            vm((NSP, R, LANES), bf16),
            vm((NSP // C, 4, LANES), f32),
            vm((qk, hv), bf16),
            vm((rows, qk), bf16),
            vm((rows, 1), f32),
            vm((rows, hv), f32),
            vm((rows, 1), f32),
            vm((rows, 1), f32),
            vm((rows, hv), bf16),
            vm((hv, D), bf16),
            vm((D // NSP, 2 * ffd), bf16),
            vm((D, 2 * ffd), bf16),
            vm((D // NSP, ffd), bf16),
            vm((D, ffd), bf16),
            vm((CONV, ffd), f32),
            vm((CONV, ffd), f32),
            vm((T * (own + HALO), D), bf16),
            vm((own, D), bf16),
            vm(((T - 1) * (own + HALO), 2 * ffd), f32),
            vm((rows, ffd), bf16),
        ]
        + [
            vm((rows, D), bf16),
            vm((own, D), bf16),
            vm((own, D), bf16),
            vm((own // 2, D), bf16),
            vm((own // 2, D), bf16),
            vm((Z, rows, D // Z), bf16),
            vm((Z, own, D // Z), bf16),
            vm((Z, own, D // Z), bf16),
            vm((Z, own // 2, D // Z), bf16),
            vm((Z, own // 2, D // Z), bf16),
        ]
        + [
            dma((4,)),
            dma((12,)),
            dma((2, 2)),
            dma((4,)),
            dma((2,)),
            dma((2,)),
            dma((2, X, 2)),
            dma((2, X, 2)),
            dma((2, 2, 2, Z, X // 2)),
            dma((2, 2, 2, Z, X // 2)),
            dma((2, 2)),
            dma((2, 2, 6)),
            dma((2, 2, 6)),
            dma((2, 2, 6)),
            dma((2, T)),
        ],
        compiler_params=pltpu.CompilerParams(
            collective_id=0, has_side_effects=True, vmem_limit_bytes=60 * 1024 * 1024
        ),
        name="cell_and_mixer",
    )(
        query_rows, key_rows, value_rows, out_gate_pre, input_gate_pre, forget_gate_pre, residual,
        mix_gain.reshape(1, D), pre_gain.reshape(1, D), post_gain.reshape(1, D),
        gate_kernel, value_kernel, out_proj, gate_proj, value_proj, down_proj,
    )


def solution(mesh):
    shape = (*SHAPES[mesh.shape["sp"]], mesh.shape["tp"])
    placed = (
        P("sp", "tp"),
        P("sp", "tp"),
        P("sp", "tp"),
        P("sp", "tp"),
        P("tp", "sp"),
        P("tp", "sp"),
        P(("sp", "tp"), None),
        P("tp", None),
        P(),
        P(),
        P("sp", "tp"),
        P("sp", "tp"),
        P(None, "tp"),
        P(None, "tp"),
        P("sp", "tp"),
        P(),
    )
    return jax.shard_map(
        functools.partial(body, shape), mesh=mesh, in_specs=placed,
        out_specs=P(("sp", "tp"), None), check_vma=False,
    )
```

```python
import functools

import jax
import jax.numpy as jnp
from jax import lax
from jax.experimental import pallas as pl
from jax.experimental.pallas import tpu as pltpu
from jax.sharding import PartitionSpec as P

f32 = jnp.float32
bf16 = jnp.bfloat16
MESH = pl.DeviceIdType.MESH

gate_cap = 15.0
epsilon = 1e-06
far_below = -1e30
CONV = 3
LANES = 128
ROW_STEP = 64
NORM_STEP = 16
CONV_STEP = 32
TILE = 256
HALO = 16
SLOT = (0, 3, 1, 2)

SHAPES = {64: (8, 4, 2)}


def softcap(values):
    return gate_cap * jnp.tanh(values * (1.0 / gate_cap))


def log_one_plus(values):
    series = values * (
        1.0 + values * (-1 / 2 + values * (1 / 3 + values * (-1 / 4 + values * (1 / 5))))
    )
    return jnp.where(values < 0.015625, series, jnp.log(1.0 + values))


def log_sigmoid(values):
    return jnp.minimum(values, 0.0) - log_one_plus(jnp.exp(-jnp.abs(values)))


def normalize(values, gains):
    return values * lax.rsqrt(jnp.mean(values * values, axis=-1, keepdims=True) + epsilon) * gains


def matmul(left, right, left_dim=1, right_dim=0):
    return lax.dot_general(
        left, right, (((left_dim,), (right_dim,)), ((), ())), preferred_element_type=f32
    )


def mod(value, size):
    return lax.rem(value + size, jnp.int32(size))


def kernel(
    Z, X, C, T,
    q_in, k_in, v_in, og_in, ig_in, fg_in, res_in, mixg_in, preg_in, postg_in, gk_in, vk_in,
    outp_ref, gatep_ref, valuep_ref, downp_ref,
    out_ref,
    q_ref, k_ref, v_ref, og_ref, ig_ref, fg_ref, res_ref, mixg_ref, preg_ref, postg_ref, gk_own, vk_own,
    msend, sib_m, csend, mrecv, st_src, sib_st, cst, st_recv, ssend, srecv, nin, m_in, kwb, runc, a1, m1, d1,
    gated, wo, ushard, wu, dshard, wd, gk_ref, vk_ref, rows_all, stream, upb, hidden,
    mix_part, mix_left, mix_right, mix_top, mix_bot,
    ffn_part, ffn_left, ffn_right, ffn_top, ffn_bot,
    loc, loaded, pre, p1, p2, post, xs, xd, zs, zd, taps, ags, mss, rss, halo,
):
    NSP = Z * X * C
    rows, qk = q_ref.shape
    hv = v_ref.shape[1]
    own, D = out_ref.shape
    ffd = gatep_ref.shape[1]
    scale = float(qk) ** -0.5
    me = lax.axis_index("sp")
    tp = lax.axis_index("tp")
    core = lax.rem(me, jnp.int32(C))
    xx = lax.rem(lax.div(me, jnp.int32(C)), jnp.int32(X))
    zz = lax.div(me, jnp.int32(C * X))
    pending = []

    def at_sp(index):
        return {"sp": index, "tp": tp}

    def at_tp(index):
        return {"sp": me, "tp": index}

    def at_zx(z, x, c):
        return z * (X * C) + x * C + c

    def remote(src, dst, ssem, rsem, device):
        return pltpu.make_async_remote_copy(
            src_ref=src, dst_ref=dst, send_sem=ssem, recv_sem=rsem,
            device_id=device, device_id_type=MESH,
        )

    def send(src, dst, ssem, rsem, device):
        copy = remote(src, dst, ssem, rsem, device)
        copy.start()
        pending.append(copy)

    def send_if(condition, src, dst, ssem, rsem, device):
        copy = remote(src, dst, ssem, rsem, device)
        pl.when(condition)(copy.start)
        pending.append((condition, copy))

    def arrived(dst, ssem, rsem, device):
        remote(dst, dst, ssem, rsem, device).wait_recv()

    def ds(start, size, step=None):
        return pl.ds(pl.multiple_of(start, step or size), size)

    sibling = at_sp(me + 1 - 2 * core)

    units = lax.rem(xx + tp, jnp.int32(T))

    def holder(x):
        return {"sp": at_zx(zz, x, core), "tp": mod(tp - x, T)}

    def source(x):
        return {"sp": at_zx(zz, x, core), "tp": units}

    barrier = pltpu.get_barrier_semaphore()

    chips = NSP // C
    chip = lax.div(me, jnp.int32(C))

    def at_chip(index):
        return at_sp(index * C + core)

    def greet(p, carry):
        pl.semaphore_signal(
            barrier, 1, device_id=at_chip(mod(chip + p, chips)), device_id_type=MESH
        )
        return carry

    lax.fori_loop(1, chips, greet, 0)
    pl.semaphore_signal(barrier, 1, device_id=sibling, device_id_type=MESH)
    for k in range(1, T):
        pl.semaphore_signal(barrier, 1, device_id=at_tp(mod(tp + k, T)), device_id_type=MESH)
    for k in range(X):

        @pl.when(xx + k > 0)
        def _(k=k):
            pl.semaphore_signal(barrier, 1, device_id=source(k), device_id_type=MESH)

    loads = [
        pltpu.make_async_copy(src, dst, loaded.at[i])
        for i, (src, dst) in enumerate((
            (ig_in, ig_ref), (fg_in, fg_ref), (k_in, k_ref), (v_in, v_ref), (q_in, q_ref),
            (og_in, og_ref), (res_in, res_ref), (mixg_in, mixg_ref), (preg_in, preg_ref),
            (postg_in, postg_ref), (gk_in, gk_own), (vk_in, vk_own),
        ))
    ]
    shard = gatep_ref.shape[0]
    local = [
        pltpu.make_async_copy(gatep_ref, ushard.at[:, pl.ds(0, ffd)], loc.at[0]),
        pltpu.make_async_copy(valuep_ref, ushard.at[:, pl.ds(ffd, ffd)], loc.at[1]),
        pltpu.make_async_copy(downp_ref, dshard, loc.at[2]),
        pltpu.make_async_copy(outp_ref, wo, loc.at[3]),
    ]
    for copy in loads + local:
        copy.start()

    steps = rows // ROW_STEP
    lane = lax.broadcasted_iota(jnp.int32, (ROW_STEP, rows), 1)
    line = lax.broadcasted_iota(jnp.int32, (ROW_STEP, rows), 0)
    loads[0].wait()
    loads[1].wait()
    li_row = softcap(ig_ref[...])
    lf_row = log_sigmoid(softcap(fg_ref[...]))

    def sums(b, run_row):
        here = line + b * ROW_STEP
        run_col = jnp.sum(jnp.where(lane <= here, lf_row, 0.0), axis=1, keepdims=True)
        runc[ds(b * ROW_STEP, ROW_STEP), :] = run_col
        return run_row + jnp.sum(jnp.where(lane == here, run_col, 0.0), axis=0, keepdims=True)

    run_row = lax.fori_loop(0, steps, sums, jnp.zeros((1, rows), f32), unroll=True)
    total = run_row[:, rows - 1 : rows]
    lead = total - run_row + li_row
    lead_max = jnp.max(lead, axis=1, keepdims=True)
    lead_weights = jnp.exp(lead - lead_max)
    loads[2].wait()
    loads[3].wait()

    def weigh(b, normer):
        here = line + b * ROW_STEP
        at = ds(b * ROW_STEP, ROW_STEP)
        column = jnp.sum(jnp.where(lane == here, lead_weights, 0.0), axis=1, keepdims=True)
        weighted = k_ref[at, :].astype(f32) * column
        kwb[at, :] = weighted.astype(bf16)
        return normer + jnp.sum(weighted, axis=0, keepdims=True)

    normer = lax.fori_loop(0, steps, weigh, jnp.zeros((1, qk), f32), unroll=True)
    nq = qk // LANES
    for r in range(nq):
        st_src[r : r + 1, :] = normer[:, r * LANES : (r + 1) * LANES]
    for r in range(nq, 4):
        st_src[r : r + 1, :] = jnp.broadcast_to(total if r == nq else lead_max, (1, LANES))
    R = msend.shape[1]
    nc = hv // LANES
    for r in range(nq):
        part = matmul(kwb[:, r * LANES : (r + 1) * LANES], v_ref[...], 0, 0)
        for rr in range(LANES // R):
            for c in range(nc):
                j = (r * (LANES // R) + rr) * nc + c
                msend[j % C * chips + j // C] = part[
                    rr * R : (rr + 1) * R, c * LANES : (c + 1) * LANES
                ].astype(bf16)

    with jax.named_scope("barrier"):
        pl.semaphore_wait(barrier, chips + T - 1 + X - 1 + jnp.minimum(xx, 1))

    send(msend, sib_m, pre.at[0, 0], pre.at[1, 0], sibling)
    send(st_src, sib_st, pre.at[0, 1], pre.at[1, 1], sibling)
    is_first = core == 0
    with jax.named_scope("pair"):
        arrived(sib_st, pre.at[0, 1], pre.at[1, 1], sibling)
        arrived(sib_m, pre.at[0, 0], pre.at[1, 0], sibling)
    one = jnp.where(is_first, st_src[...], sib_st[...])
    two = jnp.where(is_first, sib_st[...], st_src[...])

    def meet(highest, following):
        decayed = highest + following[nq : nq + 1, :]
        lead_d = following[nq + 1 : nq + 2, :]
        new = jnp.maximum(decayed, lead_d)
        return new, jnp.exp(decayed - new), jnp.exp(lead_d - new)

    pair_max, weight_one, weight_two = meet(one[nq + 1 : nq + 2, :], two)
    cst[0:nq, :] = weight_one * one[0:nq, :] + weight_two * two[0:nq, :]
    cst[nq : nq + 1, :] = one[nq : nq + 1, :] + two[nq : nq + 1, :]
    cst[nq + 1 : nq + 2, :] = pair_max
    weight_mine = jnp.where(is_first, weight_one, weight_two)
    weight_sib = jnp.where(is_first, weight_two, weight_one)

    def pair(i, carry):
        for u in range(4):
            j = i * 4 + u
            csend[j] = (
                weight_mine * msend[core * chips + j].astype(f32)
                + weight_sib * sib_m[core * chips + j].astype(f32)
            ).astype(bf16)
        return carry

    lax.fori_loop(0, chips // 4, pair, 0)

    mrecv[chip] = csend[chip]
    st_recv[chip] = cst[...]

    def scatter(p, carry):
        dst = mod(chip + p, chips)
        remote(csend.at[dst], mrecv.at[chip], p1.at[0], p1.at[1], at_chip(dst)).start()
        remote(cst, st_recv.at[chip], p1.at[2], p1.at[3], at_chip(dst)).start()
        return carry

    with jax.named_scope("scatter"):
        lax.fori_loop(1, chips, scatter, 0)

    left, right, across = mod(tp - 1, T), mod(tp + 1, T), mod(tp + 2, T)
    along_y = (tp, left, right, across, at_tp)

    def block_piece(side, low, r):
        return rows_all.at[pl.ds(block_base(side) + low * half + r * part, part)]

    def ring_start(r, ks):
        for k in ks:
            low, side = ((0, 2), (1, 1), (1, 2), (0, 1))[k]
            send(
                block_piece(0, low, r), block_piece(3 - side, low, r),
                ags.at[0, r, k], ags.at[1, r, k], at_ring(ring[side]),
            )

    def ag_wait(r, k):
        with jax.named_scope("ag" + str(k)):
            side, low = ((1, 0), (2, 1), (1, 1), (2, 0), (3, 0), (3, 1))[k]
            piece = block_piece(side, low, r)
            arrived(piece, ags.at[0, r, k], ags.at[1, r, k], at_ring(fl))
            if k < 2:
                to = at_ring((fr, fl)[k])
                send(piece, block_piece(3, low, r), ags.at[0, r, k + 4], ags.at[1, r, k + 4], to)

    for copy in local:
        copy.wait()
    for copy in loads[4:]:
        copy.wait()

    def rows_of(index):
        return ds(index * shard, shard)

    weights = ((ushard, wu), (dshard, wd))
    def spread(w):
        src, dst = weights[w]
        for k in range(X):
            send_if(
                xx + k > 0, src, dst.at[rows_of(me)], xs.at[0, k, w], xs.at[1, xx, w], holder(k)
            )

    spread(0)

    @pl.when(xx == 0)
    def _():
        for src, dst in weights:
            dst[rows_of(me), :] = src[...]

    for i, (src, dst) in enumerate(((gk_own, gk_ref), (vk_own, vk_ref))):
        send_if(xx > 0, src, dst, taps.at[0, i], taps.at[1, i], at_tp(mod(tp - xx, T)))

    @pl.when(xx == 0)
    def _():
        gk_ref[...] = gk_own[...]
        vk_ref[...] = vk_own[...]

    def inside(b, carry):
        at = ds(b * ROW_STEP, ROW_STEP)
        here = line + b * ROW_STEP
        logs = jnp.where(lane <= here, runc[at, :] - run_row + li_row, far_below)
        top = jnp.max(logs, axis=1, keepdims=True)
        scores = matmul(q_ref[at, :], k_ref[...], 1, 1) * (jnp.exp(logs - top) * scale)
        m1[at, :] = top
        d1[at, :] = jnp.sum(scores, axis=1, keepdims=True)
        a1[at, :] = matmul(scores.astype(bf16), v_ref[...])
        return carry

    with jax.named_scope("inside"):
        lax.fori_loop(0, steps, inside, 0)

    def shards(w, ks):
        for k in ks:
            piece = weights[w][1].at[rows_of(at_zx(zz, k, core))]

            @pl.when(xx + k > 0)
            def _():
                arrived(piece, xs.at[0, k, w], xs.at[1, k, w], source(k))

            send(piece, piece, xd.at[0, k, w], xd.at[1, k, w], sibling)

    def shard_twins(w):
        for k in range(X):
            piece = weights[w][1].at[rows_of(at_zx(zz, k, 1 - core))]
            arrived(piece, xd.at[0, k, w], xd.at[1, k, w], sibling)

    def all_but_one(buf):
        return buf.at[pl.ds(0, chips - 1)]

    def bulk(buf, sems, s):
        remote(all_but_one(buf), all_but_one(buf), sems.at[s], sems.at[s + 1], at_sp(me)).wait()

    with jax.named_scope("p1wait"):
        bulk(mrecv, p1, 0)
        bulk(st_recv, p1, 2)

    def advance(i, state):
        highest, memory, norm = state
        for u in range(4):
            d = i * 4 + u
            ssend[d] = memory.astype(bf16)
            nin[d, 0:nq, :] = norm
            nin[d, nq : nq + 1, :] = highest
            following = st_recv[d]
            highest, before, after = meet(highest, following)
            memory = before * memory + after * mrecv[d].astype(f32)
            norm = before * norm + after * following[0:nq, :]
        return highest, memory, norm

    lax.fori_loop(
        0, chips // 4, advance,
        (jnp.full((1, LANES), far_below, f32), jnp.zeros((R, LANES), f32), jnp.zeros((nq, LANES), f32)),
    )
    part_of_core = pl.ds(core * chips, chips)
    srecv[core * chips + chip] = ssend[chip]

    def give_back(p, carry):
        dst = mod(chip + p, chips)
        remote(
            ssend.at[dst], srecv.at[core * chips + chip], p2.at[0], p2.at[1], at_chip(dst)
        ).start()
        return carry

    with jax.named_scope("giveback"):
        lax.fori_loop(1, chips, give_back, 0)

    spread(1)
    slab = shard * X * C
    ups = (at_zx(mod(zz + 1, Z), xx, core), at_zx(mod(zz - 1, Z), xx, core))

    def z_piece(w, direction, s, h, c):
        z = mod(zz - s if direction == 0 else zz + s, Z)
        return [
            weights[w][1].at[rows_of(at_zx(z, h * (X // 2) + q, c))] for q in range(X // 2)
        ]

    def z_has(direction, s, h):
        return s < Z // 2 or (s == Z // 2 and h == direction)

    def z_send(w, direction, s, h):
        if z_has(direction, s, h):
            i = (s - 1) * 2 + h
            for q, piece in enumerate(z_piece(w, direction, s - 1, h, core)):
                send(
                    piece, piece, zs.at[0, w, direction, i, q], zs.at[1, w, direction, i, q],
                    at_sp(ups[direction]),
                )

    def z_start(w, h):
        for direction in range(2):
            z_send(w, direction, 1, h)

    def z_step(w, s, h):
        with jax.named_scope(("uring", "dring")[w] + str(s) + str(h)):
            for direction in range(2):
                if z_has(direction, s, h):
                    pieces = z_piece(w, direction, s, h, core)
                    i = (s - 1) * 2 + h
                    for q, piece in enumerate(pieces):
                        arrived(
                            piece, zs.at[0, w, direction, i, q], zs.at[1, w, direction, i, q],
                            at_sp(ups[direction]),
                        )
                    z_send(w, direction, s + 1, h)
                    for q, piece in enumerate(pieces):
                        send(
                            piece, piece, zd.at[0, w, direction, i, q], zd.at[1, w, direction, i, q],
                            sibling,
                        )

    def z_twin(w, distances):
        with jax.named_scope(("utwin", "dtwin")[w]):
            for s in distances:
                for h in range(2):
                    for direction in range(2):
                        if z_has(direction, s, h):
                            i = (s - 1) * 2 + h
                            for q, piece in enumerate(z_piece(w, direction, s, h, 1 - core)):
                                arrived(
                                    piece, zd.at[0, w, direction, i, q],
                                    zd.at[1, w, direction, i, q], sibling,
                                )

    u_events = [(0, s, h) for s in range(1, Z // 2 + 1) for h in range(2)]
    d_events = [(1, s, h) for s in range(1, Z // 2 + 1) for h in range(2)]

    def z_next(events):
        if events:
            z_step(*events.pop(0))

    with jax.named_scope("ushards"):
        shards(0, range(X // 2))
    z_start(0, 0)
    with jax.named_scope("ushards2"):
        shards(0, range(X // 2, X))

    with jax.named_scope("p2wait"):
        bulk(srecv, p2, 0)
    mine = srecv.at[part_of_core]
    send(mine, mine, post.at[0], post.at[1], sibling)
    z_start(0, 1)
    with jax.named_scope("postwait"):
        other = srecv.at[pl.ds((C - 1 - core) * chips, chips)]
        arrived(other, post.at[0], post.at[1], sibling)
    stats = nin[chip]
    ahead_max, ahead_scale, sib_scale = meet(stats[nq : nq + 1, :], sib_st[...])
    ahead_max = jnp.where(is_first, stats[nq : nq + 1, :], ahead_max)
    ahead_scale = jnp.where(is_first, 1.0, ahead_scale)
    sib_scale = jnp.where(is_first, 0.0, sib_scale)
    ahead_normer = ahead_scale * stats[0:nq, :] + sib_scale * sib_st[0:nq, :]
    for j in range(NSP):
        r, c = divmod(j, nc)
        i = j % C * chips + j // C
        m_in[r * R : (r + 1) * R, c * LANES : (c + 1) * LANES] = (
            ahead_scale * srecv[i].astype(f32) + sib_scale * sib_m[i].astype(f32)
        ).astype(bf16)
    normer_in = jnp.concatenate([ahead_normer[r : r + 1, :] for r in range(nq)], axis=1)
    stab = ahead_max[:, 0:1]

    def finish(b, carry):
        at = ds(b * ROW_STEP, ROW_STEP)
        queries = q_ref[at, :]
        carried = runc[at, :] + stab
        top = m1[at, :]
        row_max = jnp.maximum(carried, top)
        inner = jnp.exp(top - row_max)
        outer = jnp.exp(carried - row_max) * scale
        reach = jnp.sum(queries.astype(f32) * normer_in, axis=1, keepdims=True)
        denominator = inner * d1[at, :] + outer * reach
        floor = jnp.maximum(jnp.abs(denominator), jnp.exp(-row_max))
        numerator = inner * a1[at, :] + outer * matmul(queries, m_in[...])
        gate = 1.0 / (1.0 + jnp.exp(-og_ref[at, :].astype(f32)))
        gated[at, :] = (numerator / floor * gate).astype(bf16)
        return carry

    half = own // 2
    part = half // 2

    class Sums:
        def __init__(self, view, base, ring, sems, summed, from_left, from_right, relay_top, relay_bot):
            self.view, self.base, self.ring, self.sems, self.summed = view, base, ring, sems, summed
            self.from_left, self.from_right = from_left, from_right
            self.relays = (relay_top, relay_bot)

        def send(self, src, dst, r, k, side):
            to = self.ring[4](self.ring[side])
            send(src, dst, self.sems.at[0, r, k], self.sems.at[1, r, k], to)

        def wait(self, dst, r, k):
            arrived(dst, self.sems.at[0, r, k], self.sems.at[1, r, k], self.ring[4](self.ring[1]))

        def piece(self, side, low, r):
            return self.view(self.summed, self.base(side) + low * half, r)

        def at_owner(self, buf, low, r):
            return self.view(buf, low * half, r)

        def far(self, r):
            for low in range(2):
                self.send(
                    self.piece(3, low, r), self.view(self.relays[low], 0, r), r, 2 + low, 2 - low
                )

        def near(self, r):
            self.send(self.piece(2, 1, r), self.at_owner(self.from_left, 1, r), r, 0, 2)
            self.send(self.piece(1, 0, r), self.at_owner(self.from_right, 0, r), r, 1, 1)

        def relay(self, r):
            for low, buf in ((0, self.from_left), (1, self.from_right)):
                relay = self.view(self.relays[low], 0, r)
                own_piece = self.piece(2 - low, low, r)
                with jax.named_scope("relay"):
                    self.wait(relay, r, 2 + low)
                if len(relay.shape) == 3:
                    steps_here = relay.shape[0]
                else:
                    steps_here = relay.shape[0] // NORM_STEP

                def merge(b, carry, relay=relay, own_piece=own_piece):
                    at = b if len(relay.shape) == 3 else ds(b * NORM_STEP, NORM_STEP)
                    relay[at] = (relay[at].astype(f32) + own_piece[at].astype(f32)).astype(bf16)
                    return carry

                lax.fori_loop(0, steps_here, merge, 0)
                self.send(relay, self.at_owner(buf, low, r), r, 4 + low, 2 - low)

        def finish(self, r):
            with jax.named_scope("sumwait"):
                self.wait(self.at_owner(self.from_left, 1, r), r, 0)
                self.wait(self.at_owner(self.from_right, 0, r), r, 1)
                self.wait(self.at_owner(self.from_left, 0, r), r, 4)
                self.wait(self.at_owner(self.from_right, 1, r), r, 5)

    def mix_view(ref, row, r):
        return ref.at[ds(row + r * part, part, 16)]

    mixes = Sums(mix_view, lambda side: along_y[side] * own, along_y, mss, mix_part, mix_left, mix_right, mix_top, mix_bot)

    def project(block):
        lines = ds(block * own, own)

        def project_tile(n, carry):
            at = ds(n * TILE, TILE)
            mix_part[lines, at] = matmul(gated[lines, :], wo[:, at]).astype(bf16)
            return carry

        with jax.named_scope("finish"):
            each = own // ROW_STEP
            lax.fori_loop(block * each, (block + 1) * each, finish, 0)
        with jax.named_scope("project"):
            lax.fori_loop(0, D // TILE, project_tile, 0)

    project(across)
    mixes.far(0)
    mixes.far(1)
    z_next(u_events)
    project(right)
    project(left)
    mixes.near(0)
    z_next(u_events)
    project(tp)

    def at_ring(index):
        return {
            "sp": me + core * (at_zx(zz, index, core) - me),
            "tp": index + core * (tp - index),
        }

    spot = tp + core * (xx - tp)
    fl, fr, fo = mod(spot - 1, T), mod(spot + 1, T), mod(spot + 2, T)
    ring = (spot, fl, fr, fo, at_ring)
    block_rows = own + HALO

    def block_base(block):
        return SLOT[block] * block_rows + HALO

    def join(r):
        def join_rows(b, carry):
            row = lax.rem(b, jnp.int32(part // NORM_STEP)) * NORM_STEP + r * part
            row = row + lax.div(b, jnp.int32(part // NORM_STEP)) * half
            at = ds(row, NORM_STEP)
            summed = (
                mix_part[ds(tp * own + row, NORM_STEP), :].astype(f32)
                + mix_left[at, :].astype(f32)
                + mix_right[at, :].astype(f32)
            )
            values = summed.astype(bf16).astype(f32)
            joined = (res_ref[at, :].astype(f32) + normalize(values, mixg_ref[...])).astype(bf16)
            stream[at, :] = joined
            rows_all[ds(block_base(0) + row, NORM_STEP), :] = normalize(
                joined.astype(f32), preg_ref[...]
            ).astype(bf16)
            return carry

        with jax.named_scope("join"):
            lax.fori_loop(0, 2 * (part // NORM_STEP), join_rows, 0)

    mixes.relay(0)
    mixes.near(1)
    z_next(u_events)
    mixes.relay(1)
    z_next(u_events)
    with jax.named_scope("dshards"):
        shards(1, range(X))
    z_next(u_events)
    z_start(1, 0)
    mixes.finish(0)
    join(0)
    ring_start(0, (0, 1, 2, 3))
    z_next(u_events)
    z_start(1, 1)
    mixes.finish(1)
    join(1)
    ring_start(1, (0, 1))

    place = me * T + tp
    after = place + 1
    is_last = after == NSP * T
    nsp = lax.rem(lax.div(after, jnp.int32(T)), jnp.int32(NSP))
    ntp = lax.rem(after, jnp.int32(T))
    ncore = lax.rem(nsp, jnp.int32(C))
    nx = lax.rem(lax.div(nsp, jnp.int32(C)), jnp.int32(X))
    nz = lax.div(nsp, jnp.int32(C * X))
    npos = ntp + ncore * (nx - ntp)
    tail_lines = pl.ds(block_base(0) + own - HALO, HALO)
    for k in range(T):
        to_sp = nsp + ncore * (at_zx(nz, k, ncore) - nsp)
        to_tp = k + ncore * (ntp - k)
        slot = mod(npos - k, T)
        to_lines = ds(slot * block_rows, HALO, 16)
        to_self = to_sp * T + to_tp == place
        go = jnp.logical_not(jnp.logical_or(is_last, to_self))
        send_if(
            go, rows_all.at[tail_lines], rows_all.at[to_lines], halo.at[0, k], halo.at[1, slot],
            {"sp": to_sp, "tp": to_tp},
        )

        @pl.when(jnp.logical_and(to_self, jnp.logical_not(is_last)))
        def _(to_lines=to_lines):
            rows_all[to_lines, :] = rows_all[tail_lines, :]

    ring_start(1, (2, 3))

    def halo_wait(slot):
        device = at_ring(mod(spot + slot, T))
        ahead = device["sp"] * T + device["tp"] - 1
        lines = pl.ds(slot * block_rows, HALO)

        @pl.when(ahead < 0)
        def _():
            rows_all[lines, :] = jnp.zeros((HALO, D), bf16)

        @pl.when(jnp.logical_and(ahead >= 0, ahead != place))
        def _():
            arrived(rows_all.at[lines], halo.at[0, 0], halo.at[1, slot], device)

    ag_wait(0, 0)
    ag_wait(0, 1)
    z_next(u_events)
    z_next(d_events)
    ag_wait(1, 0)
    ag_wait(1, 1)
    while u_events:
        z_next(u_events)
    z_next(d_events)

    @pl.when(xx > 0)
    def _():
        for i, dst in enumerate((gk_ref, vk_ref)):
            arrived(dst, taps.at[0, i], taps.at[1, i], at_tp(mod(tp + xx, T)))

    with jax.named_scope("shtwins"):
        shard_twins(0)
        shard_twins(1)
    z_twin(0, range(1, Z // 2 + 1))

    def mix(first, last):
        for slot in range(first, last):
            halo_wait(slot)
        lines = pl.ds(first * block_rows, (last - first) * block_rows)
        within = pl.ds(0, (last - first) * block_rows)

        def raise_tile(n, carry):
            at = ds(n * TILE, TILE)
            upb[within, at] = matmul(rows_all[lines, :], wu[:, at]).astype(bf16).astype(f32)
            return carry

        with jax.named_scope("raise"):
            lax.fori_loop(0, ffd // TILE, raise_tile, 0)
        z_next(d_events)
        with jax.named_scope("raise"):
            lax.fori_loop(ffd // TILE, 2 * ffd // TILE, raise_tile, 0)
        if first > 0:
            z_next(d_events)
        windows = own // CONV_STEP

        def convolve(b, carry):
            block = lax.div(b, jnp.int32(windows))
            row = lax.rem(b, jnp.int32(windows)) * CONV_STEP
            window = ds(block * block_rows + row + HALO - 8, CONV_STEP + 8, 8)
            at = ds((first + block) * own + row, CONV_STEP)
            for c in range(0, ffd, TILE):
                both = []
                for taps_ref, start in ((gk_ref, 0), (vk_ref, ffd)):
                    block_values = upb[window, start + c : start + c + TILE]
                    summed = 0.0
                    for j in range(CONV):
                        low = 8 - CONV + 1 + j
                        summed = summed + taps_ref[j : j + 1, c : c + TILE] * block_values[low : low + CONV_STEP]
                    both.append(summed)
                hidden[at, c : c + TILE] = (both[0] / (1.0 + jnp.exp(-both[0])) * both[1]).astype(bf16)
            return carry

        with jax.named_scope("conv"):
            lax.fori_loop(0, (last - first) * windows, convolve, 0)

    zs_order = [zz]
    for d in range(1, Z // 2):
        zs_order += [mod(zz - d, Z), mod(zz + d, Z)]
    zs_order.append(mod(zz + Z // 2, Z))
    early = max(1, Z - 3)

    def lower(first, last):
        def lower_tile(tile, carry):
            away = lax.div(tile + 1, jnp.int32(2)) * (1 - 2 * lax.rem(tile, jnp.int32(2)))
            z = lax.rem(zz + away + Z, jnp.int32(Z))
            ffn_part[tile] = matmul(hidden[...], wd[ds(z * slab, slab), :], 1, 1).astype(bf16)
            return carry

        with jax.named_scope("lower"):
            lax.fori_loop(first, last, lower_tile, 0)

    def ffn_view(ref, row, r):
        tiles = pl.ds(0, early) if r == 0 else pl.ds(early, Z - early)
        return ref.at[tiles, ds(row, half), :]

    ffns = Sums(ffn_view, lambda side: SLOT[side] * own, ring, rss, ffn_part, ffn_left, ffn_right, ffn_top, ffn_bot)
    mix(0, 1)
    z_next(d_events)
    for k in (2, 3, 4, 5):
        ag_wait(0, k)
    for k in (2, 3, 4, 5):
        ag_wait(1, k)
    mix(1, T)
    while d_events and d_events[0][1] <= max(0, (early - 1) // 2):
        z_next(d_events)
    z_twin(1, range(1, (early - 1) // 2 + 1))
    lower(0, early)
    ffns.far(0)
    ffns.near(0)
    while d_events:
        z_next(d_events)
    if early < Z - 1:
        z_twin(1, range((early - 1) // 2 + 1, Z // 2))
        lower(early, Z - 1)
    z_twin(1, (Z // 2,))
    lower(Z - 1, Z)
    ffns.far(1)
    ffns.relay(0)
    ffns.near(1)
    ffns.relay(1)
    ffns.finish(0)
    ffns.finish(1)

    def close(b, carry):
        at = ds(b * NORM_STEP, NORM_STEP)
        mine = ds(b * NORM_STEP, NORM_STEP)
        values, squares = [], 0.0
        for tile in range(Z):
            summed = (
                ffn_part[tile, mine, :].astype(f32)
                + ffn_left[tile, at, :].astype(f32)
                + ffn_right[tile, at, :].astype(f32)
            )
            values.append(summed.astype(bf16).astype(f32))
            squares = squares + jnp.sum(values[-1] * values[-1], axis=-1, keepdims=True)
        factor = lax.rsqrt(squares * (1.0 / D) + epsilon)
        for tile in range(Z):
            to = ds(zs_order[tile] * slab, slab)
            out_ref[at, to] = (
                stream[at, to].astype(f32) + values[tile] * factor * postg_ref[:, to]
            ).astype(bf16)
        return carry

    with jax.named_scope("close"):
        lax.fori_loop(0, own // NORM_STEP, close, 0)

    for copy in pending:
        if isinstance(copy, tuple):
            pl.when(copy[0])(copy[1].wait_send)
        else:
            copy.wait_send()


def body(
    shape,
    query_rows, key_rows, value_rows, out_gate_pre, input_gate_pre, forget_gate_pre, residual,
    out_proj, mix_gain, pre_gain, gate_proj, value_proj, gate_kernel, value_kernel, down_proj,
    post_gain,
):
    Z, X, C, T = shape
    NSP = Z * X * C
    rows, qk = query_rows.shape
    hv = value_rows.shape[1]
    own, D = residual.shape
    ffd = gate_proj.shape[1]
    R = qk * hv // LANES // NSP
    dma = pltpu.SemaphoreType.DMA
    vm = pltpu.VMEM
    inner = pl.BlockSpec(memory_space=pltpu.VMEM)
    outer = pl.BlockSpec(memory_space=pl.ANY)
    return pl.pallas_call(
        functools.partial(kernel, Z, X, C, T),
        out_shape=pltpu.VMEM((own, D), bf16),
        in_specs=[outer] * 16,
        out_specs=inner,
        scratch_shapes=[
            vm((rows, qk), bf16),
            vm((rows, qk), bf16),
            vm((rows, hv), bf16),
            vm((rows, hv), bf16),
            vm((1, rows), f32),
            vm((1, rows), f32),
            vm((own, D), bf16),
            vm((1, D), f32),
            vm((1, D), f32),
            vm((1, D), f32),
            vm((CONV, ffd), f32),
            vm((CONV, ffd), f32),
            vm((NSP, R, LANES), bf16),
            vm((NSP, R, LANES), bf16),
            vm((NSP // C, R, LANES), bf16),
            vm((NSP // C, R, LANES), bf16),
            vm((4, LANES), f32),
            vm((4, LANES), f32),
            vm((4, LANES), f32),
            vm((NSP // C, 4, LANES), f32),
            vm((NSP // C, R, LANES), bf16),
            vm((NSP, R, LANES), bf16),
            vm((NSP // C, 4, LANES), f32),
            vm((qk, hv), bf16),
            vm((rows, qk), bf16),
            vm((rows, 1), f32),
            vm((rows, hv), f32),
            vm((rows, 1), f32),
            vm((rows, 1), f32),
            vm((rows, hv), bf16),
            vm((hv, D), bf16),
            vm((D // NSP, 2 * ffd), bf16),
            vm((D, 2 * ffd), bf16),
            vm((D // NSP, ffd), bf16),
            vm((D, ffd), bf16),
            vm((CONV, ffd), f32),
            vm((CONV, ffd), f32),
            vm((T * (own + HALO), D), bf16),
            vm((own, D), bf16),
            vm(((T - 1) * (own + HALO), 2 * ffd), f32),
            vm((rows, ffd), bf16),
        ]
        + [
            vm((rows, D), bf16),
            vm((own, D), bf16),
            vm((own, D), bf16),
            vm((own // 2, D), bf16),
            vm((own // 2, D), bf16),
            vm((Z, rows, D // Z), bf16),
            vm((Z, own, D // Z), bf16),
            vm((Z, own, D // Z), bf16),
            vm((Z, own // 2, D // Z), bf16),
            vm((Z, own // 2, D // Z), bf16),
        ]
        + [
            dma((4,)),
            dma((12,)),
            dma((2, 2)),
            dma((4,)),
            dma((2,)),
            dma((2,)),
            dma((2, X, 2)),
            dma((2, X, 2)),
            dma((2, 2, 2, Z, X // 2)),
            dma((2, 2, 2, Z, X // 2)),
            dma((2, 2)),
            dma((2, 2, 6)),
            dma((2, 2, 6)),
            dma((2, 2, 6)),
            dma((2, T)),
        ],
        compiler_params=pltpu.CompilerParams(
            collective_id=0, has_side_effects=True, vmem_limit_bytes=60 * 1024 * 1024
        ),
        name="cell_and_mixer",
    )(
        query_rows, key_rows, value_rows, out_gate_pre, input_gate_pre, forget_gate_pre, residual,
        mix_gain.reshape(1, D), pre_gain.reshape(1, D), post_gain.reshape(1, D),
        gate_kernel, value_kernel, out_proj, gate_proj, value_proj, down_proj,
    )


def solution(mesh):
    shape = (*SHAPES[mesh.shape["sp"]], mesh.shape["tp"])
    placed = (
        P("sp", "tp"),
        P("sp", "tp"),
        P("sp", "tp"),
        P("sp", "tp"),
        P("tp", "sp"),
        P("tp", "sp"),
        P(("sp", "tp"), None),
        P("tp", None),
        P(),
        P(),
        P("sp", "tp"),
        P("sp", "tp"),
        P(None, "tp"),
        P(None, "tp"),
        P("sp", "tp"),
        P(),
    )
    return jax.shard_map(
        functools.partial(body, shape), mesh=mesh, in_specs=placed,
        out_specs=P(("sp", "tp"), None), check_vma=False,
    )
```

```python
import functools

import jax
import jax.numpy as jnp
from jax import lax
from jax.experimental import pallas as pl
from jax.experimental.pallas import tpu as pltpu
from jax.sharding import PartitionSpec as P

f32 = jnp.float32
bf16 = jnp.bfloat16
MESH = pl.DeviceIdType.MESH

gate_cap = 15.0
epsilon = 1e-06
far_below = -1e30
CONV = 3
LANES = 128
ROW_STEP = 64
NORM_STEP = 16
CONV_STEP = 32
TILE = 256
HALO = 16
SLOT = (0, 3, 1, 2)

SHAPES = {64: (8, 4, 2)}


def softcap(values):
    return gate_cap * jnp.tanh(values * (1.0 / gate_cap))


def log_one_plus(values):
    series = values * (
        1.0 + values * (-1 / 2 + values * (1 / 3 + values * (-1 / 4 + values * (1 / 5))))
    )
    return jnp.where(values < 0.015625, series, jnp.log(1.0 + values))


def log_sigmoid(values):
    return jnp.minimum(values, 0.0) - log_one_plus(jnp.exp(-jnp.abs(values)))


def normalize(values, gains):
    return values * lax.rsqrt(jnp.mean(values * values, axis=-1, keepdims=True) + epsilon) * gains


def matmul(left, right, left_dim=1, right_dim=0):
    return lax.dot_general(
        left, right, (((left_dim,), (right_dim,)), ((), ())), preferred_element_type=f32
    )


def mod(value, size):
    return lax.rem(value + size, jnp.int32(size))


def kernel(
    Z, X, C, T,
    q_in, k_in, v_in, og_in, ig_in, fg_in, res_in, mixg_in, preg_in, postg_in, gk_in, vk_in,
    outp_ref, gatep_ref, valuep_ref, downp_ref,
    out_ref,
    q_ref, k_ref, v_ref, og_ref, ig_ref, fg_ref, res_ref, mixg_ref, preg_ref, postg_ref, gk_own, vk_own,
    msend, sib_m, csend, mrecv, st_src, sib_st, cst, st_recv, ssend, srecv, nin, m_in, kwb, runc, a1, m1, d1,
    gated, wo, ushard, wu, dshard, wd, gk_ref, vk_ref, rows_all, stream, upb, hidden,
    mix_part, mix_left, mix_right, mix_top, mix_bot,
    ffn_part, ffn_left, ffn_right, ffn_top, ffn_bot,
    loc, loaded, pre, p1, p2, post, xs, xd, zs, zd, taps, ags, mss, rss, halo,
):
    NSP = Z * X * C
    rows, qk = q_ref.shape
    hv = v_ref.shape[1]
    own, D = out_ref.shape
    ffd = gatep_ref.shape[1]
    scale = float(qk) ** -0.5
    me = lax.axis_index("sp")
    tp = lax.axis_index("tp")
    core = lax.rem(me, jnp.int32(C))
    xx = lax.rem(lax.div(me, jnp.int32(C)), jnp.int32(X))
    zz = lax.div(me, jnp.int32(C * X))
    pending = []

    def at_sp(index):
        return {"sp": index, "tp": tp}

    def at_tp(index):
        return {"sp": me, "tp": index}

    def at_zx(z, x, c):
        return z * (X * C) + x * C + c

    def remote(src, dst, ssem, rsem, device):
        return pltpu.make_async_remote_copy(
            src_ref=src, dst_ref=dst, send_sem=ssem, recv_sem=rsem,
            device_id=device, device_id_type=MESH,
        )

    def send(src, dst, ssem, rsem, device):
        copy = remote(src, dst, ssem, rsem, device)
        copy.start()
        pending.append(copy)

    def send_if(condition, src, dst, ssem, rsem, device):
        copy = remote(src, dst, ssem, rsem, device)
        pl.when(condition)(copy.start)
        pending.append((condition, copy))

    def arrived(dst, ssem, rsem, device):
        remote(dst, dst, ssem, rsem, device).wait_recv()

    def ds(start, size, step=None):
        return pl.ds(pl.multiple_of(start, step or size), size)

    sibling = at_sp(me + 1 - 2 * core)

    units = lax.rem(xx + tp, jnp.int32(T))

    def holder(x):
        return {"sp": at_zx(zz, x, core), "tp": mod(tp - x, T)}

    def source(x):
        return {"sp": at_zx(zz, x, core), "tp": units}

    barrier = pltpu.get_barrier_semaphore()

    chips = NSP // C
    chip = lax.div(me, jnp.int32(C))

    def at_chip(index):
        return at_sp(index * C + core)

    def greet(p, carry):
        pl.semaphore_signal(
            barrier, 1, device_id=at_chip(mod(chip + p, chips)), device_id_type=MESH
        )
        return carry

    lax.fori_loop(1, chips, greet, 0)
    pl.semaphore_signal(barrier, 1, device_id=sibling, device_id_type=MESH)
    for k in range(1, T):
        pl.semaphore_signal(barrier, 1, device_id=at_tp(mod(tp + k, T)), device_id_type=MESH)
    for k in range(X):

        @pl.when(xx + k > 0)
        def _(k=k):
            pl.semaphore_signal(barrier, 1, device_id=source(k), device_id_type=MESH)

    loads = [
        pltpu.make_async_copy(src, dst, loaded.at[i])
        for i, (src, dst) in enumerate((
            (ig_in, ig_ref), (fg_in, fg_ref), (k_in, k_ref), (v_in, v_ref), (q_in, q_ref),
            (og_in, og_ref), (res_in, res_ref), (mixg_in, mixg_ref), (preg_in, preg_ref),
            (postg_in, postg_ref), (gk_in, gk_own), (vk_in, vk_own),
        ))
    ]
    shard = gatep_ref.shape[0]
    local = [
        pltpu.make_async_copy(gatep_ref, ushard.at[:, pl.ds(0, ffd)], loc.at[0]),
        pltpu.make_async_copy(valuep_ref, ushard.at[:, pl.ds(ffd, ffd)], loc.at[1]),
        pltpu.make_async_copy(downp_ref, dshard, loc.at[2]),
        pltpu.make_async_copy(outp_ref, wo, loc.at[3]),
    ]
    for copy in loads + local:
        copy.start()

    steps = rows // ROW_STEP
    lane = lax.broadcasted_iota(jnp.int32, (ROW_STEP, rows), 1)
    line = lax.broadcasted_iota(jnp.int32, (ROW_STEP, rows), 0)
    loads[0].wait()
    loads[1].wait()
    li_row = softcap(ig_ref[...])
    lf_row = log_sigmoid(softcap(fg_ref[...]))

    def sums(b, run_row):
        here = line + b * ROW_STEP
        run_col = jnp.sum(jnp.where(lane <= here, lf_row, 0.0), axis=1, keepdims=True)
        runc[ds(b * ROW_STEP, ROW_STEP), :] = run_col
        return run_row + jnp.sum(jnp.where(lane == here, run_col, 0.0), axis=0, keepdims=True)

    run_row = lax.fori_loop(0, steps, sums, jnp.zeros((1, rows), f32), unroll=True)
    total = run_row[:, rows - 1 : rows]
    lead = total - run_row + li_row
    lead_max = jnp.max(lead, axis=1, keepdims=True)
    lead_weights = jnp.exp(lead - lead_max)
    loads[2].wait()
    loads[3].wait()

    def weigh(b, normer):
        here = line + b * ROW_STEP
        at = ds(b * ROW_STEP, ROW_STEP)
        column = jnp.sum(jnp.where(lane == here, lead_weights, 0.0), axis=1, keepdims=True)
        weighted = k_ref[at, :].astype(f32) * column
        kwb[at, :] = weighted.astype(bf16)
        return normer + jnp.sum(weighted, axis=0, keepdims=True)

    normer = lax.fori_loop(0, steps, weigh, jnp.zeros((1, qk), f32), unroll=True)
    nq = qk // LANES
    for r in range(nq):
        st_src[r : r + 1, :] = normer[:, r * LANES : (r + 1) * LANES]
    for r in range(nq, 4):
        st_src[r : r + 1, :] = jnp.broadcast_to(total if r == nq else lead_max, (1, LANES))
    R = msend.shape[1]
    nc = hv // LANES
    for r in range(nq):
        part = matmul(kwb[:, r * LANES : (r + 1) * LANES], v_ref[...], 0, 0)
        for rr in range(LANES // R):
            for c in range(nc):
                j = (r * (LANES // R) + rr) * nc + c
                msend[j % C * chips + j // C] = part[
                    rr * R : (rr + 1) * R, c * LANES : (c + 1) * LANES
                ].astype(bf16)

    with jax.named_scope("barrier"):
        pl.semaphore_wait(barrier, chips + T - 1 + X - 1 + jnp.minimum(xx, 1))

    send(msend, sib_m, pre.at[0, 0], pre.at[1, 0], sibling)
    send(st_src, sib_st, pre.at[0, 1], pre.at[1, 1], sibling)
    is_first = core == 0
    with jax.named_scope("pair"):
        arrived(sib_st, pre.at[0, 1], pre.at[1, 1], sibling)
        arrived(sib_m, pre.at[0, 0], pre.at[1, 0], sibling)
    one = jnp.where(is_first, st_src[...], sib_st[...])
    two = jnp.where(is_first, sib_st[...], st_src[...])

    def meet(highest, following):
        decayed = highest + following[nq : nq + 1, :]
        lead_d = following[nq + 1 : nq + 2, :]
        new = jnp.maximum(decayed, lead_d)
        return new, jnp.exp(decayed - new), jnp.exp(lead_d - new)

    pair_max, weight_one, weight_two = meet(one[nq + 1 : nq + 2, :], two)
    cst[0:nq, :] = weight_one * one[0:nq, :] + weight_two * two[0:nq, :]
    cst[nq : nq + 1, :] = one[nq : nq + 1, :] + two[nq : nq + 1, :]
    cst[nq + 1 : nq + 2, :] = pair_max
    weight_mine = jnp.where(is_first, weight_one, weight_two)
    weight_sib = jnp.where(is_first, weight_two, weight_one)

    def pair(i, carry):
        for u in range(4):
            j = i * 4 + u
            csend[j] = (
                weight_mine * msend[core * chips + j].astype(f32)
                + weight_sib * sib_m[core * chips + j].astype(f32)
            ).astype(bf16)
        return carry

    lax.fori_loop(0, chips // 4, pair, 0)

    mrecv[chip] = csend[chip]
    st_recv[chip] = cst[...]

    def scatter(p, carry):
        dst = mod(chip + p, chips)
        remote(csend.at[dst], mrecv.at[chip], p1.at[0], p1.at[1], at_chip(dst)).start()
        remote(cst, st_recv.at[chip], p1.at[2], p1.at[3], at_chip(dst)).start()
        return carry

    with jax.named_scope("scatter"):
        lax.fori_loop(1, chips, scatter, 0)

    left, right, across = mod(tp - 1, T), mod(tp + 1, T), mod(tp + 2, T)
    along_y = (tp, left, right, across, at_tp)

    def block_piece(side, low, r):
        return rows_all.at[pl.ds(block_base(side) + low * half + r * part, part)]

    def ring_start(r, ks):
        for k in ks:
            low, side = ((0, 2), (1, 1), (1, 2), (0, 1))[k]
            send(
                block_piece(0, low, r), block_piece(3 - side, low, r),
                ags.at[0, r, k], ags.at[1, r, k], at_ring(ring[side]),
            )

    def ag_wait(r, k):
        with jax.named_scope("ag" + str(k)):
            side, low = ((1, 0), (2, 1), (1, 1), (2, 0), (3, 0), (3, 1))[k]
            piece = block_piece(side, low, r)
            arrived(piece, ags.at[0, r, k], ags.at[1, r, k], at_ring(fl))
            if k < 2:
                to = at_ring((fr, fl)[k])
                send(piece, block_piece(3, low, r), ags.at[0, r, k + 4], ags.at[1, r, k + 4], to)

    for copy in local:
        copy.wait()
    for copy in loads[4:]:
        copy.wait()

    def rows_of(index):
        return ds(index * shard, shard)

    weights = ((ushard, wu), (dshard, wd))
    def spread(w):
        src, dst = weights[w]
        for k in range(X):
            send_if(
                xx + k > 0, src, dst.at[rows_of(me)], xs.at[0, k, w], xs.at[1, xx, w], holder(k)
            )

    spread(0)

    @pl.when(xx == 0)
    def _():
        for src, dst in weights:
            dst[rows_of(me), :] = src[...]

    for i, (src, dst) in enumerate(((gk_own, gk_ref), (vk_own, vk_ref))):
        send_if(xx > 0, src, dst, taps.at[0, i], taps.at[1, i], at_tp(mod(tp - xx, T)))

    @pl.when(xx == 0)
    def _():
        gk_ref[...] = gk_own[...]
        vk_ref[...] = vk_own[...]

    def inside(b, carry):
        at = ds(b * ROW_STEP, ROW_STEP)
        here = line + b * ROW_STEP
        logs = jnp.where(lane <= here, runc[at, :] - run_row + li_row, far_below)
        top = jnp.max(logs, axis=1, keepdims=True)
        scores = matmul(q_ref[at, :], k_ref[...], 1, 1) * (jnp.exp(logs - top) * scale)
        m1[at, :] = top
        d1[at, :] = jnp.sum(scores, axis=1, keepdims=True)
        a1[at, :] = matmul(scores.astype(bf16), v_ref[...])
        return carry

    with jax.named_scope("inside"):
        lax.fori_loop(0, steps, inside, 0)

    def shards(w, ks):
        for k in ks:
            piece = weights[w][1].at[rows_of(at_zx(zz, k, core))]

            @pl.when(xx + k > 0)
            def _():
                arrived(piece, xs.at[0, k, w], xs.at[1, k, w], source(k))

            send(piece, piece, xd.at[0, k, w], xd.at[1, k, w], sibling)

    def shard_twins(w):
        for k in range(X):
            piece = weights[w][1].at[rows_of(at_zx(zz, k, 1 - core))]
            arrived(piece, xd.at[0, k, w], xd.at[1, k, w], sibling)

    def all_but_one(buf):
        return buf.at[pl.ds(0, chips - 1)]

    def bulk(buf, sems, s):
        remote(all_but_one(buf), all_but_one(buf), sems.at[s], sems.at[s + 1], at_sp(me)).wait()

    with jax.named_scope("p1wait"):
        bulk(mrecv, p1, 0)
        bulk(st_recv, p1, 2)

    def advance(i, state):
        highest, memory, norm = state
        for u in range(4):
            d = i * 4 + u
            ssend[d] = memory.astype(bf16)
            nin[d, 0:nq, :] = norm
            nin[d, nq : nq + 1, :] = highest
            following = st_recv[d]
            highest, before, after = meet(highest, following)
            memory = before * memory + after * mrecv[d].astype(f32)
            norm = before * norm + after * following[0:nq, :]
        return highest, memory, norm

    lax.fori_loop(
        0, chips // 4, advance,
        (jnp.full((1, LANES), far_below, f32), jnp.zeros((R, LANES), f32), jnp.zeros((nq, LANES), f32)),
    )
    part_of_core = pl.ds(core * chips, chips)
    srecv[core * chips + chip] = ssend[chip]

    def give_back(p, carry):
        dst = mod(chip + p, chips)
        remote(
            ssend.at[dst], srecv.at[core * chips + chip], p2.at[0], p2.at[1], at_chip(dst)
        ).start()
        return carry

    with jax.named_scope("giveback"):
        lax.fori_loop(1, chips, give_back, 0)

    spread(1)
    slab = shard * X * C
    ups = (at_zx(mod(zz + 1, Z), xx, core), at_zx(mod(zz - 1, Z), xx, core))

    def z_piece(w, direction, s, h, c):
        z = mod(zz - s if direction == 0 else zz + s, Z)
        return [
            weights[w][1].at[rows_of(at_zx(z, h * (X // 2) + q, c))] for q in range(X // 2)
        ]

    def z_has(direction, s, h):
        return s < Z // 2 or (s == Z // 2 and h == direction)

    def z_send(w, direction, s, h):
        if z_has(direction, s, h):
            i = (s - 1) * 2 + h
            for q, piece in enumerate(z_piece(w, direction, s - 1, h, core)):
                send(
                    piece, piece, zs.at[0, w, direction, i, q], zs.at[1, w, direction, i, q],
                    at_sp(ups[direction]),
                )

    def z_start(w, h):
        for direction in range(2):
            z_send(w, direction, 1, h)

    def z_step(w, s, h):
        with jax.named_scope(("uring", "dring")[w] + str(s) + str(h)):
            for direction in range(2):
                if z_has(direction, s, h):
                    pieces = z_piece(w, direction, s, h, core)
                    i = (s - 1) * 2 + h
                    for q, piece in enumerate(pieces):
                        arrived(
                            piece, zs.at[0, w, direction, i, q], zs.at[1, w, direction, i, q],
                            at_sp(ups[direction]),
                        )
                    z_send(w, direction, s + 1, h)
                    for q, piece in enumerate(pieces):
                        send(
                            piece, piece, zd.at[0, w, direction, i, q], zd.at[1, w, direction, i, q],
                            sibling,
                        )

    def z_twin(w, distances):
        with jax.named_scope(("utwin", "dtwin")[w]):
            for s in distances:
                for h in range(2):
                    for direction in range(2):
                        if z_has(direction, s, h):
                            i = (s - 1) * 2 + h
                            for q, piece in enumerate(z_piece(w, direction, s, h, 1 - core)):
                                arrived(
                                    piece, zd.at[0, w, direction, i, q],
                                    zd.at[1, w, direction, i, q], sibling,
                                )

    u_events = [(0, s, h) for s in range(1, Z // 2 + 1) for h in range(2)]
    d_events = [(1, s, h) for s in range(1, Z // 2 + 1) for h in range(2)]

    def z_next(events):
        if events:
            z_step(*events.pop(0))

    with jax.named_scope("ushards"):
        shards(0, range(X // 2))
    z_start(0, 0)
    with jax.named_scope("ushards2"):
        shards(0, range(X // 2, X))

    with jax.named_scope("p2wait"):
        bulk(srecv, p2, 0)
    mine = srecv.at[part_of_core]
    send(mine, mine, post.at[0], post.at[1], sibling)
    z_start(0, 1)
    with jax.named_scope("postwait"):
        other = srecv.at[pl.ds((C - 1 - core) * chips, chips)]
        arrived(other, post.at[0], post.at[1], sibling)
    stats = nin[chip]
    ahead_max, ahead_scale, sib_scale = meet(stats[nq : nq + 1, :], sib_st[...])
    ahead_max = jnp.where(is_first, stats[nq : nq + 1, :], ahead_max)
    ahead_scale = jnp.where(is_first, 1.0, ahead_scale)
    sib_scale = jnp.where(is_first, 0.0, sib_scale)
    ahead_normer = ahead_scale * stats[0:nq, :] + sib_scale * sib_st[0:nq, :]
    for j in range(NSP):
        r, c = divmod(j, nc)
        i = j % C * chips + j // C
        m_in[r * R : (r + 1) * R, c * LANES : (c + 1) * LANES] = (
            ahead_scale * srecv[i].astype(f32) + sib_scale * sib_m[i].astype(f32)
        ).astype(bf16)
    normer_in = jnp.concatenate([ahead_normer[r : r + 1, :] for r in range(nq)], axis=1)
    stab = ahead_max[:, 0:1]

    def finish(b, carry):
        at = ds(b * ROW_STEP, ROW_STEP)
        queries = q_ref[at, :]
        carried = runc[at, :] + stab
        top = m1[at, :]
        row_max = jnp.maximum(carried, top)
        inner = jnp.exp(top - row_max)
        outer = jnp.exp(carried - row_max) * scale
        reach = jnp.sum(queries.astype(f32) * normer_in, axis=1, keepdims=True)
        denominator = inner * d1[at, :] + outer * reach
        floor = jnp.maximum(jnp.abs(denominator), jnp.exp(-row_max))
        numerator = inner * a1[at, :] + outer * matmul(queries, m_in[...])
        gate = 1.0 / (1.0 + jnp.exp(-og_ref[at, :].astype(f32)))
        gated[at, :] = (numerator / floor * gate).astype(bf16)
        return carry

    half = own // 2
    part = half // 2

    class Sums:
        def __init__(self, view, base, ring, sems, summed, from_left, from_right, relay_top, relay_bot):
            self.view, self.base, self.ring, self.sems, self.summed = view, base, ring, sems, summed
            self.from_left, self.from_right = from_left, from_right
            self.relays = (relay_top, relay_bot)

        def send(self, src, dst, r, k, side):
            to = self.ring[4](self.ring[side])
            send(src, dst, self.sems.at[0, r, k], self.sems.at[1, r, k], to)

        def wait(self, dst, r, k):
            arrived(dst, self.sems.at[0, r, k], self.sems.at[1, r, k], self.ring[4](self.ring[1]))

        def piece(self, side, low, r):
            return self.view(self.summed, self.base(side) + low * half, r)

        def at_owner(self, buf, low, r):
            return self.view(buf, low * half, r)

        def far(self, r):
            for low in range(2):
                self.send(
                    self.piece(3, low, r), self.view(self.relays[low], 0, r), r, 2 + low, 2 - low
                )

        def near(self, r):
            self.send(self.piece(2, 1, r), self.at_owner(self.from_left, 1, r), r, 0, 2)
            self.send(self.piece(1, 0, r), self.at_owner(self.from_right, 0, r), r, 1, 1)

        def relay(self, r):
            for low, buf in ((0, self.from_left), (1, self.from_right)):
                relay = self.view(self.relays[low], 0, r)
                own_piece = self.piece(2 - low, low, r)
                with jax.named_scope("relay"):
                    self.wait(relay, r, 2 + low)
                if len(relay.shape) == 3:
                    steps_here = relay.shape[0]
                else:
                    steps_here = relay.shape[0] // NORM_STEP

                def merge(b, carry, relay=relay, own_piece=own_piece):
                    at = b if len(relay.shape) == 3 else ds(b * NORM_STEP, NORM_STEP)
                    relay[at] = (relay[at].astype(f32) + own_piece[at].astype(f32)).astype(bf16)
                    return carry

                lax.fori_loop(0, steps_here, merge, 0)
                self.send(relay, self.at_owner(buf, low, r), r, 4 + low, 2 - low)

        def finish(self, r):
            with jax.named_scope("sumwait"):
                self.wait(self.at_owner(self.from_left, 1, r), r, 0)
                self.wait(self.at_owner(self.from_right, 0, r), r, 1)
                self.wait(self.at_owner(self.from_left, 0, r), r, 4)
                self.wait(self.at_owner(self.from_right, 1, r), r, 5)

    def mix_view(ref, row, r):
        return ref.at[ds(row + r * part, part, 16)]

    mixes = Sums(mix_view, lambda side: along_y[side] * own, along_y, mss, mix_part, mix_left, mix_right, mix_top, mix_bot)

    def project(block):
        lines = ds(block * own, own)

        def project_tile(n, carry):
            at = ds(n * TILE, TILE)
            mix_part[lines, at] = matmul(gated[lines, :], wo[:, at]).astype(bf16)
            return carry

        with jax.named_scope("finish"):
            each = own // ROW_STEP
            lax.fori_loop(block * each, (block + 1) * each, finish, 0)
        with jax.named_scope("project"):
            lax.fori_loop(0, D // TILE, project_tile, 0)

    project(across)
    mixes.far(0)
    mixes.far(1)
    z_next(u_events)
    project(right)
    project(left)
    mixes.near(0)
    z_next(u_events)
    project(tp)

    def at_ring(index):
        return {
            "sp": me + core * (at_zx(zz, index, core) - me),
            "tp": index + core * (tp - index),
        }

    spot = tp + core * (xx - tp)
    fl, fr, fo = mod(spot - 1, T), mod(spot + 1, T), mod(spot + 2, T)
    ring = (spot, fl, fr, fo, at_ring)
    block_rows = own + HALO

    def block_base(block):
        return SLOT[block] * block_rows + HALO

    def join(r):
        def join_rows(b, carry):
            row = lax.rem(b, jnp.int32(part // NORM_STEP)) * NORM_STEP + r * part
            row = row + lax.div(b, jnp.int32(part // NORM_STEP)) * half
            at = ds(row, NORM_STEP)
            summed = (
                mix_part[ds(tp * own + row, NORM_STEP), :].astype(f32)
                + mix_left[at, :].astype(f32)
                + mix_right[at, :].astype(f32)
            )
            values = summed.astype(bf16).astype(f32)
            joined = (res_ref[at, :].astype(f32) + normalize(values, mixg_ref[...])).astype(bf16)
            stream[at, :] = joined
            rows_all[ds(block_base(0) + row, NORM_STEP), :] = normalize(
                joined.astype(f32), preg_ref[...]
            ).astype(bf16)
            return carry

        with jax.named_scope("join"):
            lax.fori_loop(0, 2 * (part // NORM_STEP), join_rows, 0, unroll=2)

    mixes.relay(0)
    mixes.near(1)
    z_next(u_events)
    mixes.relay(1)
    z_next(u_events)
    with jax.named_scope("dshards"):
        shards(1, range(X))
    z_next(u_events)
    z_start(1, 0)
    mixes.finish(0)
    join(0)
    ring_start(0, (0, 1, 2, 3))
    z_next(u_events)
    z_start(1, 1)
    mixes.finish(1)
    join(1)
    ring_start(1, (0, 1))

    place = me * T + tp
    after = place + 1
    is_last = after == NSP * T
    nsp = lax.rem(lax.div(after, jnp.int32(T)), jnp.int32(NSP))
    ntp = lax.rem(after, jnp.int32(T))
    ncore = lax.rem(nsp, jnp.int32(C))
    nx = lax.rem(lax.div(nsp, jnp.int32(C)), jnp.int32(X))
    nz = lax.div(nsp, jnp.int32(C * X))
    npos = ntp + ncore * (nx - ntp)
    tail_lines = pl.ds(block_base(0) + own - HALO, HALO)
    for k in range(T):
        to_sp = nsp + ncore * (at_zx(nz, k, ncore) - nsp)
        to_tp = k + ncore * (ntp - k)
        slot = mod(npos - k, T)
        to_lines = ds(slot * block_rows, HALO, 16)
        to_self = to_sp * T + to_tp == place
        go = jnp.logical_not(jnp.logical_or(is_last, to_self))
        send_if(
            go, rows_all.at[tail_lines], rows_all.at[to_lines], halo.at[0, k], halo.at[1, slot],
            {"sp": to_sp, "tp": to_tp},
        )

        @pl.when(jnp.logical_and(to_self, jnp.logical_not(is_last)))
        def _(to_lines=to_lines):
            rows_all[to_lines, :] = rows_all[tail_lines, :]

    ring_start(1, (2, 3))

    def halo_wait(slot):
        device = at_ring(mod(spot + slot, T))
        ahead = device["sp"] * T + device["tp"] - 1
        lines = pl.ds(slot * block_rows, HALO)

        @pl.when(ahead < 0)
        def _():
            rows_all[lines, :] = jnp.zeros((HALO, D), bf16)

        @pl.when(jnp.logical_and(ahead >= 0, ahead != place))
        def _():
            arrived(rows_all.at[lines], halo.at[0, 0], halo.at[1, slot], device)

    ag_wait(0, 0)
    ag_wait(0, 1)
    z_next(u_events)
    z_next(d_events)
    ag_wait(1, 0)
    ag_wait(1, 1)
    while u_events:
        z_next(u_events)
    z_next(d_events)

    @pl.when(xx > 0)
    def _():
        for i, dst in enumerate((gk_ref, vk_ref)):
            arrived(dst, taps.at[0, i], taps.at[1, i], at_tp(mod(tp + xx, T)))

    with jax.named_scope("shtwins"):
        shard_twins(0)
        shard_twins(1)
    z_twin(0, range(1, Z // 2 + 1))

    def mix(first, last):
        for slot in range(first, last):
            halo_wait(slot)
        lines = pl.ds(first * block_rows, (last - first) * block_rows)
        within = pl.ds(0, (last - first) * block_rows)

        def raise_tile(n, carry):
            at = ds(n * TILE, TILE)
            upb[within, at] = matmul(rows_all[lines, :], wu[:, at]).astype(bf16).astype(f32)
            return carry

        with jax.named_scope("raise"):
            lax.fori_loop(0, ffd // TILE, raise_tile, 0)
        z_next(d_events)
        with jax.named_scope("raise"):
            lax.fori_loop(ffd // TILE, 2 * ffd // TILE, raise_tile, 0)
        if first > 0:
            z_next(d_events)
        windows = own // CONV_STEP

        def convolve(b, carry):
            block = lax.div(b, jnp.int32(windows))
            row = lax.rem(b, jnp.int32(windows)) * CONV_STEP
            window = ds(block * block_rows + row + HALO - 8, CONV_STEP + 8, 8)
            at = ds((first + block) * own + row, CONV_STEP)
            for c in range(0, ffd, TILE):
                both = []
                for taps_ref, start in ((gk_ref, 0), (vk_ref, ffd)):
                    block_values = upb[window, start + c : start + c + TILE]
                    summed = 0.0
                    for j in range(CONV):
                        low = 8 - CONV + 1 + j
                        summed = summed + taps_ref[j : j + 1, c : c + TILE] * block_values[low : low + CONV_STEP]
                    both.append(summed)
                hidden[at, c : c + TILE] = (both[0] / (1.0 + jnp.exp(-both[0])) * both[1]).astype(bf16)
            return carry

        with jax.named_scope("conv"):
            lax.fori_loop(0, (last - first) * windows, convolve, 0)

    zs_order = [zz]
    for d in range(1, Z // 2):
        zs_order += [mod(zz - d, Z), mod(zz + d, Z)]
    zs_order.append(mod(zz + Z // 2, Z))
    early = max(1, Z - 3)

    def lower(first, last):
        def lower_tile(tile, carry):
            away = lax.div(tile + 1, jnp.int32(2)) * (1 - 2 * lax.rem(tile, jnp.int32(2)))
            z = lax.rem(zz + away + Z, jnp.int32(Z))
            ffn_part[tile] = matmul(hidden[...], wd[ds(z * slab, slab), :], 1, 1).astype(bf16)
            return carry

        with jax.named_scope("lower"):
            lax.fori_loop(first, last, lower_tile, 0)

    def ffn_view(ref, row, r):
        tiles = pl.ds(0, early) if r == 0 else pl.ds(early, Z - early)
        return ref.at[tiles, ds(row, half), :]

    ffns = Sums(ffn_view, lambda side: SLOT[side] * own, ring, rss, ffn_part, ffn_left, ffn_right, ffn_top, ffn_bot)
    mix(0, 1)
    z_next(d_events)
    for k in (2, 3, 4, 5):
        ag_wait(0, k)
    for k in (2, 3, 4, 5):
        ag_wait(1, k)
    mix(1, T)
    while d_events and d_events[0][1] <= max(0, (early - 1) // 2):
        z_next(d_events)
    z_twin(1, range(1, (early - 1) // 2 + 1))
    lower(0, early)
    ffns.far(0)
    ffns.near(0)
    while d_events:
        z_next(d_events)
    if early < Z - 1:
        z_twin(1, range((early - 1) // 2 + 1, Z // 2))
        lower(early, Z - 1)
    z_twin(1, (Z // 2,))
    lower(Z - 1, Z)
    ffns.far(1)
    ffns.relay(0)
    ffns.near(1)
    ffns.relay(1)
    ffns.finish(0)
    ffns.finish(1)

    def close(b, carry):
        at = ds(b * NORM_STEP, NORM_STEP)
        mine = ds(b * NORM_STEP, NORM_STEP)
        values, squares = [], 0.0
        for tile in range(Z):
            summed = (
                ffn_part[tile, mine, :].astype(f32)
                + ffn_left[tile, at, :].astype(f32)
                + ffn_right[tile, at, :].astype(f32)
            )
            values.append(summed.astype(bf16).astype(f32))
            squares = squares + jnp.sum(values[-1] * values[-1], axis=-1, keepdims=True)
        factor = lax.rsqrt(squares * (1.0 / D) + epsilon)
        for tile in range(Z):
            to = ds(zs_order[tile] * slab, slab)
            out_ref[at, to] = (
                stream[at, to].astype(f32) + values[tile] * factor * postg_ref[:, to]
            ).astype(bf16)
        return carry

    with jax.named_scope("close"):
        lax.fori_loop(0, own // NORM_STEP, close, 0, unroll=2)

    for copy in pending:
        if isinstance(copy, tuple):
            pl.when(copy[0])(copy[1].wait_send)
        else:
            copy.wait_send()


def body(
    shape,
    query_rows, key_rows, value_rows, out_gate_pre, input_gate_pre, forget_gate_pre, residual,
    out_proj, mix_gain, pre_gain, gate_proj, value_proj, gate_kernel, value_kernel, down_proj,
    post_gain,
):
    Z, X, C, T = shape
    NSP = Z * X * C
    rows, qk = query_rows.shape
    hv = value_rows.shape[1]
    own, D = residual.shape
    ffd = gate_proj.shape[1]
    R = qk * hv // LANES // NSP
    dma = pltpu.SemaphoreType.DMA
    vm = pltpu.VMEM
    inner = pl.BlockSpec(memory_space=pltpu.VMEM)
    outer = pl.BlockSpec(memory_space=pl.ANY)
    return pl.pallas_call(
        functools.partial(kernel, Z, X, C, T),
        out_shape=pltpu.VMEM((own, D), bf16),
        in_specs=[outer] * 16,
        out_specs=inner,
        scratch_shapes=[
            vm((rows, qk), bf16),
            vm((rows, qk), bf16),
            vm((rows, hv), bf16),
            vm((rows, hv), bf16),
            vm((1, rows), f32),
            vm((1, rows), f32),
            vm((own, D), bf16),
            vm((1, D), f32),
            vm((1, D), f32),
            vm((1, D), f32),
            vm((CONV, ffd), f32),
            vm((CONV, ffd), f32),
            vm((NSP, R, LANES), bf16),
            vm((NSP, R, LANES), bf16),
            vm((NSP // C, R, LANES), bf16),
            vm((NSP // C, R, LANES), bf16),
            vm((4, LANES), f32),
            vm((4, LANES), f32),
            vm((4, LANES), f32),
            vm((NSP // C, 4, LANES), f32),
            vm((NSP // C, R, LANES), bf16),
            vm((NSP, R, LANES), bf16),
            vm((NSP // C, 4, LANES), f32),
            vm((qk, hv), bf16),
            vm((rows, qk), bf16),
            vm((rows, 1), f32),
            vm((rows, hv), f32),
            vm((rows, 1), f32),
            vm((rows, 1), f32),
            vm((rows, hv), bf16),
            vm((hv, D), bf16),
            vm((D // NSP, 2 * ffd), bf16),
            vm((D, 2 * ffd), bf16),
            vm((D // NSP, ffd), bf16),
            vm((D, ffd), bf16),
            vm((CONV, ffd), f32),
            vm((CONV, ffd), f32),
            vm((T * (own + HALO), D), bf16),
            vm((own, D), bf16),
            vm(((T - 1) * (own + HALO), 2 * ffd), f32),
            vm((rows, ffd), bf16),
        ]
        + [
            vm((rows, D), bf16),
            vm((own, D), bf16),
            vm((own, D), bf16),
            vm((own // 2, D), bf16),
            vm((own // 2, D), bf16),
            vm((Z, rows, D // Z), bf16),
            vm((Z, own, D // Z), bf16),
            vm((Z, own, D // Z), bf16),
            vm((Z, own // 2, D // Z), bf16),
            vm((Z, own // 2, D // Z), bf16),
        ]
        + [
            dma((4,)),
            dma((12,)),
            dma((2, 2)),
            dma((4,)),
            dma((2,)),
            dma((2,)),
            dma((2, X, 2)),
            dma((2, X, 2)),
            dma((2, 2, 2, Z, X // 2)),
            dma((2, 2, 2, Z, X // 2)),
            dma((2, 2)),
            dma((2, 2, 6)),
            dma((2, 2, 6)),
            dma((2, 2, 6)),
            dma((2, T)),
        ],
        compiler_params=pltpu.CompilerParams(
            collective_id=0, has_side_effects=True, vmem_limit_bytes=60 * 1024 * 1024
        ),
        name="cell_and_mixer",
    )(
        query_rows, key_rows, value_rows, out_gate_pre, input_gate_pre, forget_gate_pre, residual,
        mix_gain.reshape(1, D), pre_gain.reshape(1, D), post_gain.reshape(1, D),
        gate_kernel, value_kernel, out_proj, gate_proj, value_proj, down_proj,
    )


def solution(mesh):
    shape = (*SHAPES[mesh.shape["sp"]], mesh.shape["tp"])
    placed = (
        P("sp", "tp"),
        P("sp", "tp"),
        P("sp", "tp"),
        P("sp", "tp"),
        P("tp", "sp"),
        P("tp", "sp"),
        P(("sp", "tp"), None),
        P("tp", None),
        P(),
        P(),
        P("sp", "tp"),
        P("sp", "tp"),
        P(None, "tp"),
        P(None, "tp"),
        P("sp", "tp"),
        P(),
    )
    return jax.shard_map(
        functools.partial(body, shape), mesh=mesh, in_specs=placed,
        out_specs=P(("sp", "tp"), None), check_vma=False,
    )
```
